32 devices in a mesh: gr: 2 (over x), sp: 8 (over z, y), tp: 2 (over core).
Axes of the slice: x: 2, y: 2, z: 4, core: 2. Of those that a mesh axis runs over, the one named last changes fastest.
Arguments:
- context_input_tensor: bfloat16 [4, 8192, 2048], P(('gr', 'tp'), 'sp'), parts along dimension 0, may hold values from -8 to 8
- content_mapping_matrix: bfloat16 [2048, 1024], replicated, may hold values from -0.125 to 0.125
- address_mapping_matrix: bfloat16 [2048, 256], replicated, may hold values from -0.125 to 0.125
- increment_mapping_matrix: bfloat16 [2048, 16], replicated, may hold values from -0.125 to 0.125
- increment_speed_offset: float32 [16], P('sp'), may hold values from -1 to 0.5
- channel_fading_exponent: float32 [16], P('sp'), may hold values from -12 to -2
- extra_damping_spikes: float32 [4, 16, 8192], P(('gr', 'tp'), 'sp'), parts along dimension 0, may hold values from -3 to 0
- content_smoothing_coefficients: float32 [5, 16, 64], P(None, 'sp'), may hold values from -2.5 to 2.5
- address_smoothing_coefficients: float32 [5, 4, 64], replicated, may hold values from -2.5 to 2.5
- newest_lookup_matrix: bfloat16 [4, 4, 64], P(('gr', 'tp')), parts along dimension 0, may hold values from -6 to 6
- newest_output_switch: bfloat16 [4, 16, 64], P(('gr', 'tp'), 'sp'), parts along dimension 0, may hold values from -6 to 6
- cluster_scaling_coefficients: float32 [16, 64], P('sp'), may hold values from 0.1 to 1.9
Outputs:
- address_content_store: bfloat16 [4, 8192, 16, 128], P(('gr', 'tp'), None, 'sp'), parts along dimension 0
- earliest_switched_retrieval: bfloat16 [4, 16, 64], P(('gr', 'tp'), 'sp'), parts along dimension 0
The draws below stay inside these ranges and needn't reach their ends.
There are 2 independent parts, one for each index of `gr`. The reference program is written for one: setup_inputs(seed, part) draws one part's arguments, and reference() takes and returns one part's arrays. A program takes and returns all parts, laid end to end along the dimension named above; an argument that names none is the same for every part. Nothing has to cross between parts.
All inputs are finite; a program needn't handle non-finite values.
Results may differ from the reference program's by a relative error of at most 0.009.
Values may be sent and summed in bfloat16 or wider, within the bound.
No kernel may reach another device: no remote copies, remote signals or barrier semaphores. Data moves between devices by JAX's collectives and lax.ppermute only.
A program may use at most 128 MiB of HBM per device.

```python
import math
import jax
import jax.numpy as jnp
from jax import lax

MODEL = 2048
HEADS = 16
HEAD = 64
GROUPS = 4
STATE = 64
KERNEL = 5
SPAN = 1024
SEQS = 2
LEN = 8192


def draw_context_input_tensor(key, part):
    key_base, key_scale = jax.random.split(jax.random.fold_in(key, 11))
    normal_part = jnp.clip(jax.random.normal(key_base, (SEQS, LEN, MODEL), jnp.float32), -4.0, 4.0)
    block_scale = jnp.exp(jax.random.uniform(key_scale, (SEQS, LEN // SPAN, 1, 1), jnp.float32, math.log(0.5), math.log(2.0)))
    shaped = normal_part.reshape(SEQS, LEN // SPAN, SPAN, MODEL) * block_scale
    return shaped.reshape(SEQS, LEN, MODEL).astype(jnp.bfloat16)


def draw_channel_fading_exponent(key, part):
    key_order, key_slow, key_fast = jax.random.split(jax.random.fold_in(key, 23), 3)
    ranking = jax.random.permutation(key_order, HEADS)
    slow_rate = jax.random.uniform(key_slow, (HEADS,), jnp.float32, 0.3, 1.5) / LEN
    fast_rate = jnp.exp(jax.random.uniform(key_fast, (HEADS,), jnp.float32, math.log(0.015), math.log(0.05)))
    fast_count = HEADS // 2
    chosen = jnp.where(ranking < fast_count, fast_rate, slow_rate)
    return jnp.log(chosen).astype(jnp.float32)


def draw_extra_damping_spikes(key, part):
    key_place, key_depth = jax.random.split(jax.random.fold_in(key, 37))
    places = jax.random.randint(key_place, (SEQS, 4), 0, LEN)
    depths = jnp.log(1.0 - jax.random.uniform(key_depth, (SEQS, 4), jnp.float32, 0.2, 0.5))
    positions = jnp.arange(LEN, dtype=jnp.int32)
    matches = (positions[None, None, :] == places[:, :, None]).astype(jnp.float32)
    summed = jnp.sum(matches * depths[:, :, None], axis=1)
    return jnp.broadcast_to(summed[:, None, :], (SEQS, HEADS, LEN)).astype(jnp.float32)


def block_levels(rng, dims, cuts, smallest, top_value):
    loudness = 1.0
    for dim, blocks in cuts:
        draws = jax.random.uniform(jax.random.fold_in(jax.random.fold_in(rng, 6), dim), (blocks,), jnp.float32, smallest / len(cuts), top_value / len(cuts))
        loudness = loudness * jnp.repeat(jnp.exp(draws), dims[dim] // blocks).reshape((-1,) + (1,) * (len(dims) - 1 - dim))
    return loudness


def normal_values(own_key, dims, scale, reach, pieces=(), kind=jnp.bfloat16):
    values = scale * jax.random.normal(own_key, dims, jnp.float32)
    if pieces:
        values = values * block_levels(own_key, dims, pieces, -0.22, 0.18)
    return jnp.clip(values, -reach, reach).astype(kind)


def setup_inputs(seed: int = 0, part: int = 0) -> dict:
    arg_keys = jax.random.split(jax.random.key(seed), 13)
    own_keys = jax.random.split(jax.random.fold_in(arg_keys[12], part), 13)
    return {
        "context_input_tensor": draw_context_input_tensor(jax.random.fold_in(jax.random.fold_in(arg_keys[12], part), 71), part),
        "content_mapping_matrix": normal_values(arg_keys[1], (MODEL, HEADS * HEAD), MODEL ** -0.5, 0.125),
        "address_mapping_matrix": normal_values(arg_keys[2], (MODEL, GROUPS * STATE), MODEL ** -0.5, 0.125),
        "increment_mapping_matrix": normal_values(arg_keys[3], (MODEL, HEADS), MODEL ** -0.5, 0.125),
        "increment_speed_offset": jnp.clip(-1.0 + 1.5 * jax.random.uniform(arg_keys[4], (HEADS,), jnp.float32) ** block_levels(arg_keys[4], (HEADS,), ((0, 8),), -0.2, 0.2), -1.0, 0.5),
        "channel_fading_exponent": draw_channel_fading_exponent(jax.random.fold_in(arg_keys[12], 71), part),
        "extra_damping_spikes": draw_extra_damping_spikes(jax.random.fold_in(jax.random.fold_in(arg_keys[12], part), 71), part),
        "content_smoothing_coefficients": normal_values(arg_keys[7], (KERNEL, HEADS, HEAD), KERNEL ** -0.5, 2.5, ((1, 8),), jnp.float32),
        "address_smoothing_coefficients": normal_values(arg_keys[8], (KERNEL, GROUPS, STATE), KERNEL ** -0.5, 2.5, (), jnp.float32),
        "newest_lookup_matrix": normal_values(own_keys[9], (SEQS, GROUPS, STATE), 1.0, 6.0, ((0, 2),)),
        "newest_output_switch": normal_values(own_keys[10], (SEQS, HEADS, HEAD), 1.0, 6.0, ((0, 2), (1, 8))),
        "cluster_scaling_coefficients": jnp.clip(1.0 + 0.18 * jax.random.normal(arg_keys[11], (HEADS, HEAD), jnp.float32), 0.1, 1.9),
    }


EPS = 1e-05

def centred(signal, kernel):
    margin = kernel.shape[0] // 2
    length = signal.shape[0]
    padded = jnp.pad(signal, ((margin, margin), (0, 0), (0, 0)))
    summed = kernel[0] * padded[0:length]
    for offset in range(1, kernel.shape[0]):
        summed = summed + kernel[offset] * padded[offset:offset + length]
    return summed

def reference(context_input_tensor, content_mapping_matrix, address_mapping_matrix, increment_mapping_matrix, increment_speed_offset, channel_fading_exponent, extra_damping_spikes, content_smoothing_coefficients, address_smoothing_coefficients, newest_lookup_matrix, newest_output_switch, cluster_scaling_coefficients):
    repeats = HEADS // GROUPS

    def lone_context_series(packed_buffer):
        prompt_token_rows, arrival_token_rows, query_vector_row, gate_vector_row = packed_buffer
        value_proj = jnp.dot(prompt_token_rows, content_mapping_matrix, preferred_element_type=jnp.float32).astype(jnp.bfloat16).reshape(LEN, HEADS, HEAD)
        key_proj = jnp.dot(prompt_token_rows, address_mapping_matrix, preferred_element_type=jnp.float32).astype(jnp.bfloat16).reshape(LEN, GROUPS, STATE)
        rate_raw = jnp.dot(prompt_token_rows, increment_mapping_matrix, preferred_element_type=jnp.float32).astype(jnp.bfloat16)
        value_conv = jax.nn.silu(centred(value_proj.astype(jnp.float32), content_smoothing_coefficients)).astype(jnp.bfloat16)
        key_conv = jax.nn.silu(centred(key_proj.astype(jnp.float32), address_smoothing_coefficients)).astype(jnp.bfloat16)
        key_heads = jnp.repeat(key_conv, repeats, axis=1)
        smoothed_increment_speed = jax.nn.softplus(rate_raw.astype(jnp.float32) + increment_speed_offset)
        exponent_increment_amount = -jnp.exp(channel_fading_exponent) * smoothed_increment_speed + arrival_token_rows.T
        cumul = jnp.cumsum(exponent_increment_amount, axis=0)
        end_weight = jnp.exp(cumul[-1] - cumul)
        weighted = (value_conv.astype(jnp.float32) * (smoothed_increment_speed * end_weight)[:, :, None]).astype(jnp.bfloat16)
        states = jnp.einsum('lhp,lhn->hpn', weighted.astype(jnp.float32), key_heads.astype(jnp.float32))
        query_heads = jnp.repeat(query_vector_row.astype(jnp.float32), repeats, axis=0)
        raw_read = jnp.einsum('hpn,hn->hp', states, query_heads, precision=lax.Precision.HIGHEST)
        gated_read = raw_read * jax.nn.silu(gate_vector_row.astype(jnp.float32))
        head_sq = lax.optimization_barrier(jnp.sum(gated_read * gated_read, axis=1))
        group_sq = jnp.repeat(lax.optimization_barrier(jnp.sum(head_sq.reshape(GROUPS, repeats), axis=1)), repeats)
        scaled = gated_read * lax.rsqrt(group_sq / (repeats * HEAD) + EPS)[:, None] * cluster_scaling_coefficients
        kv_rows = jnp.concatenate([value_conv, key_heads], axis=-1)
        return (kv_rows, scaled.astype(jnp.bfloat16))
    address_content_store, earliest_switched_retrieval = lax.map(lone_context_series, (context_input_tensor, extra_damping_spikes, newest_lookup_matrix, newest_output_switch))
    return (address_content_store, earliest_switched_retrieval)
```

```python
import jax
import jax.numpy as jnp
from jax import lax
from jax.experimental import pallas as pl
from jax.experimental.pallas import tpu as pltpu
from jax.sharding import PartitionSpec as P

HEADS = 16
HEAD = 64
GROUPS = 4
STATE = 64
LANES = 128
EXTRA = 16
EPS = 1e-05
F32 = jnp.float32
BF16 = jnp.bfloat16


def silu(x):
    return 0.5 * x * (1.0 + jnp.tanh(0.5 * x))


def rounded(x):
    return x.astype(BF16).astype(F32)


def lane_index(shape):
    return lax.broadcasted_iota(jnp.int32, shape, 1)


def whole(shape):
    return pl.BlockSpec(shape, lambda *_: (0,) * len(shape))


def flip_permute(value, flip):
    pairs = [(source, source ^ flip) for source in range(lax.axis_size("sp"))]
    return lax.ppermute(value, "sp", pairs)


def key_block_kernel(group_devices, low_ref, high_ref, wk_ref, wr_ref, *rest):
    outs, (packed, rates) = rest[:-2], rest[-2:]
    repeats = HEADS // GROUPS
    step = pl.program_id(0)
    rows = low_ref.shape[0]
    tiles = rows // LANES
    half_tiles = rates.shape[0] // 2
    wk, wr = wk_ref[...], wr_ref[...]
    low, high = low_ref[...], high_ref[...]
    k_low = rounded(jnp.dot(low, wk, preferred_element_type=F32))
    k_high = rounded(jnp.dot(high, wk, preferred_element_type=F32))
    left = lane_index((rows, LANES)) < STATE
    for group in range(GROUPS):
        column = slice(group // 2 * LANES, (group // 2 + 1) * LANES)
        a, b = k_low[:, column], k_high[:, column]
        if group % 2 == 0:
            b = pltpu.roll(b, STATE, 1)
        else:
            a = pltpu.roll(a, STATE, 1)
        packed[group, pl.ds(pl.multiple_of(step * rows, rows), rows), :] = jnp.where(left, a, b).astype(BF16)
    eye = (
        lax.broadcasted_iota(jnp.int32, (HEADS, HEADS), 0) == lax.broadcasted_iota(jnp.int32, (HEADS, HEADS), 1)
    ).astype(BF16)
    for part, x in ((0, low), (1, high)):
        r = jnp.dot(x, wr, preferred_element_type=F32).astype(BF16)
        turned = lax.dot_general(eye, r, (((1,), (1,)), ((), ())), preferred_element_type=F32)
        for tile in range(tiles):
            rates[part * half_tiles + step * tiles + tile] = turned[:, tile * LANES : (tile + 1) * LANES]

    @pl.when(step == pl.num_programs(0) - 1)
    def _():
        half = packed.shape[1] - 2 * half_tiles * repeats
        for group in range(GROUPS):
            tail = jnp.concatenate(
                [rates[tile, group * repeats : (group + 1) * repeats, :] for tile in range(2 * half_tiles)], axis=0
            )
            packed[group, half:, :] = tail.astype(BF16)
        own = lax.axis_index("sp") // group_devices
        for offset, out in enumerate(outs):
            out[...] = packed[own ^ offset]


def key_blocks(rows, wk, wr, group_devices):
    span, model = rows.shape
    repeats = HEADS // GROUPS
    half = span // 2
    tile = half // 2
    steps = half // tile
    height = half + repeats * span // LANES
    block = jax.ShapeDtypeStruct((height, LANES), BF16)
    return pl.pallas_call(
        lambda *refs: key_block_kernel(group_devices, *refs),
        grid=(steps,),
        in_specs=[
            pl.BlockSpec((tile, model), lambda i: (i, 0)),
            pl.BlockSpec((tile, model), lambda i: (i + steps, 0)),
            whole(wk.shape),
            whole(wr.shape),
        ],
        out_specs=[whole((height, LANES))] * GROUPS,
        out_shape=[block] * GROUPS,
        scratch_shapes=[
            pltpu.VMEM((GROUPS, height, LANES), BF16),
            pltpu.VMEM((span // LANES, HEADS, LANES), F32),
        ],
        cost_estimate=pl.CostEstimate(
            flops=2 * span * model * (GROUPS * STATE + HEADS), bytes_accessed=2 * span * model, transcendentals=0
        ),
        name="key_blocks",
    )(rows, rows, wk, wr)


def value_block_kernel(cut, x_ref, w_ref, _, early, *rest):
    late, kept = rest[:-1], rest[-1]
    step = pl.program_id(0)
    share = kept.shape[2]
    devices = w_ref.shape[1] // share
    span = x_ref.shape[0]
    y = jnp.dot(x_ref[...], w_ref[...], preferred_element_type=F32)
    first_extra = jnp.concatenate([y[cut : cut + 8], y[span - 8 : span]], axis=0)
    last_extra = jnp.concatenate([y[cut - 8 : cut], y[cut - 8 : cut]], axis=0)
    for device in range(devices):
        lanes = slice(device * share, (device + 1) * share)
        early[device, :cut, :] = y[:cut, lanes].astype(BF16)
        early[device, cut:, :] = first_extra[:, lanes].astype(BF16)
        index = step * devices + device
        kept[index, : span - cut, :] = y[cut:, lanes].astype(BF16)
        kept[index, span - cut :, :] = last_extra[:, lanes].astype(BF16)

    @pl.when(step == pl.num_programs(0) - 1)
    def _():
        own = lax.axis_index("sp")
        for offset, out in enumerate(late):
            out[...] = kept[own ^ offset]


def value_blocks(rows, wv, started, devices, cut):
    span, model = rows.shape
    width = wv.shape[1]
    share = width // devices
    tile = max(2 * LANES, share)
    per_step = tile // share
    late_rows = span - cut + EXTRA
    late = jax.ShapeDtypeStruct((late_rows, share), BF16)
    out = pl.pallas_call(
        lambda *refs: value_block_kernel(cut, *refs),
        grid=(width // tile,),
        in_specs=[
            whole((span, model)),
            pl.BlockSpec((model, tile), lambda i: (0, i)),
            pl.BlockSpec(memory_space=pl.ANY),
        ],
        out_specs=[pl.BlockSpec((per_step, cut + EXTRA, share), lambda i: (i, 0, 0))]
        + [whole((late_rows, share))] * devices,
        out_shape=[jax.ShapeDtypeStruct((devices, cut + EXTRA, share), BF16)] + [late] * devices,
        scratch_shapes=[pltpu.VMEM((devices, late_rows, share), BF16)],
        cost_estimate=pl.CostEstimate(
            flops=2 * span * model * width, bytes_accessed=2 * (span * model + model * width), transcendentals=0
        ),
        name="value_blocks",
    )(rows, wv, started)
    return out[0], out[1:]


def key_read_kernel(
    group_devices, own_ref, *refs
):
    flips = GROUPS - 1
    direct, relayed = refs[:flips], refs[flips : flips + group_devices - 1]
    taps_ref, query_ref, offset_ref, decay_ref, spikes_ref, keys_ref, weight_ref, blocks, line, rates, scores = refs[
        flips + group_devices - 1 :
    ]
    repeats = HEADS // GROUPS
    sources = blocks.shape[0]
    half = keys_ref.shape[1] // 2
    heads = spikes_ref.shape[0]
    tiles = 2 * half // LANES
    me = lax.axis_index("sp")
    group, rank = me // group_devices, me % group_devices
    for offset in range(GROUPS):
        block = own_ref[...] if offset == 0 else direct[offset - 1][...]
        blocks[(group ^ offset) * group_devices + rank] = block
        for shift in range(1, group_devices):
            blocks[(group ^ offset) * group_devices + (rank ^ shift)] = relayed[shift - 1][offset]
    taps = [taps_ref[k : k + 1, :] for k in range(5)]
    query = query_ref[...]
    edge_left = lane_index((16, LANES)) < STATE
    left = lane_index((half, LANES)) < STATE
    picked = lax.broadcasted_iota(jnp.int32, (heads * tiles, repeats * tiles), 0)
    column = lax.broadcasted_iota(jnp.int32, (heads * tiles, repeats * tiles), 1)
    select = (column == (picked % tiles) * repeats + rank * heads + picked // tiles).astype(BF16)

    def one_source(source, carry):
        body = blocks[source, :half, :].astype(F32)
        before = blocks[jnp.maximum(source - 1, 0), half - 16 : half, :].astype(F32)
        after = blocks[jnp.minimum(source + 1, sources - 1), :16, :].astype(F32)
        before = jnp.where(source > 0, before, 0.0)
        after = jnp.where(source < sources - 1, after, 0.0)
        top = jnp.where(edge_left, pltpu.roll(before, STATE, 1), pltpu.roll(body[half - 16 :], STATE, 1))
        bottom = jnp.where(edge_left, pltpu.roll(body[:16], STATE, 1), pltpu.roll(after, STATE, 1))
        line[0:16, :] = top
        line[16 : 16 + half, :] = body
        line[16 + half :, :] = bottom
        total = taps[0] * line[14 : 14 + half, :]
        for k in range(1, 5):
            total = total + taps[k] * line[14 + k : 14 + k + half, :]
        y = silu(total).astype(BF16)
        score = lax.dot_general(query, y, (((1,), (1,)), ((), ())), preferred_element_type=F32)
        scores[source] = jnp.concatenate(
            [score[part : part + 1, c * LANES : (c + 1) * LANES] for part in range(2) for c in range(tiles // 2)],
            axis=0,
        )
        z = y.astype(F32)
        turned = pltpu.roll(z, STATE, 1)
        keys_ref[source, :half, :] = jnp.where(left, z, turned).astype(BF16)
        keys_ref[source, half:, :] = jnp.where(left, turned, z).astype(BF16)
        chosen = jnp.dot(select, blocks[source, half:, :], preferred_element_type=F32)
        for h in range(heads):
            rates[h, source] = chosen[h * tiles : (h + 1) * tiles]
        return carry

    lax.fori_loop(0, sources, one_source, 0)
    count = sources * tiles
    lane_row = lax.broadcasted_iota(jnp.int32, (LANES, LANES), 0)
    lane_col = lax.broadcasted_iota(jnp.int32, (LANES, LANES), 1)
    later_lanes = (lane_row > lane_col).astype(F32)
    row = lax.broadcasted_iota(jnp.int32, (count, count), 0)
    col = lax.broadcasted_iota(jnp.int32, (count, count), 1)
    later_rows = (col > row).astype(F32)
    score = scores[...].reshape(count, LANES)
    exact = dict(preferred_element_type=F32, precision=lax.Precision.HIGHEST)
    for h in range(heads):
        raw = rates[h].reshape(count, LANES) + offset_ref[h]
        rate = jnp.maximum(raw, 0.0) + jnp.log1p(jnp.exp(-jnp.abs(raw)))
        decay = jnp.exp(jnp.full((1, LANES), decay_ref[h], F32))
        step = spikes_ref[h] - decay * rate
        within = jnp.dot(step, later_lanes, **exact)
        totals = jnp.broadcast_to(jnp.sum(step, axis=1, keepdims=True), (count, LANES))
        ahead = within + jnp.dot(later_rows, totals, **exact)
        weight = rate * jnp.exp(ahead) * score
        high = rounded(weight)
        weight_ref[:, h] = high.reshape(sources, tiles, LANES)
        weight_ref[:, heads + h] = (weight - high).reshape(sources, tiles, LANES)


def key_read(own, direct, relayed, taps, query, offset, decay, spikes, group_devices, span):
    sources = group_devices * GROUPS
    heads = offset.shape[0]
    half = span // 2
    tiles = span // LANES
    smem = pl.BlockSpec(memory_space=pltpu.SMEM)
    vmem = pl.BlockSpec(memory_space=pltpu.VMEM)
    count = 1 + len(direct) + len(relayed)
    return pl.pallas_call(
        lambda *refs: key_read_kernel(group_devices, *refs),
        in_specs=[vmem] * (count + 2) + [smem, smem, vmem],
        out_specs=[vmem, vmem],
        out_shape=[
            jax.ShapeDtypeStruct((sources, span, LANES), BF16),
            jax.ShapeDtypeStruct((sources, 2 * heads, tiles, LANES), F32),
        ],
        scratch_shapes=[
            pltpu.VMEM((sources,) + own.shape, BF16),
            pltpu.VMEM((half + 32, LANES), F32),
            pltpu.VMEM((heads, sources, tiles, LANES), F32),
            pltpu.VMEM((sources, tiles, LANES), F32),
        ],
        cost_estimate=pl.CostEstimate(flops=10**9, bytes_accessed=4 * 10**6, transcendentals=10**6),
        name="key_read",
    )(own, *direct, *relayed, taps, query, offset, decay, spikes)


def convolved(line, body, before, after, taps, keys_ref, weight_ref, spread, out_ref, total, first_tile):
    rows, share = body.shape
    heads = share // HEAD
    line[0:8, :] = before
    line[8 : 8 + rows, :] = body
    line[8 + rows :, :] = after
    lanes = lane_index((LANES, LANES))
    weight = weight_ref[0].reshape(-1, LANES)
    tiles = weight_ref.shape[2]
    tile_of = lax.broadcasted_iota(jnp.int32, weight.shape, 0) % tiles
    for tile in range(rows // LANES):
        start = tile * LANES
        y = taps[0] * line[6 + start : 6 + start + LANES, :]
        for k in range(1, 5):
            y = y + taps[k] * line[6 + k + start : 6 + k + start + LANES, :]
        y = silu(y).astype(BF16)
        keys = keys_ref[0, start : start + LANES, :].astype(F32)
        z = y.astype(F32)
        if share == LANES:
            pieces = [jnp.where(lanes < HEAD, z, keys), jnp.where(lanes < HEAD, pltpu.roll(z, HEAD, 1), keys)]
        else:
            pieces = [
                jnp.concatenate([z[:, h * HEAD : (h + 1) * HEAD], keys[:, STATE:]], axis=1) for h in range(heads)
            ]
        stacked = jnp.concatenate(pieces, axis=0).astype(BF16)
        if heads > 1:
            stacked = jnp.dot(spread, stacked, preferred_element_type=F32).astype(BF16)
        out_ref[0, heads * start : heads * (start + LANES), :] = stacked
        masked = jnp.where(tile_of == first_tile + tile, weight, 0.0).astype(BF16)
        total[...] += jnp.dot(masked, y, preferred_element_type=F32)


def spread_matrix(heads):
    size = heads * LANES
    row = lax.broadcasted_iota(jnp.int32, (size, size), 0)
    col = lax.broadcasted_iota(jnp.int32, (size, size), 1)
    return (col == (row % heads) * LANES + row // heads).astype(BF16)


def early_kernel(cut, block_ref, previous_ref, keys_ref, weight_ref, taps_ref, out_ref, read_ref, line, total, spread):
    source = pl.program_id(0)
    heads = block_ref.shape[2] // HEAD

    @pl.when(source == 0)
    def _():
        total[...] = jnp.zeros_like(total)
        spread[...] = spread_matrix(heads)

    taps = [taps_ref[k : k + 1, :] for k in range(5)]
    block = block_ref[0].astype(F32)
    before = jnp.where(source > 0, previous_ref[0].astype(F32)[8:16], 0.0)
    convolved(
        line, block[:cut], before, block[cut : cut + 8], taps, keys_ref, weight_ref, spread[...], out_ref, total, 0
    )
    read_ref[...] = total[...]


def early_rows(blocks, keys, weight, taps, cut):
    sources, height, share = blocks.shape
    span = keys.shape[1]
    heads = share // HEAD
    rows = weight.shape[1] * weight.shape[2]
    return pl.pallas_call(
        lambda *refs: early_kernel(cut, *refs),
        grid=(sources,),
        in_specs=[
            pl.BlockSpec((1, height, share), lambda s: (s, 0, 0)),
            pl.BlockSpec((1, EXTRA, share), lambda s: (jnp.maximum(s - 1, 0), cut // EXTRA, 0)),
            pl.BlockSpec((1, cut, LANES), lambda s: (s, 0, 0)),
            pl.BlockSpec((1,) + weight.shape[1:], lambda s: (s, 0, 0, 0)),
            whole(taps.shape),
        ],
        out_specs=[pl.BlockSpec((1, heads * cut, LANES), lambda s: (s, 0, 0)), whole((rows, share))],
        out_shape=[
            jax.ShapeDtypeStruct((sources, heads * span, LANES), BF16),
            jax.ShapeDtypeStruct((rows, share), F32),
        ],
        scratch_shapes=[
            pltpu.VMEM((cut + 16, share), F32),
            pltpu.VMEM((rows, share), F32),
            pltpu.VMEM((heads * LANES, heads * LANES), BF16),
        ],
        cost_estimate=pl.CostEstimate(flops=2 * 10**9, bytes_accessed=6 * 10**6, transcendentals=10**6),
        name="early_rows",
    )(blocks, blocks, keys, weight, taps)


def late_kernel(cut, *refs):
    sources = pl.num_programs(0)
    count = len(refs) - 13
    blocks = refs[:count]
    following_ref, keys_ref, weight_ref, taps_ref, gate_ref, read_ref, _, out_ref, gated_ref, line, total, spread, kept = refs[
        count:
    ]
    source = pl.program_id(0)
    share = line.shape[1]
    heads = share // HEAD

    @pl.when(source == 0)
    def _():
        total[...] = read_ref[...]
        spread[...] = spread_matrix(heads)
        own = lax.axis_index("sp")
        for offset in range(count):
            kept[own ^ offset] = blocks[offset][...]

    taps = [taps_ref[k : k + 1, :] for k in range(5)]
    block = kept[source].astype(F32)
    rows = block.shape[0] - EXTRA
    after = jnp.where(source < sources - 1, following_ref[0].astype(F32)[:8], 0.0)
    convolved(
        line,
        block[:rows],
        block[rows : rows + 8],
        after,
        taps,
        keys_ref,
        weight_ref,
        spread[...],
        out_ref,
        total,
        cut // LANES,
    )

    @pl.when(source == sources - 1)
    def _():
        tiles = weight_ref.shape[2]
        shape = total.shape
        head = (lax.broadcasted_iota(jnp.int32, shape, 0) // tiles) % heads
        mine = head == lane_index(shape) // HEAD
        read = jnp.sum(jnp.where(mine, total[...], 0.0), axis=0, keepdims=True)
        gated_ref[...] = read * silu(gate_ref[...])


def late_rows(late, early, keys, weight, taps, gate, read, out, cut):
    sources = len(late)
    height, share = late[0].shape
    span = keys.shape[1]
    rows = span - cut
    heads = share // HEAD
    step = cut // rows
    return pl.pallas_call(
        lambda *refs: late_kernel(cut, *refs),
        grid=(sources,),
        in_specs=[whole((height, share))] * sources
        + [
            pl.BlockSpec((1, EXTRA, share), lambda s: (jnp.minimum(s + 1, sources - 1), 0, 0)),
            pl.BlockSpec((1, rows, LANES), lambda s: (s, step, 0)),
            pl.BlockSpec((1,) + weight.shape[1:], lambda s: (s, 0, 0, 0)),
            whole(taps.shape),
            whole(gate.shape),
            whole(read.shape),
            pl.BlockSpec(memory_space=pl.ANY),
        ],
        out_specs=[pl.BlockSpec((1, heads * rows, LANES), lambda s: (s, step, 0)), whole((8, share))],
        out_shape=[jax.ShapeDtypeStruct(out.shape, BF16), jax.ShapeDtypeStruct((8, share), F32)],
        scratch_shapes=[
            pltpu.VMEM((rows + 16, share), F32),
            pltpu.VMEM(read.shape, F32),
            pltpu.VMEM((heads * LANES, heads * LANES), BF16),
            pltpu.VMEM((sources, height, share), BF16),
        ],
        input_output_aliases={sources + 6: 0},
        cost_estimate=pl.CostEstimate(flops=10**9, bytes_accessed=2 * 10**6, transcendentals=10**6),
        name="late_rows",
    )(*late, early, keys, weight, taps, gate, read, out)


def on_device(
    context_input_tensor,
    content_mapping_matrix,
    address_mapping_matrix,
    increment_mapping_matrix,
    increment_speed_offset,
    channel_fading_exponent,
    extra_damping_spikes,
    content_smoothing_coefficients,
    address_smoothing_coefficients,
    newest_lookup_matrix,
    newest_output_switch,
    cluster_scaling_coefficients,
):
    rows = context_input_tensor[0]
    span = rows.shape[0]
    repeats = HEADS // GROUPS
    heads = increment_speed_offset.shape[0]
    share = heads * HEAD
    group_devices = repeats // heads
    devices = lax.axis_size("sp")
    group = lax.axis_index("sp") // group_devices
    cut = span // 4 * 3

    blocks = key_blocks(rows, address_mapping_matrix, increment_mapping_matrix, group_devices)
    direct = [None] * (GROUPS - 1)
    for offset in reversed(range(1, GROUPS)):
        direct[offset - 1] = flip_permute(blocks[offset], offset * group_devices)
    early, late = value_blocks(rows, content_mapping_matrix, blocks[0], devices, cut)
    early_blocks = lax.all_to_all(early, "sp", 0, 0, tiled=True)
    held = jnp.stack([blocks[0]] + direct)
    relayed = [flip_permute(held, shift) for shift in range(1, group_devices)]
    late_blocks = [None] * devices
    late_blocks[0] = late[0]
    for offset in reversed(range(1, devices)):
        late_blocks[offset] = flip_permute(late[offset], offset)

    key_taps = lax.dynamic_slice_in_dim(address_smoothing_coefficients, group, 1, 1)[:, 0]
    key_taps = jnp.pad(jnp.concatenate([key_taps, key_taps], axis=1), ((0, 3), (0, 0)))
    value_taps = jnp.pad(content_smoothing_coefficients.reshape(-1, share), ((0, 3), (0, 0)))
    query = lax.dynamic_slice_in_dim(newest_lookup_matrix[0], group, 1, 0)
    blank = jnp.zeros_like(query)
    query_rows = jnp.concatenate(
        [jnp.concatenate([query, blank], axis=1), jnp.concatenate([blank, query], axis=1)], axis=0
    )
    query_rows = jnp.pad(query_rows, ((0, 14), (0, 0)))
    spikes = extra_damping_spikes[0].reshape(heads, -1, LANES)
    gate = jnp.broadcast_to(newest_output_switch[0].astype(F32).reshape(1, share), (8, share))

    keys, weight = key_read(
        blocks[0],
        direct,
        relayed,
        key_taps,
        query_rows,
        increment_speed_offset,
        channel_fading_exponent,
        spikes,
        group_devices,
        span,
    )
    out, read = early_rows(early_blocks, keys, weight, value_taps, cut)
    out, gated = late_rows(late_blocks, early_blocks, keys, weight, value_taps, gate, read, out, cut)
    gated = gated[0]
    group_sq = jnp.sum(gated * gated).reshape(1)
    for level in range(group_devices.bit_length() - 1):
        group_sq = group_sq + flip_permute(group_sq, 2**level)
    scaled = gated * lax.rsqrt(group_sq[0] / (repeats * HEAD) + EPS) * cluster_scaling_coefficients.reshape(share)
    store = out.reshape(1, devices * span, heads, HEAD + STATE)
    return store, scaled.astype(BF16).reshape(1, heads, HEAD)


def solution(mesh):
    placed = (
        P(("gr", "tp"), "sp", None),
        P(),
        P(),
        P(),
        P("sp"),
        P("sp"),
        P(("gr", "tp"), "sp", None),
        P(None, "sp", None),
        P(),
        P(("gr", "tp"), None, None),
        P(("gr", "tp"), "sp", None),
        P("sp", None),
    )
    return jax.shard_map(
        on_device,
        mesh=mesh,
        in_specs=placed,
        out_specs=(P(("gr", "tp"), None, "sp", None), P(("gr", "tp"), "sp", None)),
        check_vma=False,
    )
```

```python
import jax
import jax.numpy as jnp
from jax import lax
from jax.experimental import pallas as pl
from jax.experimental.pallas import tpu as pltpu
from jax.sharding import PartitionSpec as P


HEADS = 16
HEAD = 64
GROUPS = 4
STATE = 64
LANES = 128
EXTRA = 16
VMEM_LIMIT = 24 * 2**20
EPS = 1e-05
F32 = jnp.float32
BF16 = jnp.bfloat16


def silu(x):
    return 0.5 * x * (1.0 + jnp.tanh(0.5 * x))


def rounded(x):
    return x.astype(BF16).astype(F32)


def lane_index(shape):
    return lax.broadcasted_iota(jnp.int32, shape, 1)


def whole(shape):
    return pl.BlockSpec(shape, lambda *_: (0,) * len(shape))


def on_chip(x):
    return pltpu.with_memory_space_constraint(x, pltpu.VMEM)


def off_chip(x):
    return pltpu.with_memory_space_constraint(x, pltpu.HBM)


def flip_permute(value, flip):
    pairs = [(source, source ^ flip) for source in range(lax.axis_size("sp"))]
    return lax.ppermute(value, "sp", pairs)


def key_block_kernel(group_devices, low_ref, high_ref, wk_ref, wr_ref, *rest):
    outs, (packed, rates) = rest[:-2], rest[-2:]
    repeats = HEADS // GROUPS
    step = pl.program_id(0)
    rows = low_ref.shape[0]
    tiles = rows // LANES
    half_tiles = rates.shape[0] // 2
    wk, wr = wk_ref[...], wr_ref[...]
    both = jnp.concatenate([low_ref[...], high_ref[...]], axis=0)
    k_both = rounded(jnp.dot(both, wk, preferred_element_type=F32))
    k_low, k_high = k_both[:rows], k_both[rows:]
    r_both = lax.dot_general(both, wr, (((1,), (1,)), ((), ())), preferred_element_type=F32).astype(BF16)
    left = lane_index((rows, LANES)) < STATE
    for group in range(GROUPS):
        column = slice(group // 2 * LANES, (group // 2 + 1) * LANES)
        a, b = k_low[:, column], k_high[:, column]
        if group % 2 == 0:
            b = pltpu.roll(b, STATE, 1)
        else:
            a = pltpu.roll(a, STATE, 1)
        packed[group, pl.ds(pl.multiple_of(step * rows, rows), rows), :] = jnp.where(left, a, b).astype(BF16)
    eye = (
        lax.broadcasted_iota(jnp.int32, (HEADS, HEADS), 0) == lax.broadcasted_iota(jnp.int32, (HEADS, HEADS), 1)
    ).astype(BF16)
    for part in range(2):
        r = r_both[part * rows : (part + 1) * rows]
        turned = lax.dot_general(eye, r, (((1,), (1,)), ((), ())), preferred_element_type=F32)
        for tile in range(tiles):
            rates[part * half_tiles + step * tiles + tile] = turned[:, tile * LANES : (tile + 1) * LANES]

    @pl.when(step == pl.num_programs(0) - 1)
    def _():
        half = packed.shape[1] - 2 * half_tiles * repeats
        for group in range(GROUPS):
            tail = jnp.concatenate(
                [rates[tile, group * repeats : (group + 1) * repeats, :] for tile in range(2 * half_tiles)], axis=0
            )
            packed[group, half:, :] = tail.astype(BF16)
        own = lax.axis_index("sp") // group_devices
        for offset, out in enumerate(outs):
            out[...] = packed[own ^ offset]


def key_blocks(rows, wk, wr, group_devices):
    span, model = rows.shape
    repeats = HEADS // GROUPS
    half = span // 2
    tile = half // 2
    steps = half // tile
    height = half + repeats * span // LANES
    block = jax.ShapeDtypeStruct((height, LANES), BF16)
    return pl.pallas_call(
        lambda *refs: key_block_kernel(group_devices, *refs),
        grid=(steps,),
        in_specs=[
            pl.BlockSpec((tile, model), lambda i: (i, 0)),
            pl.BlockSpec((tile, model), lambda i: (i + steps, 0)),
            whole(wk.shape),
            whole(wr.shape),
        ],
        out_specs=[whole((height, LANES))] * GROUPS,
        out_shape=[block] * GROUPS,
        scratch_shapes=[
            pltpu.VMEM((GROUPS, height, LANES), BF16),
            pltpu.VMEM((span // LANES, HEADS, LANES), F32),
        ],
        compiler_params=pltpu.CompilerParams(vmem_limit_bytes=VMEM_LIMIT),
        cost_estimate=pl.CostEstimate(
            flops=2 * span * model * (GROUPS * STATE + HEADS), bytes_accessed=2 * span * model, transcendentals=0
        ),
        name="key_blocks",
    )(off_chip(rows), off_chip(rows), off_chip(wk), wr)


def early_values_kernel(x_ref, after_ref, last_ref, w_ref, _, out_ref):
    rows = x_ref.shape[0]
    share = out_ref.shape[2]
    x = jnp.concatenate([x_ref[...], after_ref[...], last_ref[...]], axis=0)
    y = jnp.dot(x, w_ref[...], preferred_element_type=F32)
    extra = jnp.concatenate([y[rows : rows + 8], y[rows + 24 : rows + 32]], axis=0)
    for device in range(out_ref.shape[0]):
        lanes = slice(device * share, (device + 1) * share)
        out_ref[device, :rows, :] = y[:rows, lanes].astype(BF16)
        out_ref[device, rows:, :] = extra[:, lanes].astype(BF16)


def early_values(rows, wv, started, devices, cut):
    span, model = rows.shape
    width = wv.shape[1]
    share = width // devices
    tile = max(2 * LANES, share)
    return pl.pallas_call(
        early_values_kernel,
        grid=(width // tile,),
        in_specs=[
            whole((cut, model)),
            pl.BlockSpec((EXTRA, model), lambda i: (cut // EXTRA, 0)),
            pl.BlockSpec((EXTRA, model), lambda i: (span // EXTRA - 1, 0)),
            pl.BlockSpec((model, tile), lambda i: (0, i)),
            pl.BlockSpec(memory_space=pl.ANY),
        ],
        out_specs=pl.BlockSpec((tile // share, cut + EXTRA, share), lambda i: (i, 0, 0)),
        out_shape=jax.ShapeDtypeStruct((devices, cut + EXTRA, share), BF16),
        compiler_params=pltpu.CompilerParams(vmem_limit_bytes=VMEM_LIMIT),
        cost_estimate=pl.CostEstimate(
            flops=2 * cut * model * width, bytes_accessed=2 * (cut * model + model * width), transcendentals=0
        ),
        name="early_values",
    )(off_chip(rows), off_chip(rows), off_chip(rows), off_chip(wv), started)


def late_values_kernel(x_ref, before_ref, w_ref, _, *rest):
    outs, kept = rest[:-1], rest[-1]
    step = pl.program_id(0)
    share = kept.shape[2]
    devices = w_ref.shape[1] // share
    x = jnp.concatenate([x_ref[...], before_ref[...]], axis=0)
    y = jnp.dot(x, w_ref[...], preferred_element_type=F32)
    for device in range(devices):
        lanes = slice(device * share, (device + 1) * share)
        kept[step * devices + device] = y[:, lanes].astype(BF16)

    @pl.when(step == pl.num_programs(0) - 1)
    def _():
        own = lax.axis_index("sp")
        for offset, out in enumerate(outs):
            out[...] = kept[own ^ offset]


def late_values(rows, wv, started, devices, cut):
    span, model = rows.shape
    width = wv.shape[1]
    share = width // devices
    tile = max(2 * LANES, share)
    late = span - cut
    block = (late + EXTRA, share)
    return pl.pallas_call(
        late_values_kernel,
        grid=(width // tile,),
        in_specs=[
            pl.BlockSpec((late, model), lambda i: (cut // late, 0)),
            pl.BlockSpec((EXTRA, model), lambda i: (cut // EXTRA - 1, 0)),
            pl.BlockSpec((model, tile), lambda i: (0, i)),
            pl.BlockSpec(memory_space=pl.ANY),
        ],
        out_specs=[whole(block)] * devices,
        out_shape=[jax.ShapeDtypeStruct(block, BF16)] * devices,
        scratch_shapes=[pltpu.VMEM((devices,) + block, BF16)],
        compiler_params=pltpu.CompilerParams(vmem_limit_bytes=VMEM_LIMIT),
        cost_estimate=pl.CostEstimate(
            flops=2 * late * model * width, bytes_accessed=2 * (late * model + model * width), transcendentals=0
        ),
        name="late_values",
    )(off_chip(rows), off_chip(rows), off_chip(wv), started)


def key_read_kernel(
    group_devices, own_ref, *refs
):
    flips = GROUPS - 1
    direct, relayed = refs[:flips], refs[flips : flips + group_devices - 1]
    (
        taps_ref,
        query_ref,
        offset_ref,
        decay_ref,
        spikes_ref,
        keys_ref,
        weight_ref,
        blocks,
        line,
        rates,
        scores,
        spikes,
    ) = refs[flips + group_devices - 1 :]
    repeats = HEADS // GROUPS
    sources = blocks.shape[0]
    half = keys_ref.shape[1] // 2
    heads = spikes_ref.shape[1]
    tiles = 2 * half // LANES
    me = lax.axis_index("sp")
    group, rank = me // group_devices, me % group_devices
    for offset in range(GROUPS):
        block = own_ref[...] if offset == 0 else direct[offset - 1][...]
        blocks[(group ^ offset) * group_devices + rank] = block
        for shift in range(1, group_devices):
            blocks[(group ^ offset) * group_devices + (rank ^ shift)] = relayed[shift - 1][offset]
    taps = []
    for k in range(5):
        tap = taps_ref[k, pl.ds(group, 1), :]
        taps.append(jnp.concatenate([tap, tap], axis=1))
    asked = query_ref[0].astype(F32)
    asked = jnp.where(lax.broadcasted_iota(jnp.int32, asked.shape, 0) == group, asked, 0.0)
    asked = jnp.sum(asked, axis=0, keepdims=True)
    asked = jnp.broadcast_to(jnp.concatenate([asked, asked], axis=1), (16, LANES))
    part_row = lax.broadcasted_iota(jnp.int32, (16, LANES), 0)
    query = jnp.where(part_row == lane_index((16, LANES)) // STATE, asked, 0.0).astype(BF16)
    edge_left = lane_index((16, LANES)) < STATE
    left = lane_index((half, LANES)) < STATE
    picked = lax.broadcasted_iota(jnp.int32, (heads * tiles, repeats * tiles), 0)
    column = lax.broadcasted_iota(jnp.int32, (heads * tiles, repeats * tiles), 1)
    select = (column == (picked % tiles) * repeats + rank * heads + picked // tiles).astype(BF16)

    def one_source(source, carry):
        body = blocks[source, :half, :].astype(F32)
        before = blocks[jnp.maximum(source - 1, 0), half - 16 : half, :].astype(F32)
        after = blocks[jnp.minimum(source + 1, sources - 1), :16, :].astype(F32)
        before = jnp.where(source > 0, before, 0.0)
        after = jnp.where(source < sources - 1, after, 0.0)
        top = jnp.where(edge_left, pltpu.roll(before, STATE, 1), pltpu.roll(body[half - 16 :], STATE, 1))
        bottom = jnp.where(edge_left, pltpu.roll(body[:16], STATE, 1), pltpu.roll(after, STATE, 1))
        line[0:16, :] = top
        line[16 : 16 + half, :] = body
        line[16 + half :, :] = bottom
        total = taps[0] * line[14 : 14 + half, :]
        for k in range(1, 5):
            total = total + taps[k] * line[14 + k : 14 + k + half, :]
        y = silu(total).astype(BF16)
        score = lax.dot_general(query, y, (((1,), (1,)), ((), ())), preferred_element_type=F32)
        scores[source] = jnp.concatenate(
            [score[part : part + 1, c * LANES : (c + 1) * LANES] for part in range(2) for c in range(tiles // 2)],
            axis=0,
        )
        z = y.astype(F32)
        turned = pltpu.roll(z, STATE, 1)
        keys_ref[source, :half, :] = jnp.where(left, z, turned).astype(BF16)
        keys_ref[source, half:, :] = jnp.where(left, turned, z).astype(BF16)
        chosen = jnp.dot(select, blocks[source, half:, :], preferred_element_type=F32)
        for h in range(heads):
            rates[h, source] = chosen[h * tiles : (h + 1) * tiles]
        return carry

    lax.fori_loop(0, sources, one_source, 0)
    count = sources * tiles
    lane_row = lax.broadcasted_iota(jnp.int32, (LANES, LANES), 0)
    lane_col = lax.broadcasted_iota(jnp.int32, (LANES, LANES), 1)
    later_lanes = (lane_row > lane_col).astype(F32)
    row = lax.broadcasted_iota(jnp.int32, (count, count), 0)
    col = lax.broadcasted_iota(jnp.int32, (count, count), 1)
    later_rows = (col > row).astype(F32)
    score = scores[...].reshape(count, LANES)
    for h in range(heads):
        for c in range(count):
            spikes[h, c : c + 1, :] = spikes_ref[0, h : h + 1, c * LANES : (c + 1) * LANES]
    exact = dict(preferred_element_type=F32, precision=lax.Precision.HIGHEST)
    for h in range(heads):
        raw = rates[h].reshape(count, LANES) + offset_ref[h]
        rate = jnp.maximum(raw, 0.0) + jnp.log1p(jnp.exp(-jnp.abs(raw)))
        decay = jnp.exp(jnp.full((1, LANES), decay_ref[h], F32))
        step = spikes[h] - decay * rate
        within = jnp.dot(step, later_lanes, **exact)
        totals = jnp.broadcast_to(jnp.sum(step, axis=1, keepdims=True), (count, LANES))
        ahead = within + jnp.dot(later_rows, totals, **exact)
        weight = rate * jnp.exp(ahead) * score
        high = rounded(weight)
        weight_ref[:, h] = high.reshape(sources, tiles, LANES)
        weight_ref[:, heads + h] = (weight - high).reshape(sources, tiles, LANES)


def key_read(own, direct, relayed, taps, query, offset, decay, spikes, group_devices, span):
    sources = group_devices * GROUPS
    heads = offset.shape[0]
    half = span // 2
    tiles = span // LANES
    smem = pl.BlockSpec(memory_space=pltpu.SMEM)
    vmem = pl.BlockSpec(memory_space=pltpu.VMEM)
    count = 1 + len(direct) + len(relayed)
    return pl.pallas_call(
        lambda *refs: key_read_kernel(group_devices, *refs),
        in_specs=[vmem] * (count + 2) + [smem, smem, vmem],
        out_specs=[vmem, vmem],
        out_shape=[
            jax.ShapeDtypeStruct((sources, span, LANES), BF16),
            jax.ShapeDtypeStruct((sources, 2 * heads, tiles, LANES), F32),
        ],
        scratch_shapes=[
            pltpu.VMEM((sources,) + own.shape, BF16),
            pltpu.VMEM((half + 32, LANES), F32),
            pltpu.VMEM((heads, sources, tiles, LANES), F32),
            pltpu.VMEM((sources, tiles, LANES), F32),
            pltpu.VMEM((heads, sources * tiles, LANES), F32),
        ],
        compiler_params=pltpu.CompilerParams(vmem_limit_bytes=VMEM_LIMIT),
        cost_estimate=pl.CostEstimate(flops=10**9, bytes_accessed=4 * 10**6, transcendentals=10**6),
        name="key_read",
    )(*(on_chip(x) for x in [own, *direct, *relayed, taps, query]), offset, decay, on_chip(spikes))


def convolved(line, woven, body, before, after, taps_ref, keys_ref, weight_ref, source, start_row, out_ref, total):
    rows, share = body.shape
    heads = share // HEAD
    line[0:8, :] = before
    line[8 : 8 + rows, :] = body
    line[8 + rows :, :] = after
    taps = [jnp.concatenate([taps_ref[k, h : h + 1, :] for h in range(heads)], axis=1) for k in range(5)]
    left = lane_index((LANES, LANES)) < HEAD
    tiles = weight_ref.shape[2]
    weight = weight_ref[source].reshape(-1, LANES)
    tile_of = lax.broadcasted_iota(jnp.int32, weight.shape, 0) % tiles
    read = jnp.zeros(total.shape, F32)
    for tile in range(rows // LANES):
        start = tile * LANES
        y = taps[0] * line[6 + start : 6 + start + LANES, :]
        for k in range(1, 5):
            y = y + taps[k] * line[6 + k + start : 6 + k + start + LANES, :]
        y = silu(y).astype(BF16)
        keys = keys_ref[0, start : start + LANES, :].astype(F32)
        z = y.astype(F32)
        if share == LANES:
            pieces = [jnp.where(left, z, keys), jnp.where(left, pltpu.roll(z, HEAD, 1), keys)]
        else:
            pieces = [
                jnp.concatenate([z[:, h * HEAD : (h + 1) * HEAD], keys[:, STATE:]], axis=1) for h in range(heads)
            ]
        for h, piece in enumerate(pieces):
            woven[pl.ds(heads * start + h, LANES, heads), :] = piece
        masked = jnp.where(tile_of == start_row // LANES + tile, weight, 0.0).astype(BF16)
        read = read + jnp.dot(masked, y, preferred_element_type=F32)
        part = slice(heads * start, heads * (start + LANES))
        out_ref[0, part, :] = woven[part, :].astype(BF16)
    total[...] += read


def scratch_for(rows, share, reads):
    return [
        pltpu.VMEM((rows + 16, share), F32),
        pltpu.VMEM((share // HEAD * rows, LANES), F32),
        pltpu.VMEM((reads, share), F32),
    ]


def early_kernel(cut, block_ref, keys_ref, weight_ref, taps_ref, out_ref, read_ref, line, woven, total):
    source = pl.program_id(0)

    @pl.when(source == 0)
    def _():
        total[...] = jnp.zeros_like(total)

    block = block_ref[source].astype(F32)
    before = block_ref[jnp.maximum(source - 1, 0), cut : cut + EXTRA, :].astype(F32)[8:]
    before = jnp.where(source > 0, before, 0.0)
    convolved(
        line,
        woven,
        block[:cut],
        before,
        block[cut : cut + 8],
        taps_ref,
        keys_ref,
        weight_ref,
        source,
        0,
        out_ref,
        total,
    )
    read_ref[...] = total[...]


def early_rows(blocks, keys, weight, taps, cut):
    sources, _, share = blocks.shape
    span = keys.shape[1]
    heads = share // HEAD
    reads = weight.shape[1] * weight.shape[2]
    vmem = pl.BlockSpec(memory_space=pltpu.VMEM)
    return pl.pallas_call(
        lambda *refs: early_kernel(cut, *refs),
        grid=(sources,),
        in_specs=[vmem, pl.BlockSpec((1, cut, LANES), lambda s: (s, 0, 0)), vmem, vmem],
        out_specs=[pl.BlockSpec((1, heads * cut, LANES), lambda s: (s, 0, 0)), whole((reads, share))],
        out_shape=[
            jax.ShapeDtypeStruct((sources, heads * span, LANES), BF16),
            jax.ShapeDtypeStruct((reads, share), F32),
        ],
        scratch_shapes=scratch_for(cut, share, reads),
        compiler_params=pltpu.CompilerParams(vmem_limit_bytes=VMEM_LIMIT),
        cost_estimate=pl.CostEstimate(flops=2 * 10**9, bytes_accessed=6 * 10**6, transcendentals=10**6),
        name="early_rows",
    )(on_chip(blocks), keys, on_chip(weight), on_chip(taps))


def late_kernel(cut, last, order_ref, *refs):
    count = pl.num_programs(0)
    others = 13 if last else 11
    blocks, refs = refs[:-others], refs[-others:]
    early_ref, keys_ref, weight_ref, taps_ref, read_ref = refs[:5]
    gate_ref = refs[5] if last else None
    refs = refs[6 if last else 5 :]
    out_ref, read_out = refs[1], refs[2]
    square_ref = refs[3] if last else None
    line, woven, total = refs[-3:]
    step = pl.program_id(0)
    sources = early_ref.shape[0]
    rows, share = line.shape[0] - 16, line.shape[1]
    heads = share // HEAD

    @pl.when(step == 0)
    def _():
        total[...] = read_ref[...]

    for index, block_ref in enumerate(blocks):

        @pl.when(step == index)
        def _(block_ref=block_ref):
            source = order_ref[index]
            block = block_ref[...].astype(F32)
            after = early_ref[jnp.minimum(source + 1, sources - 1), :16, :].astype(F32)[:8]
            after = jnp.where(source < sources - 1, after, 0.0)
            convolved(
                line,
                woven,
                block[:rows],
                block[rows + 8 :],
                after,
                taps_ref,
                keys_ref,
                weight_ref,
                source,
                cut,
                out_ref,
                total,
            )

    @pl.when(step == count - 1)
    def _():
        if not last:
            read_out[...] = total[...]
            return
        tiles = weight_ref.shape[2]
        shape = total.shape
        head = (lax.broadcasted_iota(jnp.int32, shape, 0) // tiles) % heads
        mine = head == lane_index(shape) // HEAD
        read = jnp.sum(jnp.where(mine, total[...], 0.0), axis=0, keepdims=True)
        read = jnp.concatenate([read[:, h * HEAD : (h + 1) * HEAD] for h in range(heads)], axis=0)
        gated = read * silu(gate_ref[0].astype(F32))
        read_out[...] = gated
        square = jnp.sum(jnp.sum(gated * gated, axis=1, keepdims=True), axis=0, keepdims=True)
        square_ref[...] = jnp.broadcast_to(square, square_ref.shape)


def late_rows(offsets, late, early, keys, weight, taps, read, gate, out, cut, last):
    height, share = late[0].shape
    rows = height - EXTRA
    heads = share // HEAD
    place = cut // rows
    vmem = pl.BlockSpec(memory_space=pltpu.VMEM)
    near = [on_chip(x) for x in [late[k] for k in offsets] + [early]]
    far = [on_chip(x) for x in [weight, taps, read] + ([gate] if last else [])]
    inputs = near + [keys] + far
    order = lax.axis_index("sp") ^ jnp.array(offsets, jnp.int32)
    if last:
        small = [jax.ShapeDtypeStruct((heads, HEAD), F32), jax.ShapeDtypeStruct((1, LANES), F32)]
    else:
        small = [jax.ShapeDtypeStruct(read.shape, F32)]
    return pl.pallas_call(
        lambda *refs: late_kernel(cut, last, *refs),
        grid_spec=pltpu.PrefetchScalarGridSpec(
            num_scalar_prefetch=1,
            grid=(len(offsets),),
            in_specs=[vmem] * len(near)
            + [pl.BlockSpec((1, rows, LANES), lambda i, order: (order[i], place, 0))]
            + [vmem] * len(far)
            + [pl.BlockSpec(memory_space=pl.ANY)],
            out_specs=[pl.BlockSpec((1, heads * rows, LANES), lambda i, order: (order[i], place, 0))]
            + [whole(x.shape) for x in small],
            scratch_shapes=scratch_for(rows, share, read.shape[0]),
        ),
        out_shape=[jax.ShapeDtypeStruct(out.shape, BF16)] + small,
        input_output_aliases={len(inputs) + 1: 0},
        compiler_params=pltpu.CompilerParams(vmem_limit_bytes=VMEM_LIMIT),
        cost_estimate=pl.CostEstimate(flops=10**9, bytes_accessed=2 * 10**6, transcendentals=10**6),
        name="late_rows",
    )(order, *inputs, out)


def on_device(
    context_input_tensor,
    content_mapping_matrix,
    address_mapping_matrix,
    increment_mapping_matrix,
    increment_speed_offset,
    channel_fading_exponent,
    extra_damping_spikes,
    content_smoothing_coefficients,
    address_smoothing_coefficients,
    newest_lookup_matrix,
    newest_output_switch,
    cluster_scaling_coefficients,
):
    rows = context_input_tensor[0]
    span = rows.shape[0]
    repeats = HEADS // GROUPS
    heads = increment_speed_offset.shape[0]
    group_devices = repeats // heads
    devices = lax.axis_size("sp")
    cut = span // 2

    blocks = key_blocks(rows, address_mapping_matrix, increment_mapping_matrix.T, group_devices)
    direct = [None] * (GROUPS - 1)
    for offset in range(1, GROUPS):
        direct[offset - 1] = flip_permute(blocks[offset], offset * group_devices)
    early = early_values(rows, content_mapping_matrix, blocks[0], devices, cut)
    early_blocks = lax.all_to_all(early, "sp", 0, 0, tiled=True)
    late = late_values(rows, content_mapping_matrix, early, devices, cut)
    held = jnp.stack([blocks[0]] + direct)
    relayed = []
    for shift in range(1, group_devices):
        relayed.append(flip_permute(held, shift))
    late_blocks = [None] * devices
    late_blocks[0] = late[0]
    for offset in range(1, devices):
        late_blocks[offset] = flip_permute(late[offset], offset)

    keys, weight = key_read(
        blocks[0],
        direct,
        relayed,
        address_smoothing_coefficients,
        newest_lookup_matrix,
        increment_speed_offset,
        channel_fading_exponent,
        extra_damping_spikes,
        group_devices,
        span,
    )
    taps = content_smoothing_coefficients
    out, read = early_rows(early_blocks, keys, weight, taps, cut)
    half, quarter = devices // 2, devices // 4
    waves = (range(half), range(half + quarter, devices), range(half, half + quarter))
    for index, offsets in enumerate(waves):
        last = index == len(waves) - 1
        out, read, *square = late_rows(
            list(offsets), late_blocks, early_blocks, keys, weight, taps, read, newest_output_switch, out, cut, last
        )
    group_sq = square[0]
    for level in range(group_devices.bit_length() - 1):
        group_sq = group_sq + flip_permute(group_sq, 2**level)
    scaled = read * lax.rsqrt(group_sq[0, 0] / (repeats * HEAD) + EPS) * cluster_scaling_coefficients
    store = out.reshape(1, devices * span, heads, HEAD + STATE)
    return store, scaled.astype(BF16).reshape(1, heads, HEAD)


def solution(mesh):
    placed = (
        P(("gr", "tp"), "sp", None),
        P(),
        P(),
        P(),
        P("sp"),
        P("sp"),
        P(("gr", "tp"), "sp", None),
        P(None, "sp", None),
        P(),
        P(("gr", "tp"), None, None),
        P(("gr", "tp"), "sp", None),
        P("sp", None),
    )

    return jax.shard_map(
        on_device,
        mesh=mesh,
        in_specs=placed,
        out_specs=(P(("gr", "tp"), None, "sp", None), P(("gr", "tp"), "sp", None)),
        check_vma=False,
    )
```

```python
import jax
import jax.numpy as jnp
from jax import lax
from jax.experimental import pallas as pl
from jax.experimental.pallas import tpu as pltpu
from jax.sharding import PartitionSpec as P


HEADS = 16
HEAD = 64
GROUPS = 4
STATE = 64
LANES = 128
EXTRA = 8
TILE_ROWS = 16
VMEM_LIMIT = 24 * 2**20
EPS = 1e-05
F32 = jnp.float32
BF16 = jnp.bfloat16


def silu(x):
    return 0.5 * x * (1.0 + jnp.tanh(0.5 * x))


def rounded(x):
    return x.astype(BF16).astype(F32)


def lane_index(shape):
    return lax.broadcasted_iota(jnp.int32, shape, 1)


def whole(shape):
    return pl.BlockSpec(shape, lambda *_: (0,) * len(shape))


def on_chip(x):
    return pltpu.with_memory_space_constraint(x, pltpu.VMEM)


def off_chip(x):
    return pltpu.with_memory_space_constraint(x, pltpu.HBM)


def flip_permute(value, flip):
    pairs = [(source, source ^ flip) for source in range(lax.axis_size("sp"))]
    return lax.ppermute(value, "sp", pairs)


def key_block_kernel(group_devices, low_ref, high_ref, wk_ref, wr_ref, *rest):
    outs, (packed, rates) = rest[:-2], rest[-2:]
    repeats = HEADS // GROUPS
    step = pl.program_id(0)
    rows = low_ref.shape[0]
    tiles = rows // LANES
    half_tiles = rates.shape[0] // 2
    wk, wr = wk_ref[...], wr_ref[...]
    both = jnp.concatenate([low_ref[...], high_ref[...]], axis=0)
    k_both = rounded(jnp.dot(both, wk, preferred_element_type=F32))
    k_low, k_high = k_both[:rows], k_both[rows:]
    r_both = lax.dot_general(both, wr, (((1,), (1,)), ((), ())), preferred_element_type=F32).astype(BF16)
    left = lane_index((rows, LANES)) < STATE
    for group in range(GROUPS):
        column = slice(group // 2 * LANES, (group // 2 + 1) * LANES)
        a, b = k_low[:, column], k_high[:, column]
        if group % 2 == 0:
            b = pltpu.roll(b, STATE, 1)
        else:
            a = pltpu.roll(a, STATE, 1)
        packed[group, pl.ds(pl.multiple_of(step * rows, rows), rows), :] = jnp.where(left, a, b).astype(BF16)
    eye = (
        lax.broadcasted_iota(jnp.int32, (HEADS, HEADS), 0) == lax.broadcasted_iota(jnp.int32, (HEADS, HEADS), 1)
    ).astype(BF16)
    for part in range(2):
        r = r_both[part * rows : (part + 1) * rows]
        turned = lax.dot_general(eye, r, (((1,), (1,)), ((), ())), preferred_element_type=F32)
        for tile in range(tiles):
            rates[part * half_tiles + step * tiles + tile] = turned[:, tile * LANES : (tile + 1) * LANES]

    @pl.when(step == pl.num_programs(0) - 1)
    def _():
        half = packed.shape[1] - 2 * half_tiles * repeats
        for group in range(GROUPS):
            tail = jnp.concatenate(
                [rates[tile, group * repeats : (group + 1) * repeats, :] for tile in range(2 * half_tiles)], axis=0
            )
            packed[group, half:, :] = tail.astype(BF16)
        own = lax.axis_index("sp") // group_devices
        for offset, out in enumerate(outs):
            out[...] = packed[own ^ offset]


def key_blocks(rows, wk, wr, group_devices):
    span, model = rows.shape
    repeats = HEADS // GROUPS
    half = span // 2
    tile = half // 2
    steps = half // tile
    height = half + repeats * span // LANES
    block = jax.ShapeDtypeStruct((height, LANES), BF16)
    return pl.pallas_call(
        lambda *refs: key_block_kernel(group_devices, *refs),
        grid=(steps,),
        in_specs=[
            pl.BlockSpec((tile, model), lambda i: (i, 0)),
            pl.BlockSpec((tile, model), lambda i: (i + steps, 0)),
            whole(wk.shape),
            whole(wr.shape),
        ],
        out_specs=[whole((height, LANES))] * GROUPS,
        out_shape=[block] * GROUPS,
        scratch_shapes=[
            pltpu.VMEM((GROUPS, height, LANES), BF16),
            pltpu.VMEM((span // LANES, HEADS, LANES), F32),
        ],
        compiler_params=pltpu.CompilerParams(vmem_limit_bytes=VMEM_LIMIT),
        cost_estimate=pl.CostEstimate(
            flops=2 * span * model * (GROUPS * STATE + HEADS), bytes_accessed=2 * span * model, transcendentals=0
        ),
        name="key_blocks",
    )(off_chip(rows), off_chip(rows), off_chip(wk), off_chip(wr))


def value_kernel(x_refs, w_ref, outs, kept):
    step = pl.program_id(0)
    share = kept.shape[2]
    devices = w_ref.shape[1] // share
    rows = x_refs[0].shape[0]
    x = jnp.concatenate([ref[...] for ref in x_refs], axis=0) if len(x_refs) > 1 else x_refs[0][...]
    y = jnp.dot(x, w_ref[...], preferred_element_type=F32)
    for device in range(devices):
        lanes = slice(device * share, (device + 1) * share)
        index = step * devices + device
        kept[index, :rows, :] = y[:rows, lanes].astype(BF16)
        if len(x_refs) > 1:
            half = EXTRA // 2
            last = y.shape[0]
            extra = jnp.concatenate([y[rows : rows + half, lanes], y[last - half :, lanes]], axis=0)
            kept[index, rows:, :] = extra.astype(BF16)

    @pl.when(step == pl.num_programs(0) - 1)
    def _():
        own = lax.axis_index("sp")
        for offset, out in enumerate(outs):
            out[...] = kept[own ^ offset]


def value_blocks(rows, wv, started, devices, cut, early):
    span, model = rows.shape
    width = wv.shape[1]
    share = width // devices
    tile = max(2 * LANES, share)
    if early:
        specs = [
            whole((cut, model)),
            pl.BlockSpec((TILE_ROWS, model), lambda i: (cut // TILE_ROWS, 0)),
            pl.BlockSpec((TILE_ROWS, model), lambda i: (span // TILE_ROWS - 1, 0)),
        ]
        block = (cut + EXTRA, share)
    else:
        specs = [pl.BlockSpec((span - cut, model), lambda i: (cut // (span - cut), 0))]
        block = (span - cut, share)
    count = len(specs)

    def kernel(*refs):
        value_kernel(refs[:count], refs[count], refs[count + 2 : -1], refs[-1])

    return pl.pallas_call(
        kernel,
        grid=(width // tile,),
        in_specs=specs + [pl.BlockSpec((model, tile), lambda i: (0, i)), pl.BlockSpec(memory_space=pl.ANY)],
        out_specs=[whole(block)] * devices,
        out_shape=[jax.ShapeDtypeStruct(block, BF16)] * devices,
        scratch_shapes=[pltpu.VMEM((devices,) + block, BF16)],
        compiler_params=pltpu.CompilerParams(vmem_limit_bytes=VMEM_LIMIT),
        cost_estimate=pl.CostEstimate(
            flops=2 * block[0] * model * width,
            bytes_accessed=2 * (block[0] * model + model * width),
            transcendentals=0,
        ),
        name="early_values" if early else "late_values",
    )(*[off_chip(rows)] * count, off_chip(wv), started)


def key_read_kernel(
    group_devices, held_ref, *refs
):
    relayed = refs[: group_devices - 1]
    (
        taps_ref,
        query_ref,
        offset_ref,
        decay_ref,
        spikes_ref,
        keys_ref,
        weight_ref,
        blocks,
        line,
        rates,
        scores,
        spikes,
    ) = refs[group_devices - 1 :]
    repeats = HEADS // GROUPS
    sources = blocks.shape[0]
    half = keys_ref.shape[1] // 2
    heads = spikes_ref.shape[1]
    tiles = 2 * half // LANES
    me = lax.axis_index("sp")
    group, rank = me // group_devices, me % group_devices
    for offset in range(GROUPS):
        blocks[(group ^ offset) * group_devices + rank] = held_ref[offset]
        for shift in range(1, group_devices):
            blocks[(group ^ offset) * group_devices + (rank ^ shift)] = relayed[shift - 1][offset]
    taps = []
    for k in range(5):
        tap = taps_ref[k, pl.ds(group, 1), :]
        taps.append(jnp.concatenate([tap, tap], axis=1))
    asked = query_ref[0].astype(F32)
    asked = jnp.where(lax.broadcasted_iota(jnp.int32, asked.shape, 0) == group, asked, 0.0)
    asked = jnp.sum(asked, axis=0, keepdims=True)
    asked = jnp.broadcast_to(jnp.concatenate([asked, asked], axis=1), (16, LANES))
    part_row = lax.broadcasted_iota(jnp.int32, (16, LANES), 0)
    query = jnp.where(part_row == lane_index((16, LANES)) // STATE, asked, 0.0).astype(BF16)
    edge_left = lane_index((16, LANES)) < STATE
    left = lane_index((half, LANES)) < STATE
    picked = lax.broadcasted_iota(jnp.int32, (heads * tiles, repeats * tiles), 0)
    column = lax.broadcasted_iota(jnp.int32, (heads * tiles, repeats * tiles), 1)
    select = (column == (picked % tiles) * repeats + rank * heads + picked // tiles).astype(BF16)

    def one_source(source, carry):
        body = blocks[source, :half, :].astype(F32)
        before = blocks[jnp.maximum(source - 1, 0), half - 16 : half, :].astype(F32)
        after = blocks[jnp.minimum(source + 1, sources - 1), :16, :].astype(F32)
        before = jnp.where(source > 0, before, 0.0)
        after = jnp.where(source < sources - 1, after, 0.0)
        top = jnp.where(edge_left, pltpu.roll(before, STATE, 1), pltpu.roll(body[half - 16 :], STATE, 1))
        bottom = jnp.where(edge_left, pltpu.roll(body[:16], STATE, 1), pltpu.roll(after, STATE, 1))
        line[0:16, :] = top
        line[16 : 16 + half, :] = body
        line[16 + half :, :] = bottom
        total = taps[0] * line[14 : 14 + half, :]
        for k in range(1, 5):
            total = total + taps[k] * line[14 + k : 14 + k + half, :]
        y = silu(total).astype(BF16)
        score = lax.dot_general(query, y, (((1,), (1,)), ((), ())), preferred_element_type=F32)
        scores[source] = jnp.concatenate(
            [score[part : part + 1, c * LANES : (c + 1) * LANES] for part in range(2) for c in range(tiles // 2)],
            axis=0,
        )
        z = y.astype(F32)
        turned = pltpu.roll(z, STATE, 1)
        keys_ref[source, :half, :] = jnp.where(left, z, turned).astype(BF16)
        keys_ref[source, half:, :] = jnp.where(left, turned, z).astype(BF16)
        chosen = jnp.dot(select, blocks[source, half:, :], preferred_element_type=F32)
        for h in range(heads):
            rates[h, source] = chosen[h * tiles : (h + 1) * tiles]
        return carry

    lax.fori_loop(0, sources, one_source, 0)
    count = sources * tiles
    lane_row = lax.broadcasted_iota(jnp.int32, (LANES, LANES), 0)
    lane_col = lax.broadcasted_iota(jnp.int32, (LANES, LANES), 1)
    later_lanes = (lane_row > lane_col).astype(F32)
    row = lax.broadcasted_iota(jnp.int32, (count, count), 0)
    col = lax.broadcasted_iota(jnp.int32, (count, count), 1)
    later_rows = (col > row).astype(F32)
    score = scores[...].reshape(count, LANES)
    for h in range(heads):
        for c in range(count):
            spikes[h, c : c + 1, :] = spikes_ref[0, h : h + 1, c * LANES : (c + 1) * LANES]
    exact = dict(preferred_element_type=F32, precision=lax.Precision.HIGHEST)
    for h in range(heads):
        raw = rates[h].reshape(count, LANES) + offset_ref[h]
        rate = jnp.maximum(raw, 0.0) + jnp.log1p(jnp.exp(-jnp.abs(raw)))
        decay = jnp.exp(jnp.full((1, LANES), decay_ref[h], F32))
        step = spikes[h] - decay * rate
        within = jnp.dot(step, later_lanes, **exact)
        totals = jnp.broadcast_to(jnp.sum(step, axis=1, keepdims=True), (count, LANES))
        ahead = within + jnp.dot(later_rows, totals, **exact)
        weight = rate * jnp.exp(ahead) * score
        high = rounded(weight)
        weight_ref[:, h] = high.reshape(sources, tiles, LANES)
        weight_ref[:, heads + h] = (weight - high).reshape(sources, tiles, LANES)


def key_read(held, relayed, taps, query, offset, decay, spikes, group_devices, span):
    sources = group_devices * GROUPS
    heads = offset.shape[0]
    half = span // 2
    tiles = span // LANES
    smem = pl.BlockSpec(memory_space=pltpu.SMEM)
    vmem = pl.BlockSpec(memory_space=pltpu.VMEM)
    count = 1 + len(relayed)
    return pl.pallas_call(
        lambda *refs: key_read_kernel(group_devices, *refs),
        in_specs=[vmem] * (count + 2) + [smem, smem, vmem],
        out_specs=[vmem, vmem],
        out_shape=[
            jax.ShapeDtypeStruct((sources, span, LANES), BF16),
            jax.ShapeDtypeStruct((sources, 2 * heads, tiles, LANES), F32),
        ],
        scratch_shapes=[
            pltpu.VMEM((sources,) + held.shape[1:], BF16),
            pltpu.VMEM((half + 32, LANES), F32),
            pltpu.VMEM((heads, sources, tiles, LANES), F32),
            pltpu.VMEM((sources, tiles, LANES), F32),
            pltpu.VMEM((heads, sources * tiles, LANES), F32),
        ],
        compiler_params=pltpu.CompilerParams(vmem_limit_bytes=VMEM_LIMIT),
        cost_estimate=pl.CostEstimate(flops=10**9, bytes_accessed=4 * 10**6, transcendentals=10**6),
        name="key_read",
    )(*(on_chip(x) for x in [held, *relayed, taps, query]), offset, decay, on_chip(spikes))


def convolved(line, body, before, after, taps_ref, weight_ref, source, start_row, total):
    rows, share = body.shape
    heads = share // HEAD
    line[0:8, :] = before
    line[8 : 8 + rows, :] = body
    line[8 + rows :, :] = after
    taps = [jnp.concatenate([taps_ref[k, h : h + 1, :] for h in range(heads)], axis=1) for k in range(5)]
    tiles = weight_ref.shape[2]
    weight = weight_ref[source].reshape(-1, LANES)
    tile_of = lax.broadcasted_iota(jnp.int32, weight.shape, 0) % tiles
    read = jnp.zeros(total.shape, F32)
    values = []
    for tile in range(rows // LANES):
        start = tile * LANES
        y = taps[0] * line[6 + start : 6 + start + LANES, :]
        for k in range(1, 5):
            y = y + taps[k] * line[6 + k + start : 6 + k + start + LANES, :]
        y = silu(y).astype(BF16)
        masked = jnp.where(tile_of == start_row // LANES + tile, weight, 0.0).astype(BF16)
        read = read + jnp.dot(masked, y, preferred_element_type=F32)
        values.append(y)
    total[...] += read
    return values


def wove(woven, values, keys_ref, source, start_row, out_ref):
    share = values[0].shape[1]
    heads = share // HEAD
    left = lane_index((LANES, LANES)) < HEAD
    for tile, y in enumerate(values):
        start = tile * LANES
        keys = keys_ref[source, start_row + start : start_row + start + LANES, :].astype(F32)
        z = y.astype(F32)
        if share == LANES:
            pieces = [jnp.where(left, z, keys), jnp.where(left, pltpu.roll(z, HEAD, 1), keys)]
        else:
            pieces = [
                jnp.concatenate([z[:, h * HEAD : (h + 1) * HEAD], keys[:, STATE:]], axis=1) for h in range(heads)
            ]
        for h, piece in enumerate(pieces):
            woven[pl.ds(heads * start + h, LANES, heads), :] = piece
        part = slice(heads * start, heads * (start + LANES))
        out_ref[0, part, :] = woven[part, :].astype(BF16)


def line_scratch(rows, share):
    return pltpu.VMEM((rows + 16, share), F32)


def woven_scratch(rows, share):
    return pltpu.VMEM((share // HEAD * rows, LANES), F32)


def early_kernel(cut, *refs):
    blocks = refs[:-10]
    keys_ref, weight_ref, taps_ref, out_ref, read_ref, edges_ref, kept, line, woven, total = refs[-10:]
    source = pl.program_id(0)
    own = lax.axis_index("sp")

    @pl.when(source == 0)
    def _():
        total[...] = jnp.zeros_like(total)
        for offset, block_ref in enumerate(blocks):
            kept[own ^ offset] = block_ref[...]
            edges_ref[own ^ offset, :TILE_ROWS, :] = block_ref[:TILE_ROWS, :]
            edges_ref[own ^ offset, TILE_ROWS:, :] = block_ref[cut - TILE_ROWS : cut, :]

    block = kept[source].astype(F32)
    before = kept[jnp.maximum(source - 1, 0), cut:, :].astype(F32)
    before = jnp.where(source > 0, before, 0.0)
    values = convolved(line, block[:cut], before, block[cut:], taps_ref, weight_ref, source, 0, total)
    wove(woven, values, keys_ref, source, 0, out_ref)
    read_ref[...] = total[...]


def early_rows(blocks, keys, weight, taps, cut):
    sources, span = keys.shape[:2]
    height, share = blocks[0].shape
    heads = share // HEAD
    reads = weight.shape[1] * weight.shape[2]
    edges = (sources, 2 * TILE_ROWS, share)
    vmem = pl.BlockSpec(memory_space=pltpu.VMEM)
    inputs = [*blocks, keys, weight, taps]
    return pl.pallas_call(
        lambda *refs: early_kernel(cut, *refs),
        grid=(sources,),
        in_specs=[vmem] * len(inputs),
        out_specs=[
            pl.BlockSpec((1, heads * cut, LANES), lambda s: (s, 0, 0)),
            whole((reads, share)),
            whole(edges),
        ],
        out_shape=[
            jax.ShapeDtypeStruct((sources, heads * span, LANES), BF16),
            jax.ShapeDtypeStruct((reads, share), F32),
            jax.ShapeDtypeStruct(edges, BF16),
        ],
        scratch_shapes=[
            pltpu.VMEM((sources, height, share), BF16),
            line_scratch(cut, share),
            woven_scratch(cut, share),
            pltpu.VMEM((reads, share), F32),
        ],
        compiler_params=pltpu.CompilerParams(vmem_limit_bytes=VMEM_LIMIT),
        cost_estimate=pl.CostEstimate(flops=2 * 10**9, bytes_accessed=6 * 10**6, transcendentals=10**6),
        name="early_rows",
    )(*(on_chip(x) for x in inputs))


def late_values_of(offset, block_ref, edges_ref, taps_ref, weight_ref, line, total, cut):
    source = lax.axis_index("sp") ^ offset
    sources = edges_ref.shape[0]
    before = edges_ref[source, TILE_ROWS:, :].astype(F32)[TILE_ROWS - 8 :]
    after = edges_ref[jnp.minimum(source + 1, sources - 1), :TILE_ROWS, :].astype(F32)[:8]
    after = jnp.where(source < sources - 1, after, 0.0)
    body = block_ref[...].astype(F32)
    return convolved(line, body, before, after, taps_ref, weight_ref, source, cut, total)


def late_kernel(cut, offsets, *refs):
    count = len(offsets)
    blocks = refs[:count]
    edges_ref, keys_ref, weight_ref, taps_ref, read_ref, _, out_ref, total, line, woven = refs[count:]
    step = pl.program_id(0)

    @pl.when(step == 0)
    def _():
        total[...] = read_ref[...]

    for index, offset in enumerate(offsets):

        @pl.when(step == index)
        def _(index=index, offset=offset):
            values = late_values_of(offset, blocks[index], edges_ref, taps_ref, weight_ref, line, total, cut)
            wove(woven, values, keys_ref, lax.axis_index("sp") ^ offset, cut, out_ref)


def wave_offset(step, offsets):
    offset = step + offsets[0]
    for index in range(1, len(offsets)):
        gap = offsets[index] - offsets[index - 1] - 1
        if gap:
            offset = offset + gap * (step >= index).astype(jnp.int32)
    return offset


def late_out_spec(offsets, shape):
    rows = shape[1] // 2
    return pl.BlockSpec((1, rows, LANES), lambda i: (lax.axis_index("sp") ^ wave_offset(i, offsets), 1, 0))


def late_rows(offsets, late, edges, keys, weight, taps, read, out, cut):
    rows, share = late[0].shape
    vmem = pl.BlockSpec(memory_space=pltpu.VMEM)
    inputs = [late[k] for k in offsets] + [edges, keys, weight, taps, read]
    return pl.pallas_call(
        lambda *refs: late_kernel(cut, offsets, *refs),
        grid=(len(offsets),),
        in_specs=[vmem] * len(inputs) + [pl.BlockSpec(memory_space=pl.ANY)],
        out_specs=[late_out_spec(offsets, out.shape), whole(read.shape)],
        out_shape=[jax.ShapeDtypeStruct(out.shape, BF16), jax.ShapeDtypeStruct(read.shape, F32)],
        scratch_shapes=[line_scratch(rows, share), woven_scratch(rows, share)],
        input_output_aliases={len(inputs): 0},
        compiler_params=pltpu.CompilerParams(vmem_limit_bytes=VMEM_LIMIT),
        cost_estimate=pl.CostEstimate(flops=10**9, bytes_accessed=2 * 10**6, transcendentals=10**6),
        name="late_rows",
    )(*(on_chip(x) for x in inputs), out)


def last_read_kernel(cut, offsets, *refs):
    count = len(offsets)
    blocks = refs[:count]
    edges_ref, weight_ref, taps_ref, read_ref, gate_ref, values_ref, gated_ref, square_ref, line, total = refs[count:]
    total[...] = read_ref[...]
    for index, offset in enumerate(offsets):
        part = line.at[index]
        values = late_values_of(offset, blocks[index], edges_ref, taps_ref, weight_ref, part, total, cut)
        for tile, y in enumerate(values):
            values_ref[index, tile * LANES : (tile + 1) * LANES, :] = y
    tiles = weight_ref.shape[2]
    shape = total.shape
    heads = shape[1] // HEAD
    head = (lax.broadcasted_iota(jnp.int32, shape, 0) // tiles) % heads
    mine = head == lane_index(shape) // HEAD
    read = jnp.sum(jnp.where(mine, total[...], 0.0), axis=0, keepdims=True)
    read = jnp.concatenate([read[:, h * HEAD : (h + 1) * HEAD] for h in range(heads)], axis=0)
    gated = read * silu(gate_ref[0].astype(F32))
    gated_ref[...] = gated
    square = jnp.sum(jnp.sum(gated * gated, axis=1, keepdims=True), axis=0, keepdims=True)
    square_ref[...] = jnp.broadcast_to(square, square_ref.shape)


def last_read(offsets, late, edges, weight, taps, read, gate, cut):
    rows, share = late[0].shape
    vmem = pl.BlockSpec(memory_space=pltpu.VMEM)
    inputs = [late[k] for k in offsets] + [edges, weight, taps, read, gate]
    return pl.pallas_call(
        lambda *refs: last_read_kernel(cut, offsets, *refs),
        in_specs=[vmem] * len(inputs),
        out_specs=[vmem] * 3,
        out_shape=[
            jax.ShapeDtypeStruct((len(offsets), rows, share), BF16),
            jax.ShapeDtypeStruct((share // HEAD, HEAD), F32),
            jax.ShapeDtypeStruct((1, LANES), F32),
        ],
        scratch_shapes=[pltpu.VMEM((len(offsets), rows + 16, share), F32), pltpu.VMEM(read.shape, F32)],
        compiler_params=pltpu.CompilerParams(vmem_limit_bytes=VMEM_LIMIT),
        cost_estimate=pl.CostEstimate(flops=10**9, bytes_accessed=10**6, transcendentals=10**6),
        name="last_read",
    )(*(on_chip(x) for x in inputs))


def last_rows_kernel(cut, offsets, values_ref, keys_ref, _, out_ref, woven):
    step = pl.program_id(0)
    rows = values_ref.shape[1]
    values = [values_ref[step, start : start + LANES, :] for start in range(0, rows, LANES)]
    wove(woven, values, keys_ref, lax.axis_index("sp") ^ wave_offset(step, offsets), cut, out_ref)


def last_rows(offsets, values, keys, out, cut):
    rows, share = values.shape[1:]
    vmem = pl.BlockSpec(memory_space=pltpu.VMEM)
    return pl.pallas_call(
        lambda *refs: last_rows_kernel(cut, offsets, *refs),
        grid=(len(offsets),),
        in_specs=[vmem, vmem, pl.BlockSpec(memory_space=pl.ANY)],
        out_specs=late_out_spec(offsets, out.shape),
        out_shape=jax.ShapeDtypeStruct(out.shape, BF16),
        scratch_shapes=[woven_scratch(rows, share)],
        input_output_aliases={2: 0},
        compiler_params=pltpu.CompilerParams(vmem_limit_bytes=VMEM_LIMIT),
        cost_estimate=pl.CostEstimate(flops=10**9, bytes_accessed=2 * 10**6, transcendentals=0),
        name="last_rows",
    )(on_chip(values), on_chip(keys), out)


def on_device(
    context_input_tensor,
    content_mapping_matrix,
    address_mapping_matrix,
    increment_mapping_matrix,
    increment_speed_offset,
    channel_fading_exponent,
    extra_damping_spikes,
    content_smoothing_coefficients,
    address_smoothing_coefficients,
    newest_lookup_matrix,
    newest_output_switch,
    cluster_scaling_coefficients,
):
    rows = context_input_tensor[0]
    span = rows.shape[0]
    repeats = HEADS // GROUPS
    heads = increment_speed_offset.shape[0]
    group_devices = repeats // heads
    devices = lax.axis_size("sp")
    cut = span // 2

    blocks = key_blocks(rows, address_mapping_matrix, increment_mapping_matrix.T, group_devices)
    direct = [None] * (GROUPS - 1)
    for offset in range(1, GROUPS):
        direct[offset - 1] = flip_permute(blocks[offset], offset * group_devices)
    early = value_blocks(rows, content_mapping_matrix, blocks[0], devices, cut, True)
    late = value_blocks(rows, content_mapping_matrix, early[0], devices, cut, False)
    held = jnp.stack([blocks[0]] + direct)
    relayed = []
    for shift in range(1, group_devices):
        relayed.append(flip_permute(held, shift))
    early_blocks, late_blocks = [early[0]], [late[0]]
    for offset in range(1, devices):
        early_blocks.append(flip_permute(early[offset], offset))
        late_blocks.append(flip_permute(late[offset], offset))

    keys, weight = key_read(
        held,
        relayed,
        address_smoothing_coefficients,
        newest_lookup_matrix,
        increment_speed_offset,
        channel_fading_exponent,
        extra_damping_spikes,
        group_devices,
        span,
    )
    taps = content_smoothing_coefficients
    out, read, edges = early_rows(early_blocks, keys, weight, taps, cut)
    across = [offset for offset in range(devices) if offset % group_devices]
    along = [offset for offset in range(devices) if offset % group_devices == 0]
    near = [offset for offset in across if offset < devices // 2]
    final = [offset for offset in across if offset >= devices // 2]
    for wave in (along, near):
        out, read = late_rows(wave, late_blocks, edges, keys, weight, taps, read, out, cut)
    values, gated, group_sq = last_read(final, late_blocks, edges, weight, taps, read, newest_output_switch, cut)
    for level in range(group_devices.bit_length() - 1):
        group_sq = group_sq + flip_permute(group_sq, 2**level)
    out = last_rows(final, values, keys, out, cut)
    scaled = gated * lax.rsqrt(group_sq[0, 0] / (repeats * HEAD) + EPS) * cluster_scaling_coefficients
    store = out.reshape(1, devices * span, heads, HEAD + STATE)
    return store, scaled.astype(BF16).reshape(1, heads, HEAD)


def solution(mesh):
    placed = (
        P(("gr", "tp"), "sp", None),
        P(),
        P(),
        P(),
        P("sp"),
        P("sp"),
        P(("gr", "tp"), "sp", None),
        P(None, "sp", None),
        P(),
        P(("gr", "tp"), None, None),
        P(("gr", "tp"), "sp", None),
        P("sp", None),
    )

    return jax.shard_map(
        on_device,
        mesh=mesh,
        in_specs=placed,
        out_specs=(P(("gr", "tp"), None, "sp", None), P(("gr", "tp"), "sp", None)),
        check_vma=False,
    )
```

```python
import jax
import jax.numpy as jnp
from jax import lax
from jax.experimental import pallas as pl
from jax.experimental.pallas import tpu as pltpu
from jax.sharding import PartitionSpec as P


HEADS = 16
HEAD = 64
GROUPS = 4
STATE = 64
LANES = 128
EXTRA = 8
TILE_ROWS = 16
VMEM_LIMIT = 24 * 2**20
EPS = 1e-05
F32 = jnp.float32
BF16 = jnp.bfloat16


def silu(x):
    return 0.5 * x * (1.0 + jnp.tanh(0.5 * x))


def rounded(x):
    return x.astype(BF16).astype(F32)


def lane_index(shape):
    return lax.broadcasted_iota(jnp.int32, shape, 1)


def whole(shape):
    return pl.BlockSpec(shape, lambda *_: (0,) * len(shape))


def on_chip(x):
    return pltpu.with_memory_space_constraint(x, pltpu.VMEM)


def off_chip(x):
    return pltpu.with_memory_space_constraint(x, pltpu.HBM)


def flip_permute(value, flip):
    pairs = [(source, source ^ flip) for source in range(lax.axis_size("sp"))]
    return lax.ppermute(value, "sp", pairs)


def key_block_kernel(group_devices, low_ref, high_ref, wk_ref, wr_ref, *rest):
    outs, (packed, rates) = rest[:-2], rest[-2:]
    repeats = HEADS // GROUPS
    step = pl.program_id(0)
    rows = low_ref.shape[0]
    tiles = rows // LANES
    half_tiles = rates.shape[0] // 2
    wk, wr = wk_ref[...], wr_ref[...]
    both = jnp.concatenate([low_ref[...], high_ref[...]], axis=0)
    k_both = rounded(jnp.dot(both, wk, preferred_element_type=F32))
    k_low, k_high = k_both[:rows], k_both[rows:]
    r_both = lax.dot_general(both, wr, (((1,), (1,)), ((), ())), preferred_element_type=F32).astype(BF16)
    left = lane_index((rows, LANES)) < STATE
    for group in range(GROUPS):
        column = slice(group // 2 * LANES, (group // 2 + 1) * LANES)
        a, b = k_low[:, column], k_high[:, column]
        if group % 2 == 0:
            b = pltpu.roll(b, STATE, 1)
        else:
            a = pltpu.roll(a, STATE, 1)
        packed[group, pl.ds(pl.multiple_of(step * rows, rows), rows), :] = jnp.where(left, a, b).astype(BF16)
    eye = (
        lax.broadcasted_iota(jnp.int32, (HEADS, HEADS), 0) == lax.broadcasted_iota(jnp.int32, (HEADS, HEADS), 1)
    ).astype(BF16)
    for part in range(2):
        r = r_both[part * rows : (part + 1) * rows]
        turned = lax.dot_general(eye, r, (((1,), (1,)), ((), ())), preferred_element_type=F32)
        for tile in range(tiles):
            rates[part * half_tiles + step * tiles + tile] = turned[:, tile * LANES : (tile + 1) * LANES]

    @pl.when(step == pl.num_programs(0) - 1)
    def _():
        half = packed.shape[1] - 2 * half_tiles * repeats
        for group in range(GROUPS):
            tail = jnp.concatenate(
                [rates[tile, group * repeats : (group + 1) * repeats, :] for tile in range(2 * half_tiles)], axis=0
            )
            packed[group, half:, :] = tail.astype(BF16)
        own = lax.axis_index("sp") // group_devices
        for offset, out in enumerate(outs):
            out[...] = packed[own ^ offset]


def key_blocks(rows, wk, wr, group_devices):
    span, model = rows.shape
    repeats = HEADS // GROUPS
    half = span // 2
    tile = half // 2
    steps = half // tile
    height = half + repeats * span // LANES
    block = jax.ShapeDtypeStruct((height, LANES), BF16)
    return pl.pallas_call(
        lambda *refs: key_block_kernel(group_devices, *refs),
        grid=(steps,),
        in_specs=[
            pl.BlockSpec((tile, model), lambda i: (i, 0)),
            pl.BlockSpec((tile, model), lambda i: (i + steps, 0)),
            whole(wk.shape),
            whole(wr.shape),
        ],
        out_specs=[whole((height, LANES))] * GROUPS,
        out_shape=[block] * GROUPS,
        scratch_shapes=[
            pltpu.VMEM((GROUPS, height, LANES), BF16),
            pltpu.VMEM((span // LANES, HEADS, LANES), F32),
        ],
        compiler_params=pltpu.CompilerParams(vmem_limit_bytes=VMEM_LIMIT),
        cost_estimate=pl.CostEstimate(
            flops=2 * span * model * (GROUPS * STATE + HEADS), bytes_accessed=2 * span * model, transcendentals=0
        ),
        name="key_blocks",
    )(off_chip(rows), off_chip(rows), off_chip(wk), off_chip(wr))


def value_kernel(x_refs, w_ref, outs, kept):
    step = pl.program_id(0)
    share = kept.shape[2]
    devices = w_ref.shape[1] // share
    rows = x_refs[0].shape[0]
    x = jnp.concatenate([ref[...] for ref in x_refs], axis=0) if len(x_refs) > 1 else x_refs[0][...]
    y = jnp.dot(x, w_ref[...], preferred_element_type=F32)
    for device in range(devices):
        lanes = slice(device * share, (device + 1) * share)
        index = step * devices + device
        kept[index, :rows, :] = y[:rows, lanes].astype(BF16)
        if len(x_refs) > 1:
            half = EXTRA // 2
            last = y.shape[0]
            extra = jnp.concatenate([y[rows : rows + half, lanes], y[last - half :, lanes]], axis=0)
            kept[index, rows:, :] = extra.astype(BF16)

    @pl.when(step == pl.num_programs(0) - 1)
    def _():
        own = lax.axis_index("sp")
        for offset, out in enumerate(outs):
            out[...] = kept[own ^ offset]


def value_blocks(rows, wv, started, devices, cut, early):
    span, model = rows.shape
    width = wv.shape[1]
    share = width // devices
    tile = max(2 * LANES, share)
    if early:
        specs = [
            whole((cut, model)),
            pl.BlockSpec((TILE_ROWS, model), lambda i: (cut // TILE_ROWS, 0)),
            pl.BlockSpec((TILE_ROWS, model), lambda i: (span // TILE_ROWS - 1, 0)),
        ]
        block = (cut + EXTRA, share)
    else:
        specs = [pl.BlockSpec((span - cut, model), lambda i: (cut // (span - cut), 0))]
        block = (span - cut, share)
    count = len(specs)

    def kernel(*refs):
        value_kernel(refs[:count], refs[count], refs[count + 2 : -1], refs[-1])

    return pl.pallas_call(
        kernel,
        grid=(width // tile,),
        in_specs=specs + [pl.BlockSpec((model, tile), lambda i: (0, i)), pl.BlockSpec(memory_space=pl.ANY)],
        out_specs=[whole(block)] * devices,
        out_shape=[jax.ShapeDtypeStruct(block, BF16)] * devices,
        scratch_shapes=[pltpu.VMEM((devices,) + block, BF16)],
        compiler_params=pltpu.CompilerParams(vmem_limit_bytes=VMEM_LIMIT),
        cost_estimate=pl.CostEstimate(
            flops=2 * block[0] * model * width,
            bytes_accessed=2 * (block[0] * model + model * width),
            transcendentals=0,
        ),
        name="early_values" if early else "late_values",
    )(*[off_chip(rows)] * count, off_chip(wv), started)


def key_read_kernel(
    group_devices, *refs
):
    count = GROUPS * group_devices
    held, refs = refs[:count], refs[count:]
    (
        taps_ref,
        query_ref,
        offset_ref,
        decay_ref,
        spikes_ref,
        keys_ref,
        weight_ref,
        blocks,
        line,
        rates,
        scores,
        spikes,
    ) = refs
    repeats = HEADS // GROUPS
    sources = blocks.shape[0]
    half = keys_ref.shape[1] // 2
    heads = spikes_ref.shape[1]
    tiles = 2 * half // LANES
    me = lax.axis_index("sp")
    group, rank = me // group_devices, me % group_devices
    for offset in range(GROUPS):
        for shift in range(group_devices):
            blocks[(group ^ offset) * group_devices + (rank ^ shift)] = held[shift * GROUPS + offset][...]
    taps = []
    for k in range(5):
        tap = taps_ref[k, pl.ds(group, 1), :]
        taps.append(jnp.concatenate([tap, tap], axis=1))
    asked = query_ref[0].astype(F32)
    asked = jnp.where(lax.broadcasted_iota(jnp.int32, asked.shape, 0) == group, asked, 0.0)
    asked = jnp.sum(asked, axis=0, keepdims=True)
    asked = jnp.broadcast_to(jnp.concatenate([asked, asked], axis=1), (16, LANES))
    part_row = lax.broadcasted_iota(jnp.int32, (16, LANES), 0)
    query = jnp.where(part_row == lane_index((16, LANES)) // STATE, asked, 0.0).astype(BF16)
    edge_left = lane_index((16, LANES)) < STATE
    left = lane_index((half, LANES)) < STATE
    picked = lax.broadcasted_iota(jnp.int32, (heads * tiles, repeats * tiles), 0)
    column = lax.broadcasted_iota(jnp.int32, (heads * tiles, repeats * tiles), 1)
    select = (column == (picked % tiles) * repeats + rank * heads + picked // tiles).astype(BF16)

    def one_source(source, carry):
        body = blocks[source, :half, :].astype(F32)
        before = blocks[jnp.maximum(source - 1, 0), half - 16 : half, :].astype(F32)
        after = blocks[jnp.minimum(source + 1, sources - 1), :16, :].astype(F32)
        before = jnp.where(source > 0, before, 0.0)
        after = jnp.where(source < sources - 1, after, 0.0)
        top = jnp.where(edge_left, pltpu.roll(before, STATE, 1), pltpu.roll(body[half - 16 :], STATE, 1))
        bottom = jnp.where(edge_left, pltpu.roll(body[:16], STATE, 1), pltpu.roll(after, STATE, 1))
        line[0:16, :] = top
        line[16 : 16 + half, :] = body
        line[16 + half :, :] = bottom
        total = taps[0] * line[14 : 14 + half, :]
        for k in range(1, 5):
            total = total + taps[k] * line[14 + k : 14 + k + half, :]
        y = silu(total).astype(BF16)
        score = lax.dot_general(query, y, (((1,), (1,)), ((), ())), preferred_element_type=F32)
        scores[source] = jnp.concatenate(
            [score[part : part + 1, c * LANES : (c + 1) * LANES] for part in range(2) for c in range(tiles // 2)],
            axis=0,
        )
        z = y.astype(F32)
        turned = pltpu.roll(z, STATE, 1)
        keys_ref[source, :half, :] = jnp.where(left, z, turned).astype(BF16)
        keys_ref[source, half:, :] = jnp.where(left, turned, z).astype(BF16)
        chosen = jnp.dot(select, blocks[source, half:, :], preferred_element_type=F32)
        for h in range(heads):
            rates[h, source] = chosen[h * tiles : (h + 1) * tiles]
        return carry

    lax.fori_loop(0, sources, one_source, 0)
    count = sources * tiles
    lane_row = lax.broadcasted_iota(jnp.int32, (LANES, LANES), 0)
    lane_col = lax.broadcasted_iota(jnp.int32, (LANES, LANES), 1)
    later_lanes = (lane_row > lane_col).astype(F32)
    row = lax.broadcasted_iota(jnp.int32, (count, count), 0)
    col = lax.broadcasted_iota(jnp.int32, (count, count), 1)
    later_rows = (col > row).astype(F32)
    score = scores[...].reshape(count, LANES)
    for h in range(heads):
        for c in range(count):
            spikes[h, c : c + 1, :] = spikes_ref[0, h : h + 1, c * LANES : (c + 1) * LANES]
    exact = dict(preferred_element_type=F32, precision=lax.Precision.HIGHEST)
    for h in range(heads):
        raw = rates[h].reshape(count, LANES) + offset_ref[h]
        rate = jnp.maximum(raw, 0.0) + jnp.log1p(jnp.exp(-jnp.abs(raw)))
        decay = jnp.exp(jnp.full((1, LANES), decay_ref[h], F32))
        step = spikes[h] - decay * rate
        within = jnp.dot(step, later_lanes, **exact)
        totals = jnp.broadcast_to(jnp.sum(step, axis=1, keepdims=True), (count, LANES))
        ahead = within + jnp.dot(later_rows, totals, **exact)
        weight = rate * jnp.exp(ahead) * score
        high = rounded(weight)
        weight_ref[:, h] = high.reshape(sources, tiles, LANES)
        weight_ref[:, heads + h] = (weight - high).reshape(sources, tiles, LANES)


def key_read(held, relayed, taps, query, offset, decay, spikes, group_devices, span):
    sources = group_devices * GROUPS
    heads = offset.shape[0]
    half = span // 2
    tiles = span // LANES
    smem = pl.BlockSpec(memory_space=pltpu.SMEM)
    vmem = pl.BlockSpec(memory_space=pltpu.VMEM)
    count = len(held) + len(relayed)
    return pl.pallas_call(
        lambda *refs: key_read_kernel(group_devices, *refs),
        in_specs=[vmem] * (count + 2) + [smem, smem, vmem],
        out_specs=[vmem, vmem],
        out_shape=[
            jax.ShapeDtypeStruct((sources, span, LANES), BF16),
            jax.ShapeDtypeStruct((sources, 2 * heads, tiles, LANES), F32),
        ],
        scratch_shapes=[
            pltpu.VMEM((sources,) + held[0].shape, BF16),
            pltpu.VMEM((half + 32, LANES), F32),
            pltpu.VMEM((heads, sources, tiles, LANES), F32),
            pltpu.VMEM((sources, tiles, LANES), F32),
            pltpu.VMEM((heads, sources * tiles, LANES), F32),
        ],
        compiler_params=pltpu.CompilerParams(vmem_limit_bytes=VMEM_LIMIT),
        cost_estimate=pl.CostEstimate(flops=10**9, bytes_accessed=4 * 10**6, transcendentals=10**6),
        name="key_read",
    )(*(on_chip(x) for x in [*held, *relayed, taps, query]), offset, decay, on_chip(spikes))


def convolved(line, body, before, after, taps_ref, weight_ref, source, start_row, total):
    rows, share = body.shape
    heads = share // HEAD
    line[0:8, :] = before
    line[8 : 8 + rows, :] = body
    line[8 + rows :, :] = after
    taps = [jnp.concatenate([taps_ref[k, h : h + 1, :] for h in range(heads)], axis=1) for k in range(5)]
    tiles = weight_ref.shape[2]
    weight = weight_ref[source].reshape(-1, LANES)
    tile_of = lax.broadcasted_iota(jnp.int32, weight.shape, 0) % tiles
    read = jnp.zeros(total.shape, F32)
    values = []
    for tile in range(rows // LANES):
        start = tile * LANES
        y = taps[0] * line[6 + start : 6 + start + LANES, :]
        for k in range(1, 5):
            y = y + taps[k] * line[6 + k + start : 6 + k + start + LANES, :]
        y = silu(y).astype(BF16)
        masked = jnp.where(tile_of == start_row // LANES + tile, weight, 0.0).astype(BF16)
        read = read + jnp.dot(masked, y, preferred_element_type=F32)
        values.append(y)
    total[...] += read
    return values


def wove(woven, values, keys_ref, source, start_row, out_ref):
    share = values[0].shape[1]
    heads = share // HEAD
    left = lane_index((LANES, LANES)) < HEAD
    for tile, y in enumerate(values):
        start = tile * LANES
        keys = keys_ref[source, start_row + start : start_row + start + LANES, :].astype(F32)
        z = y.astype(F32)
        if share == LANES:
            pieces = [jnp.where(left, z, keys), jnp.where(left, pltpu.roll(z, HEAD, 1), keys)]
        else:
            pieces = [
                jnp.concatenate([z[:, h * HEAD : (h + 1) * HEAD], keys[:, STATE:]], axis=1) for h in range(heads)
            ]
        for h, piece in enumerate(pieces):
            woven[pl.ds(heads * start + h, LANES, heads), :] = piece
        part = slice(heads * start, heads * (start + LANES))
        out_ref[0, part, :] = woven[part, :].astype(BF16)


def line_scratch(rows, share):
    return pltpu.VMEM((rows + 16, share), F32)


def woven_scratch(rows, share):
    return pltpu.VMEM((share // HEAD * rows, LANES), F32)


def early_kernel(cut, *refs):
    blocks = refs[:-10]
    keys_ref, weight_ref, taps_ref, out_ref, read_ref, edges_ref, kept, line, woven, total = refs[-10:]
    source = pl.program_id(0)
    own = lax.axis_index("sp")

    @pl.when(source == 0)
    def _():
        total[...] = jnp.zeros_like(total)
        for offset, block_ref in enumerate(blocks):
            kept[own ^ offset] = block_ref[...]
            edges_ref[own ^ offset, :TILE_ROWS, :] = block_ref[:TILE_ROWS, :]
            edges_ref[own ^ offset, TILE_ROWS:, :] = block_ref[cut - TILE_ROWS : cut, :]

    block = kept[source].astype(F32)
    before = kept[jnp.maximum(source - 1, 0), cut:, :].astype(F32)
    before = jnp.where(source > 0, before, 0.0)
    values = convolved(line, block[:cut], before, block[cut:], taps_ref, weight_ref, source, 0, total)
    wove(woven, values, keys_ref, source, 0, out_ref)
    read_ref[...] = total[...]


def early_rows(blocks, keys, weight, taps, cut):
    sources, span = keys.shape[:2]
    height, share = blocks[0].shape
    heads = share // HEAD
    reads = weight.shape[1] * weight.shape[2]
    edges = (sources, 2 * TILE_ROWS, share)
    vmem = pl.BlockSpec(memory_space=pltpu.VMEM)
    inputs = [*blocks, keys, weight, taps]
    return pl.pallas_call(
        lambda *refs: early_kernel(cut, *refs),
        grid=(sources,),
        in_specs=[vmem] * len(inputs),
        out_specs=[
            pl.BlockSpec((1, heads * cut, LANES), lambda s: (s, 0, 0)),
            whole((reads, share)),
            whole(edges),
        ],
        out_shape=[
            jax.ShapeDtypeStruct((sources, heads * span, LANES), BF16),
            jax.ShapeDtypeStruct((reads, share), F32),
            jax.ShapeDtypeStruct(edges, BF16),
        ],
        scratch_shapes=[
            pltpu.VMEM((sources, height, share), BF16),
            line_scratch(cut, share),
            woven_scratch(cut, share),
            pltpu.VMEM((reads, share), F32),
        ],
        compiler_params=pltpu.CompilerParams(vmem_limit_bytes=VMEM_LIMIT),
        cost_estimate=pl.CostEstimate(flops=2 * 10**9, bytes_accessed=6 * 10**6, transcendentals=10**6),
        name="early_rows",
    )(*(on_chip(x) for x in inputs))


def late_values_of(offset, block_ref, edges_ref, taps_ref, weight_ref, line, total, cut):
    source = lax.axis_index("sp") ^ offset
    sources = edges_ref.shape[0]
    before = edges_ref[source, TILE_ROWS:, :].astype(F32)[TILE_ROWS - 8 :]
    after = edges_ref[jnp.minimum(source + 1, sources - 1), :TILE_ROWS, :].astype(F32)[:8]
    after = jnp.where(source < sources - 1, after, 0.0)
    body = block_ref[...].astype(F32)
    return convolved(line, body, before, after, taps_ref, weight_ref, source, cut, total)


def late_kernel(cut, offsets, *refs):
    count = len(offsets)
    blocks = refs[:count]
    edges_ref, keys_ref, weight_ref, taps_ref, read_ref, _, out_ref, total, line, woven = refs[count:]
    step = pl.program_id(0)

    @pl.when(step == 0)
    def _():
        total[...] = read_ref[...]

    for index, offset in enumerate(offsets):

        @pl.when(step == index)
        def _(index=index, offset=offset):
            values = late_values_of(offset, blocks[index], edges_ref, taps_ref, weight_ref, line, total, cut)
            wove(woven, values, keys_ref, lax.axis_index("sp") ^ offset, cut, out_ref)


def wave_offset(step, offsets):
    offset = step + offsets[0]
    for index in range(1, len(offsets)):
        gap = offsets[index] - offsets[index - 1] - 1
        if gap:
            offset = offset + gap * (step >= index).astype(jnp.int32)
    return offset


def late_out_spec(offsets, shape):
    rows = shape[1] // 2
    return pl.BlockSpec((1, rows, LANES), lambda i: (lax.axis_index("sp") ^ wave_offset(i, offsets), 1, 0))


def late_rows(offsets, late, edges, keys, weight, taps, read, out, cut):
    rows, share = late[0].shape
    vmem = pl.BlockSpec(memory_space=pltpu.VMEM)
    inputs = [late[k] for k in offsets] + [edges, keys, weight, taps, read]
    return pl.pallas_call(
        lambda *refs: late_kernel(cut, offsets, *refs),
        grid=(len(offsets),),
        in_specs=[vmem] * len(inputs) + [pl.BlockSpec(memory_space=pl.ANY)],
        out_specs=[late_out_spec(offsets, out.shape), whole(read.shape)],
        out_shape=[jax.ShapeDtypeStruct(out.shape, BF16), jax.ShapeDtypeStruct(read.shape, F32)],
        scratch_shapes=[line_scratch(rows, share), woven_scratch(rows, share)],
        input_output_aliases={len(inputs): 0},
        compiler_params=pltpu.CompilerParams(vmem_limit_bytes=VMEM_LIMIT),
        cost_estimate=pl.CostEstimate(flops=10**9, bytes_accessed=2 * 10**6, transcendentals=10**6),
        name="late_rows",
    )(*(on_chip(x) for x in inputs), out)


def last_read_kernel(cut, offsets, *refs):
    count = len(offsets)
    blocks = refs[:count]
    edges_ref, weight_ref, taps_ref, read_ref, gate_ref, values_ref, gated_ref, square_ref, line, total = refs[count:]
    total[...] = read_ref[...]
    for index, offset in enumerate(offsets):
        part = line.at[index]
        values = late_values_of(offset, blocks[index], edges_ref, taps_ref, weight_ref, part, total, cut)
        for tile, y in enumerate(values):
            values_ref[index, tile * LANES : (tile + 1) * LANES, :] = y
    tiles = weight_ref.shape[2]
    shape = total.shape
    heads = shape[1] // HEAD
    head = (lax.broadcasted_iota(jnp.int32, shape, 0) // tiles) % heads
    mine = head == lane_index(shape) // HEAD
    read = jnp.sum(jnp.where(mine, total[...], 0.0), axis=0, keepdims=True)
    read = jnp.concatenate([read[:, h * HEAD : (h + 1) * HEAD] for h in range(heads)], axis=0)
    gated = read * silu(gate_ref[0].astype(F32))
    gated_ref[...] = gated
    square = jnp.sum(jnp.sum(gated * gated, axis=1, keepdims=True), axis=0, keepdims=True)
    square_ref[...] = jnp.broadcast_to(square, square_ref.shape)


def last_read(offsets, late, edges, weight, taps, read, gate, cut):
    rows, share = late[0].shape
    vmem = pl.BlockSpec(memory_space=pltpu.VMEM)
    inputs = [late[k] for k in offsets] + [edges, weight, taps, read, gate]
    return pl.pallas_call(
        lambda *refs: last_read_kernel(cut, offsets, *refs),
        in_specs=[vmem] * len(inputs),
        out_specs=[vmem] * 3,
        out_shape=[
            jax.ShapeDtypeStruct((len(offsets), rows, share), BF16),
            jax.ShapeDtypeStruct((share // HEAD, HEAD), F32),
            jax.ShapeDtypeStruct((1, LANES), F32),
        ],
        scratch_shapes=[pltpu.VMEM((len(offsets), rows + 16, share), F32), pltpu.VMEM(read.shape, F32)],
        compiler_params=pltpu.CompilerParams(vmem_limit_bytes=VMEM_LIMIT),
        cost_estimate=pl.CostEstimate(flops=10**9, bytes_accessed=10**6, transcendentals=10**6),
        name="last_read",
    )(*(on_chip(x) for x in inputs))


def last_rows_kernel(cut, offsets, values_ref, keys_ref, _, out_ref, woven):
    step = pl.program_id(0)
    rows = values_ref.shape[1]
    values = [values_ref[step, start : start + LANES, :] for start in range(0, rows, LANES)]
    wove(woven, values, keys_ref, lax.axis_index("sp") ^ wave_offset(step, offsets), cut, out_ref)


def last_rows(offsets, values, keys, out, cut):
    rows, share = values.shape[1:]
    vmem = pl.BlockSpec(memory_space=pltpu.VMEM)
    return pl.pallas_call(
        lambda *refs: last_rows_kernel(cut, offsets, *refs),
        grid=(len(offsets),),
        in_specs=[vmem, vmem, pl.BlockSpec(memory_space=pl.ANY)],
        out_specs=late_out_spec(offsets, out.shape),
        out_shape=jax.ShapeDtypeStruct(out.shape, BF16),
        scratch_shapes=[woven_scratch(rows, share)],
        input_output_aliases={2: 0},
        compiler_params=pltpu.CompilerParams(vmem_limit_bytes=VMEM_LIMIT),
        cost_estimate=pl.CostEstimate(flops=10**9, bytes_accessed=2 * 10**6, transcendentals=0),
        name="last_rows",
    )(on_chip(values), on_chip(keys), out)


def on_device(
    context_input_tensor,
    content_mapping_matrix,
    address_mapping_matrix,
    increment_mapping_matrix,
    increment_speed_offset,
    channel_fading_exponent,
    extra_damping_spikes,
    content_smoothing_coefficients,
    address_smoothing_coefficients,
    newest_lookup_matrix,
    newest_output_switch,
    cluster_scaling_coefficients,
):
    rows = context_input_tensor[0]
    span = rows.shape[0]
    repeats = HEADS // GROUPS
    heads = increment_speed_offset.shape[0]
    group_devices = repeats // heads
    devices = lax.axis_size("sp")
    cut = span // 2

    blocks = key_blocks(rows, address_mapping_matrix, increment_mapping_matrix.T, group_devices)
    direct = [None] * (GROUPS - 1)
    for offset in range(1, GROUPS):
        direct[offset - 1] = flip_permute(blocks[offset], offset * group_devices)
    early = value_blocks(rows, content_mapping_matrix, blocks[0], devices, cut, True)
    late = value_blocks(rows, content_mapping_matrix, early[0], devices, cut, False)
    held = [blocks[0]] + direct
    relayed = []
    for shift in range(1, group_devices):
        for offset in range(GROUPS):
            relayed.append(flip_permute(held[offset], shift))
    early_blocks, late_blocks = [early[0]], [late[0]]
    for offset in range(1, devices):
        early_blocks.append(flip_permute(early[offset], offset))
        late_blocks.append(flip_permute(late[offset], offset))

    keys, weight = key_read(
        held,
        relayed,
        address_smoothing_coefficients,
        newest_lookup_matrix,
        increment_speed_offset,
        channel_fading_exponent,
        extra_damping_spikes,
        group_devices,
        span,
    )
    taps = content_smoothing_coefficients
    out, read, edges = early_rows(early_blocks, keys, weight, taps, cut)
    half = devices // 2
    first, final = list(range(half)), list(range(half, devices))
    out, read = late_rows(first, late_blocks, edges, keys, weight, taps, read, out, cut)
    values, gated, group_sq = last_read(final, late_blocks, edges, weight, taps, read, newest_output_switch, cut)
    for level in range(group_devices.bit_length() - 1):
        group_sq = group_sq + flip_permute(group_sq, 2**level)
    out = last_rows(final, values, keys, out, cut)
    scaled = gated * lax.rsqrt(group_sq[0, 0] / (repeats * HEAD) + EPS) * cluster_scaling_coefficients
    store = out.reshape(1, devices * span, heads, HEAD + STATE)
    return store, scaled.astype(BF16).reshape(1, heads, HEAD)


def solution(mesh):
    placed = (
        P(("gr", "tp"), "sp", None),
        P(),
        P(),
        P(),
        P("sp"),
        P("sp"),
        P(("gr", "tp"), "sp", None),
        P(None, "sp", None),
        P(),
        P(("gr", "tp"), None, None),
        P(("gr", "tp"), "sp", None),
        P("sp", None),
    )

    return jax.shard_map(
        on_device,
        mesh=mesh,
        in_specs=placed,
        out_specs=(P(("gr", "tp"), None, "sp", None), P(("gr", "tp"), "sp", None)),
        check_vma=False,
    )
```

```python
import jax
import jax.numpy as jnp
from jax import lax
from jax.experimental import pallas as pl
from jax.experimental.pallas import tpu as pltpu
from jax.sharding import PartitionSpec as P


HEADS = 16
HEAD = 64
GROUPS = 4
STATE = 64
LANES = 128
EXTRA = 8
TILE_ROWS = 16
VMEM_LIMIT = 24 * 2**20
EPS = 1e-05
F32 = jnp.float32
BF16 = jnp.bfloat16


def silu(x):
    return 0.5 * x * (1.0 + jnp.tanh(0.5 * x))


def rounded(x):
    return x.astype(BF16).astype(F32)


def lane_index(shape):
    return lax.broadcasted_iota(jnp.int32, shape, 1)


def whole(shape):
    return pl.BlockSpec(shape, lambda *_: (0,) * len(shape))


def on_chip(x):
    return pltpu.with_memory_space_constraint(x, pltpu.VMEM)


def off_chip(x):
    return pltpu.with_memory_space_constraint(x, pltpu.HBM)


def flip_permute(value, flip):
    pairs = [(source, source ^ flip) for source in range(lax.axis_size("sp"))]
    return lax.ppermute(value, "sp", pairs)


def key_block_kernel(group_devices, low_ref, high_ref, wk_ref, *rest):
    outs, packed = rest[:-1], rest[-1]
    step = pl.program_id(0)
    rows = low_ref.shape[0]
    both = jnp.concatenate([low_ref[...], high_ref[...]], axis=0)
    k_both = rounded(jnp.dot(both, wk_ref[...], preferred_element_type=F32))
    k_low, k_high = k_both[:rows], k_both[rows:]
    left = lane_index((rows, LANES)) < STATE
    for group in range(GROUPS):
        column = slice(group // 2 * LANES, (group // 2 + 1) * LANES)
        a, b = k_low[:, column], k_high[:, column]
        if group % 2 == 0:
            b = pltpu.roll(b, STATE, 1)
        else:
            a = pltpu.roll(a, STATE, 1)
        packed[group, pl.ds(pl.multiple_of(step * rows, rows), rows), :] = jnp.where(left, a, b).astype(BF16)

    @pl.when(step == pl.num_programs(0) - 1)
    def _():
        own = lax.axis_index("sp") // group_devices
        for offset, out in enumerate(outs):
            out[...] = packed[own ^ offset]


def key_blocks(rows, wk, group_devices):
    span, model = rows.shape
    half = span // 2
    tile = half // 2
    steps = half // tile
    block = jax.ShapeDtypeStruct((half, LANES), BF16)
    return pl.pallas_call(
        lambda *refs: key_block_kernel(group_devices, *refs),
        grid=(steps,),
        in_specs=[
            pl.BlockSpec((tile, model), lambda i: (i, 0)),
            pl.BlockSpec((tile, model), lambda i: (i + steps, 0)),
            whole(wk.shape),
        ],
        out_specs=[whole(block.shape)] * GROUPS,
        out_shape=[block] * GROUPS,
        scratch_shapes=[pltpu.VMEM((GROUPS,) + block.shape, BF16)],
        compiler_params=pltpu.CompilerParams(vmem_limit_bytes=VMEM_LIMIT),
        cost_estimate=pl.CostEstimate(
            flops=2 * span * model * GROUPS * STATE, bytes_accessed=2 * span * model, transcendentals=0
        ),
        name="key_blocks",
    )(off_chip(rows), off_chip(rows), off_chip(wk))


def early_value_kernel(x_ref, after_ref, last_ref, other_ref, w_ref, wr_ref, _, *rest):
    outs, (kept, rates) = rest[:-2], rest[-2:]
    step = pl.program_id(0)
    share = kept.shape[2]
    devices = w_ref.shape[1] // share
    rows = x_ref.shape[0]
    x = jnp.concatenate([x_ref[...], after_ref[...], last_ref[...]], axis=0)
    y = jnp.dot(x, w_ref[...], preferred_element_type=F32)
    last = y.shape[0]
    half = EXTRA // 2
    extra = jnp.concatenate([y[rows : rows + half], y[last - half :]], axis=0)
    for device in range(devices):
        lanes = slice(device * share, (device + 1) * share)
        index = step * devices + device
        kept[index, :rows, :] = y[:rows, lanes].astype(BF16)
        kept[index, kept.shape[1] - EXTRA :, :] = extra[:, lanes].astype(BF16)
    part = other_ref.shape[0]
    pieces = part // share
    own_rows = x_ref[pl.ds(pl.multiple_of(step * part, part), part), :]
    both = jnp.concatenate([own_rows, other_ref[...]], axis=0)
    r = lax.dot_general(both, wr_ref[...], (((1,), (1,)), ((), ())), preferred_element_type=F32).astype(BF16)
    eye = (
        lax.broadcasted_iota(jnp.int32, (HEADS, HEADS), 0) == lax.broadcasted_iota(jnp.int32, (HEADS, HEADS), 1)
    ).astype(BF16)
    turned = lax.dot_general(eye, r, (((1,), (1,)), ((), ())), preferred_element_type=F32)
    count = rates.shape[0]
    for piece in range(pieces):
        rates[step * pieces + piece] = turned[:, piece * share : (piece + 1) * share]
        rates[count // 2 + step * pieces + piece] = turned[:, part + piece * share : part + (piece + 1) * share]

    @pl.when(step == pl.num_programs(0) - 1)
    def _():
        heads = share // HEAD
        for device in range(kept.shape[0]):
            tile = [rates[t, h : h + 1, :] for h in range(device * heads, (device + 1) * heads) for t in range(count)]
            kept[device, rows : rows + heads * count, :] = jnp.concatenate(tile, axis=0).astype(BF16)
        own = lax.axis_index("sp")
        for offset, out in enumerate(outs):
            out[...] = kept[own ^ offset]


def early_values(rows, wv, wr, started, devices, cut):
    span, model = rows.shape
    width = wv.shape[1]
    share = width // devices
    tile = max(2 * LANES, share)
    steps = width // tile
    part = cut // steps
    block = (cut + span // HEAD + EXTRA, share)
    x = off_chip(rows)
    return pl.pallas_call(
        early_value_kernel,
        grid=(steps,),
        in_specs=[
            whole((cut, model)),
            pl.BlockSpec((TILE_ROWS, model), lambda i: (cut // TILE_ROWS, 0)),
            pl.BlockSpec((TILE_ROWS, model), lambda i: (span // TILE_ROWS - 1, 0)),
            pl.BlockSpec((part, model), lambda i: (cut // part + i, 0)),
            pl.BlockSpec((model, tile), lambda i: (0, i)),
            whole(wr.shape),
            pl.BlockSpec(memory_space=pl.ANY),
        ],
        out_specs=[whole(block)] * devices,
        out_shape=[jax.ShapeDtypeStruct(block, BF16)] * devices,
        scratch_shapes=[pltpu.VMEM((devices,) + block, BF16), pltpu.VMEM((span // share, HEADS, share), F32)],
        compiler_params=pltpu.CompilerParams(vmem_limit_bytes=VMEM_LIMIT),
        cost_estimate=pl.CostEstimate(
            flops=2 * cut * model * width, bytes_accessed=2 * (span * model + model * width), transcendentals=0
        ),
        name="early_values",
    )(x, x, x, x, off_chip(wv), off_chip(wr), started)


def late_value_kernel(x_ref, w_ref, _, *rest):
    outs, kept = rest[:-1], rest[-1]
    step = pl.program_id(0)
    share = kept.shape[2]
    devices = w_ref.shape[1] // share
    y = jnp.dot(x_ref[...], w_ref[...], preferred_element_type=F32)
    for device in range(devices):
        kept[step * devices + device] = y[:, device * share : (device + 1) * share].astype(BF16)

    @pl.when(step == pl.num_programs(0) - 1)
    def _():
        own = lax.axis_index("sp")
        for offset, out in enumerate(outs):
            out[...] = kept[own ^ offset]


def late_values(rows, wv, started, devices, cut):
    span, model = rows.shape
    width = wv.shape[1]
    share = width // devices
    tile = max(2 * LANES, share)
    late = span - cut
    block = (late, share)
    return pl.pallas_call(
        late_value_kernel,
        grid=(width // tile,),
        in_specs=[
            pl.BlockSpec((late, model), lambda i: (cut // late, 0)),
            pl.BlockSpec((model, tile), lambda i: (0, i)),
            pl.BlockSpec(memory_space=pl.ANY),
        ],
        out_specs=[whole(block)] * devices,
        out_shape=[jax.ShapeDtypeStruct(block, BF16)] * devices,
        scratch_shapes=[pltpu.VMEM((devices,) + block, BF16)],
        compiler_params=pltpu.CompilerParams(vmem_limit_bytes=VMEM_LIMIT),
        cost_estimate=pl.CostEstimate(
            flops=2 * late * model * width, bytes_accessed=2 * (late * model + model * width), transcendentals=0
        ),
        name="late_values",
    )(off_chip(rows), off_chip(wv), started)


def key_read_kernel(group_devices, *refs):
    count = GROUPS * group_devices
    held = refs[:count]
    taps_ref, query_ref, keys_ref, score_ref, blocks, line = refs[count:]
    sources = blocks.shape[0]
    half = blocks.shape[1]
    tiles = 2 * half // LANES
    me = lax.axis_index("sp")
    group, rank = me // group_devices, me % group_devices
    for offset in range(GROUPS):
        for shift in range(group_devices):
            blocks[(group ^ offset) * group_devices + (rank ^ shift)] = held[shift * GROUPS + offset][...]
    taps = []
    for k in range(5):
        tap = taps_ref[k, pl.ds(group, 1), :]
        taps.append(jnp.concatenate([tap, tap], axis=1))
    asked = query_ref[0].astype(F32)
    asked = jnp.where(lax.broadcasted_iota(jnp.int32, asked.shape, 0) == group, asked, 0.0)
    asked = jnp.sum(asked, axis=0, keepdims=True)
    asked = jnp.broadcast_to(jnp.concatenate([asked, asked], axis=1), (16, LANES))
    part_row = lax.broadcasted_iota(jnp.int32, (16, LANES), 0)
    query = jnp.where(part_row == lane_index((16, LANES)) // STATE, asked, 0.0).astype(BF16)
    edge_left = lane_index((16, LANES)) < STATE
    left = lane_index((half, LANES)) < STATE

    def one_source(source, carry):
        body = blocks[source, :half, :].astype(F32)
        before = blocks[jnp.maximum(source - 1, 0), half - 16 : half, :].astype(F32)
        after = blocks[jnp.minimum(source + 1, sources - 1), :16, :].astype(F32)
        before = jnp.where(source > 0, before, 0.0)
        after = jnp.where(source < sources - 1, after, 0.0)
        top = jnp.where(edge_left, pltpu.roll(before, STATE, 1), pltpu.roll(body[half - 16 :], STATE, 1))
        bottom = jnp.where(edge_left, pltpu.roll(body[:16], STATE, 1), pltpu.roll(after, STATE, 1))
        line[0:16, :] = top
        line[16 : 16 + half, :] = body
        line[16 + half :, :] = bottom
        total = taps[0] * line[14 : 14 + half, :]
        for k in range(1, 5):
            total = total + taps[k] * line[14 + k : 14 + k + half, :]
        y = silu(total).astype(BF16)
        score = lax.dot_general(query, y, (((1,), (1,)), ((), ())), preferred_element_type=F32)
        score_ref[source] = jnp.concatenate(
            [score[part : part + 1, c * LANES : (c + 1) * LANES] for part in range(2) for c in range(tiles // 2)],
            axis=0,
        )
        z = y.astype(F32)
        turned = pltpu.roll(z, STATE, 1)
        keys_ref[source, :half, :] = jnp.where(left, z, turned).astype(BF16)
        keys_ref[source, half:, :] = jnp.where(left, turned, z).astype(BF16)
        return carry

    lax.fori_loop(0, sources, one_source, 0)


def key_read(held, taps, query, group_devices, span):
    sources = len(held)
    vmem = pl.BlockSpec(memory_space=pltpu.VMEM)
    inputs = [*held, taps, query]
    return pl.pallas_call(
        lambda *refs: key_read_kernel(group_devices, *refs),
        in_specs=[vmem] * len(inputs),
        out_specs=[vmem, vmem],
        out_shape=[
            jax.ShapeDtypeStruct((sources, span, LANES), BF16),
            jax.ShapeDtypeStruct((sources, span // LANES, LANES), F32),
        ],
        scratch_shapes=[
            pltpu.VMEM((sources,) + held[0].shape, BF16),
            pltpu.VMEM((span // 2 + 32, LANES), F32),
        ],
        compiler_params=pltpu.CompilerParams(vmem_limit_bytes=VMEM_LIMIT),
        cost_estimate=pl.CostEstimate(flops=10**9, bytes_accessed=4 * 10**6, transcendentals=10**6),
        name="key_read",
    )(*(on_chip(x) for x in inputs))


def read_weights(blocks, cut, score_ref, offset_ref, decay_ref, spikes_ref, spikes, weight_ref):
    sources, tiles = score_ref.shape[:2]
    share = blocks.shape[2]
    heads = share // HEAD
    count = sources * tiles
    lane_row = lax.broadcasted_iota(jnp.int32, (LANES, LANES), 0)
    lane_col = lax.broadcasted_iota(jnp.int32, (LANES, LANES), 1)
    later_lanes = (lane_row > lane_col).astype(F32)
    row = lax.broadcasted_iota(jnp.int32, (count, count), 0)
    col = lax.broadcasted_iota(jnp.int32, (count, count), 1)
    later_rows = (col > row).astype(F32)
    score = score_ref[...].reshape(count, LANES)
    for h in range(heads):
        for c in range(count):
            spikes[h, c : c + 1, :] = spikes_ref[0, h : h + 1, c * LANES : (c + 1) * LANES]
    exact = dict(preferred_element_type=F32, precision=lax.Precision.HIGHEST)
    pieces = LANES // share
    for h in range(heads):
        rates = []
        for source in range(sources):
            sent = blocks[source, cut : cut + heads * tiles * pieces, :]
            if pieces == 1:
                rates.append(sent.astype(F32)[h * tiles : (h + 1) * tiles])
            else:
                picks = []
                for piece in range(pieces):
                    wanted = lax.broadcasted_iota(jnp.int32, (tiles, sent.shape[0]), 0)
                    column = lax.broadcasted_iota(jnp.int32, (tiles, sent.shape[0]), 1)
                    pick = (column == (h * tiles + wanted) * pieces + piece).astype(BF16)
                    picks.append(jnp.dot(pick, sent, preferred_element_type=F32))
                rates.append(jnp.concatenate(picks, axis=1))
        raw = jnp.concatenate(rates, axis=0) + offset_ref[h]
        rate = jnp.maximum(raw, 0.0) + jnp.log1p(jnp.exp(-jnp.abs(raw)))
        decay = jnp.exp(jnp.full((1, LANES), decay_ref[h], F32))
        step = spikes[h] - decay * rate
        within = jnp.dot(step, later_lanes, **exact)
        totals = jnp.broadcast_to(jnp.sum(step, axis=1, keepdims=True), (count, LANES))
        ahead = within + jnp.dot(later_rows, totals, **exact)
        weight = rate * jnp.exp(ahead) * score
        high = rounded(weight)
        weight_ref[:, h] = high.reshape(sources, tiles, LANES)
        weight_ref[:, heads + h] = (weight - high).reshape(sources, tiles, LANES)


def convolved(line, body, before, after, taps_ref, weight_ref, source, start_row, total):
    rows, share = body.shape
    heads = share // HEAD
    line[0:8, :] = before
    line[8 : 8 + rows, :] = body
    line[8 + rows :, :] = after
    taps = [jnp.concatenate([taps_ref[k, h : h + 1, :] for h in range(heads)], axis=1) for k in range(5)]
    tiles = weight_ref.shape[2]
    weight = weight_ref[source].reshape(-1, LANES)
    tile_of = lax.broadcasted_iota(jnp.int32, weight.shape, 0) % tiles
    read = jnp.zeros(total.shape, F32)
    values = []
    for tile in range(rows // LANES):
        start = tile * LANES
        y = taps[0] * line[6 + start : 6 + start + LANES, :]
        for k in range(1, 5):
            y = y + taps[k] * line[6 + k + start : 6 + k + start + LANES, :]
        y = silu(y).astype(BF16)
        masked = jnp.where(tile_of == start_row // LANES + tile, weight, 0.0).astype(BF16)
        read = read + jnp.dot(masked, y, preferred_element_type=F32)
        values.append(y)
    total[...] += read
    return values


def wove(woven, values, keys_ref, source, start_row, out_ref):
    share = values[0].shape[1]
    heads = share // HEAD
    left = lane_index((LANES, LANES)) < HEAD
    for tile, y in enumerate(values):
        start = tile * LANES
        keys = keys_ref[source, start_row + start : start_row + start + LANES, :].astype(F32)
        z = y.astype(F32)
        if share == LANES:
            pieces = [jnp.where(left, z, keys), jnp.where(left, pltpu.roll(z, HEAD, 1), keys)]
        else:
            pieces = [
                jnp.concatenate([z[:, h * HEAD : (h + 1) * HEAD], keys[:, STATE:]], axis=1) for h in range(heads)
            ]
        for h, piece in enumerate(pieces):
            woven[pl.ds(heads * start + h, LANES, heads), :] = piece
        part = slice(heads * start, heads * (start + LANES))
        out_ref[0, part, :] = woven[part, :].astype(BF16)


def line_scratch(rows, share):
    return pltpu.VMEM((rows + 16, share), F32)


def woven_scratch(rows, share):
    return pltpu.VMEM((share // HEAD * rows, LANES), F32)


def early_kernel(cut, *refs):
    blocks, refs = refs[:-15], refs[-15:]
    keys_ref, score_ref, taps_ref, spikes_ref, offset_ref, decay_ref = refs[:6]
    out_ref, read_ref, edges_ref, weight_ref, kept, line, woven, total, spikes = refs[6:]
    source = pl.program_id(0)
    own = lax.axis_index("sp")

    @pl.when(source == 0)
    def _():
        total[...] = jnp.zeros_like(total)
        for offset, block_ref in enumerate(blocks):
            kept[own ^ offset] = block_ref[...]
            edges_ref[own ^ offset, :TILE_ROWS, :] = block_ref[:TILE_ROWS, :]
            edges_ref[own ^ offset, TILE_ROWS:, :] = block_ref[cut - TILE_ROWS : cut, :]
        read_weights(kept, cut, score_ref, offset_ref, decay_ref, spikes_ref, spikes, weight_ref)

    block = kept[source].astype(F32)
    before = kept[jnp.maximum(source - 1, 0), kept.shape[1] - EXTRA :, :].astype(F32)
    before = jnp.where(source > 0, before, 0.0)
    beside = block[block.shape[0] - EXTRA :]
    values = convolved(line, block[:cut], before, beside, taps_ref, weight_ref, source, 0, total)
    wove(woven, values, keys_ref, source, 0, out_ref)
    read_ref[...] = total[...]


def early_rows(blocks, keys, score, taps, spikes, offset, decay, cut):
    sources, span = keys.shape[:2]
    height, share = blocks[0].shape
    heads = share // HEAD
    tiles = span // LANES
    reads = 2 * heads * tiles
    edges = (sources, 2 * TILE_ROWS, share)
    vmem = pl.BlockSpec(memory_space=pltpu.VMEM)
    smem = pl.BlockSpec(memory_space=pltpu.SMEM)
    inputs = [*blocks, keys, score, taps, spikes]
    weight = (sources, 2 * heads, tiles, LANES)
    return pl.pallas_call(
        lambda *refs: early_kernel(cut, *refs),
        grid=(sources,),
        in_specs=[vmem] * len(inputs) + [smem, smem],
        out_specs=[
            pl.BlockSpec((1, heads * cut, LANES), lambda s: (s, 0, 0)),
            whole((reads, share)),
            whole(edges),
            whole(weight),
        ],
        out_shape=[
            jax.ShapeDtypeStruct((sources, heads * span, LANES), BF16),
            jax.ShapeDtypeStruct((reads, share), F32),
            jax.ShapeDtypeStruct(edges, BF16),
            jax.ShapeDtypeStruct(weight, F32),
        ],
        scratch_shapes=[
            pltpu.VMEM((sources, height, share), BF16),
            line_scratch(cut, share),
            woven_scratch(cut, share),
            pltpu.VMEM((reads, share), F32),
            pltpu.VMEM((heads, sources * tiles, LANES), F32),
        ],
        compiler_params=pltpu.CompilerParams(vmem_limit_bytes=VMEM_LIMIT),
        cost_estimate=pl.CostEstimate(flops=2 * 10**9, bytes_accessed=6 * 10**6, transcendentals=10**6),
        name="early_rows",
    )(*(on_chip(x) for x in inputs), offset, decay)


def late_values_of(offset, block_ref, edges_ref, taps_ref, weight_ref, line, total, cut):
    source = lax.axis_index("sp") ^ offset
    sources = edges_ref.shape[0]
    before = edges_ref[source, TILE_ROWS:, :].astype(F32)[TILE_ROWS - 8 :]
    after = edges_ref[jnp.minimum(source + 1, sources - 1), :TILE_ROWS, :].astype(F32)[:8]
    after = jnp.where(source < sources - 1, after, 0.0)
    body = block_ref[...].astype(F32)
    return convolved(line, body, before, after, taps_ref, weight_ref, source, cut, total)


def late_kernel(cut, offsets, *refs):
    count = len(offsets)
    blocks = refs[:count]
    edges_ref, keys_ref, weight_ref, taps_ref, read_ref, _, out_ref, total, line, woven = refs[count:]
    step = pl.program_id(0)

    @pl.when(step == 0)
    def _():
        total[...] = read_ref[...]

    for index, offset in enumerate(offsets):

        @pl.when(step == index)
        def _(index=index, offset=offset):
            values = late_values_of(offset, blocks[index], edges_ref, taps_ref, weight_ref, line, total, cut)
            wove(woven, values, keys_ref, lax.axis_index("sp") ^ offset, cut, out_ref)


def wave_offset(step, offsets):
    offset = step + offsets[0]
    for index in range(1, len(offsets)):
        gap = offsets[index] - offsets[index - 1] - 1
        if gap:
            offset = offset + gap * (step >= index).astype(jnp.int32)
    return offset


def late_out_spec(offsets, shape):
    rows = shape[1] // 2
    return pl.BlockSpec((1, rows, LANES), lambda i: (lax.axis_index("sp") ^ wave_offset(i, offsets), 1, 0))


def late_rows(offsets, late, edges, keys, weight, taps, read, out, cut):
    rows, share = late[0].shape
    vmem = pl.BlockSpec(memory_space=pltpu.VMEM)
    inputs = [late[k] for k in offsets] + [edges, keys, weight, taps, read]
    return pl.pallas_call(
        lambda *refs: late_kernel(cut, offsets, *refs),
        grid=(len(offsets),),
        in_specs=[vmem] * len(inputs) + [pl.BlockSpec(memory_space=pl.ANY)],
        out_specs=[late_out_spec(offsets, out.shape), whole(read.shape)],
        out_shape=[jax.ShapeDtypeStruct(out.shape, BF16), jax.ShapeDtypeStruct(read.shape, F32)],
        scratch_shapes=[line_scratch(rows, share), woven_scratch(rows, share)],
        input_output_aliases={len(inputs): 0},
        compiler_params=pltpu.CompilerParams(vmem_limit_bytes=VMEM_LIMIT),
        cost_estimate=pl.CostEstimate(flops=10**9, bytes_accessed=2 * 10**6, transcendentals=10**6),
        name="late_rows",
    )(*(on_chip(x) for x in inputs), out)


def last_read_kernel(cut, offsets, *refs):
    count = len(offsets)
    blocks = refs[:count]
    edges_ref, weight_ref, taps_ref, read_ref, gate_ref, values_ref, gated_ref, square_ref, line, total = refs[count:]
    total[...] = read_ref[...]
    for index, offset in enumerate(offsets):
        part = line.at[index]
        values = late_values_of(offset, blocks[index], edges_ref, taps_ref, weight_ref, part, total, cut)
        for tile, y in enumerate(values):
            values_ref[index, tile * LANES : (tile + 1) * LANES, :] = y
    tiles = weight_ref.shape[2]
    shape = total.shape
    heads = shape[1] // HEAD
    head = (lax.broadcasted_iota(jnp.int32, shape, 0) // tiles) % heads
    mine = head == lane_index(shape) // HEAD
    read = jnp.sum(jnp.where(mine, total[...], 0.0), axis=0, keepdims=True)
    read = jnp.concatenate([read[:, h * HEAD : (h + 1) * HEAD] for h in range(heads)], axis=0)
    gated = read * silu(gate_ref[0].astype(F32))
    gated_ref[...] = gated
    square = jnp.sum(jnp.sum(gated * gated, axis=1, keepdims=True), axis=0, keepdims=True)
    square_ref[...] = jnp.broadcast_to(square, square_ref.shape)


def last_read(offsets, late, edges, weight, taps, read, gate, cut):
    rows, share = late[0].shape
    vmem = pl.BlockSpec(memory_space=pltpu.VMEM)
    inputs = [late[k] for k in offsets] + [edges, weight, taps, read, gate]
    return pl.pallas_call(
        lambda *refs: last_read_kernel(cut, offsets, *refs),
        in_specs=[vmem] * len(inputs),
        out_specs=[vmem] * 3,
        out_shape=[
            jax.ShapeDtypeStruct((len(offsets), rows, share), BF16),
            jax.ShapeDtypeStruct((share // HEAD, HEAD), F32),
            jax.ShapeDtypeStruct((1, LANES), F32),
        ],
        scratch_shapes=[pltpu.VMEM((len(offsets), rows + 16, share), F32), pltpu.VMEM(read.shape, F32)],
        compiler_params=pltpu.CompilerParams(vmem_limit_bytes=VMEM_LIMIT),
        cost_estimate=pl.CostEstimate(flops=10**9, bytes_accessed=10**6, transcendentals=10**6),
        name="last_read",
    )(*(on_chip(x) for x in inputs))


def last_rows_kernel(cut, offsets, values_ref, keys_ref, _, out_ref, woven):
    step = pl.program_id(0)
    rows = values_ref.shape[1]
    values = [values_ref[step, start : start + LANES, :] for start in range(0, rows, LANES)]
    wove(woven, values, keys_ref, lax.axis_index("sp") ^ wave_offset(step, offsets), cut, out_ref)


def last_rows(offsets, values, keys, out, cut):
    rows, share = values.shape[1:]
    vmem = pl.BlockSpec(memory_space=pltpu.VMEM)
    return pl.pallas_call(
        lambda *refs: last_rows_kernel(cut, offsets, *refs),
        grid=(len(offsets),),
        in_specs=[vmem, vmem, pl.BlockSpec(memory_space=pl.ANY)],
        out_specs=late_out_spec(offsets, out.shape),
        out_shape=jax.ShapeDtypeStruct(out.shape, BF16),
        scratch_shapes=[woven_scratch(rows, share)],
        input_output_aliases={2: 0},
        compiler_params=pltpu.CompilerParams(vmem_limit_bytes=VMEM_LIMIT),
        cost_estimate=pl.CostEstimate(flops=10**9, bytes_accessed=2 * 10**6, transcendentals=0),
        name="last_rows",
    )(on_chip(values), on_chip(keys), out)


def on_device(
    context_input_tensor,
    content_mapping_matrix,
    address_mapping_matrix,
    increment_mapping_matrix,
    increment_speed_offset,
    channel_fading_exponent,
    extra_damping_spikes,
    content_smoothing_coefficients,
    address_smoothing_coefficients,
    newest_lookup_matrix,
    newest_output_switch,
    cluster_scaling_coefficients,
):
    rows = context_input_tensor[0]
    span = rows.shape[0]
    repeats = HEADS // GROUPS
    heads = increment_speed_offset.shape[0]
    group_devices = repeats // heads
    devices = lax.axis_size("sp")
    cut = span // 2

    blocks = key_blocks(rows, address_mapping_matrix, group_devices)
    direct = [None] * (GROUPS - 1)
    for offset in range(1, GROUPS):
        direct[offset - 1] = flip_permute(blocks[offset], offset * group_devices)
    early = early_values(rows, content_mapping_matrix, increment_mapping_matrix.T, blocks[0], devices, cut)
    late = late_values(rows, content_mapping_matrix, early[0], devices, cut)
    held = [blocks[0]] + direct
    relayed = []
    for shift in range(1, group_devices):
        for offset in range(GROUPS):
            relayed.append(flip_permute(held[offset], shift))
    early_blocks, late_blocks = [early[0]], [late[0]]
    for offset in range(1, devices):
        early_blocks.append(flip_permute(early[offset], offset))
        late_blocks.append(flip_permute(late[offset], offset))

    keys, score = key_read(held + relayed, address_smoothing_coefficients, newest_lookup_matrix, group_devices, span)
    taps = content_smoothing_coefficients
    out, read, edges, weight = early_rows(
        early_blocks,
        keys,
        score,
        taps,
        extra_damping_spikes,
        increment_speed_offset,
        channel_fading_exponent,
        cut,
    )
    half = devices // 2
    first, final = list(range(half)), list(range(half, devices))
    out, read = late_rows(first, late_blocks, edges, keys, weight, taps, read, out, cut)
    values, gated, group_sq = last_read(final, late_blocks, edges, weight, taps, read, newest_output_switch, cut)
    for level in range(group_devices.bit_length() - 1):
        group_sq = group_sq + flip_permute(group_sq, 2**level)
    out = last_rows(final, values, keys, out, cut)
    scaled = gated * lax.rsqrt(group_sq[0, 0] / (repeats * HEAD) + EPS) * cluster_scaling_coefficients
    store = out.reshape(1, devices * span, heads, HEAD + STATE)
    return store, scaled.astype(BF16).reshape(1, heads, HEAD)


def solution(mesh):
    placed = (
        P(("gr", "tp"), "sp", None),
        P(),
        P(),
        P(),
        P("sp"),
        P("sp"),
        P(("gr", "tp"), "sp", None),
        P(None, "sp", None),
        P(),
        P(("gr", "tp"), None, None),
        P(("gr", "tp"), "sp", None),
        P("sp", None),
    )

    return jax.shard_map(
        on_device,
        mesh=mesh,
        in_specs=placed,
        out_specs=(P(("gr", "tp"), None, "sp", None), P(("gr", "tp"), "sp", None)),
        check_vma=False,
    )
```

```python
import jax
import jax.numpy as jnp
from jax import lax
from jax.experimental import pallas as pl
from jax.experimental.pallas import tpu as pltpu
from jax.sharding import PartitionSpec as P


HEADS = 16
HEAD = 64
GROUPS = 4
STATE = 64
LANES = 128
EXTRA = 8
TILE_ROWS = 16
VMEM_LIMIT = 24 * 2**20
EPS = 1e-05
F32 = jnp.float32
BF16 = jnp.bfloat16


def silu(x):
    return 0.5 * x * (1.0 + jnp.tanh(0.5 * x))


def rounded(x):
    return x.astype(BF16).astype(F32)


def lane_index(shape):
    return lax.broadcasted_iota(jnp.int32, shape, 1)


def whole(shape):
    return pl.BlockSpec(shape, lambda *_: (0,) * len(shape))


def on_chip(x):
    return pltpu.with_memory_space_constraint(x, pltpu.VMEM)


def off_chip(x):
    return pltpu.with_memory_space_constraint(x, pltpu.HBM)


def flip_permute(value, flip):
    pairs = [(source, source ^ flip) for source in range(lax.axis_size("sp"))]
    return lax.ppermute(value, "sp", pairs)


def key_block_kernel(group_devices, low_ref, high_ref, wk_ref, *rest):
    outs, packed = rest[:-1], rest[-1]
    step = pl.program_id(0)
    rows = low_ref.shape[0]
    both = jnp.concatenate([low_ref[...], high_ref[...]], axis=0)
    k_both = rounded(jnp.dot(both, wk_ref[...], preferred_element_type=F32))
    k_low, k_high = k_both[:rows], k_both[rows:]
    left = lane_index((rows, LANES)) < STATE
    for group in range(GROUPS):
        column = slice(group // 2 * LANES, (group // 2 + 1) * LANES)
        a, b = k_low[:, column], k_high[:, column]
        if group % 2 == 0:
            b = pltpu.roll(b, STATE, 1)
        else:
            a = pltpu.roll(a, STATE, 1)
        packed[group, pl.ds(pl.multiple_of(step * rows, rows), rows), :] = jnp.where(left, a, b).astype(BF16)

    @pl.when(step == pl.num_programs(0) - 1)
    def _():
        own = lax.axis_index("sp") // group_devices
        for offset, out in enumerate(outs):
            out[...] = packed[own ^ offset]


def key_blocks(rows, wk, group_devices):
    span, model = rows.shape
    half = span // 2
    tile = half // 2
    steps = half // tile
    block = jax.ShapeDtypeStruct((half, LANES), BF16)
    return pl.pallas_call(
        lambda *refs: key_block_kernel(group_devices, *refs),
        grid=(steps,),
        in_specs=[
            pl.BlockSpec((tile, model), lambda i: (i, 0)),
            pl.BlockSpec((tile, model), lambda i: (i + steps, 0)),
            whole(wk.shape),
        ],
        out_specs=[whole(block.shape)] * GROUPS,
        out_shape=[block] * GROUPS,
        scratch_shapes=[pltpu.VMEM((GROUPS,) + block.shape, BF16)],
        compiler_params=pltpu.CompilerParams(vmem_limit_bytes=VMEM_LIMIT),
        cost_estimate=pl.CostEstimate(
            flops=2 * span * model * GROUPS * STATE, bytes_accessed=2 * span * model, transcendentals=0
        ),
        name="key_blocks",
    )(off_chip(rows), off_chip(rows), off_chip(wk))


def early_value_kernel(x_ref, after_ref, last_ref, other_ref, w_ref, wr_ref, _, *rest):
    outs, (kept, rates) = rest[:-2], rest[-2:]
    step = pl.program_id(0)
    share = kept.shape[2]
    devices = w_ref.shape[1] // share
    rows = x_ref.shape[0]
    x = jnp.concatenate([x_ref[...], after_ref[...], last_ref[...]], axis=0)
    y = jnp.dot(x, w_ref[...], preferred_element_type=F32)
    last = y.shape[0]
    half = EXTRA // 2
    extra = jnp.concatenate([y[rows : rows + half], y[last - half :]], axis=0)
    for device in range(devices):
        lanes = slice(device * share, (device + 1) * share)
        index = step * devices + device
        kept[index, :rows, :] = y[:rows, lanes].astype(BF16)
        kept[index, kept.shape[1] - EXTRA :, :] = extra[:, lanes].astype(BF16)
    part = other_ref.shape[0]
    pieces = part // share
    own_rows = x_ref[pl.ds(pl.multiple_of(step * part, part), part), :]
    both = jnp.concatenate([own_rows, other_ref[...]], axis=0)
    r = lax.dot_general(both, wr_ref[...], (((1,), (1,)), ((), ())), preferred_element_type=F32).astype(BF16)
    eye = (
        lax.broadcasted_iota(jnp.int32, (HEADS, HEADS), 0) == lax.broadcasted_iota(jnp.int32, (HEADS, HEADS), 1)
    ).astype(BF16)
    turned = lax.dot_general(eye, r, (((1,), (1,)), ((), ())), preferred_element_type=F32)
    count = rates.shape[0]
    for piece in range(pieces):
        rates[step * pieces + piece] = turned[:, piece * share : (piece + 1) * share]
        rates[count // 2 + step * pieces + piece] = turned[:, part + piece * share : part + (piece + 1) * share]

    @pl.when(step == pl.num_programs(0) - 1)
    def _():
        heads = share // HEAD
        for device in range(kept.shape[0]):
            tile = [rates[t, h : h + 1, :] for h in range(device * heads, (device + 1) * heads) for t in range(count)]
            kept[device, rows : rows + heads * count, :] = jnp.concatenate(tile, axis=0).astype(BF16)
        own = lax.axis_index("sp")
        for offset, out in enumerate(outs):
            out[...] = kept[own ^ offset]


def early_values(rows, wv, wr, started, devices, cut):
    span, model = rows.shape
    width = wv.shape[1]
    share = width // devices
    tile = max(2 * LANES, share)
    steps = width // tile
    part = cut // steps
    block = (cut + span // HEAD + EXTRA, share)
    x = off_chip(rows)
    return pl.pallas_call(
        early_value_kernel,
        grid=(steps,),
        in_specs=[
            whole((cut, model)),
            pl.BlockSpec((TILE_ROWS, model), lambda i: (cut // TILE_ROWS, 0)),
            pl.BlockSpec((TILE_ROWS, model), lambda i: (span // TILE_ROWS - 1, 0)),
            pl.BlockSpec((part, model), lambda i: (cut // part + i, 0)),
            pl.BlockSpec((model, tile), lambda i: (0, i)),
            whole(wr.shape),
            pl.BlockSpec(memory_space=pl.ANY),
        ],
        out_specs=[whole(block)] * devices,
        out_shape=[jax.ShapeDtypeStruct(block, BF16)] * devices,
        scratch_shapes=[pltpu.VMEM((devices,) + block, BF16), pltpu.VMEM((span // share, HEADS, share), F32)],
        compiler_params=pltpu.CompilerParams(vmem_limit_bytes=VMEM_LIMIT),
        cost_estimate=pl.CostEstimate(
            flops=2 * cut * model * width, bytes_accessed=2 * (span * model + model * width), transcendentals=0
        ),
        name="early_values",
    )(x, x, x, x, off_chip(wv), off_chip(wr), started)


def late_value_kernel(x_ref, w_ref, _, *rest):
    outs, kept = rest[:-1], rest[-1]
    step = pl.program_id(0)
    share = kept.shape[2]
    devices = w_ref.shape[1] // share
    y = jnp.dot(x_ref[...], w_ref[...], preferred_element_type=F32)
    for device in range(devices):
        kept[step * devices + device] = y[:, device * share : (device + 1) * share].astype(BF16)

    @pl.when(step == pl.num_programs(0) - 1)
    def _():
        own = lax.axis_index("sp")
        for offset, out in enumerate(outs):
            out[...] = kept[own ^ offset]


def late_values(rows, wv, started, devices, cut):
    span, model = rows.shape
    width = wv.shape[1]
    share = width // devices
    tile = max(2 * LANES, share)
    late = span - cut
    block = (late, share)
    return pl.pallas_call(
        late_value_kernel,
        grid=(width // tile,),
        in_specs=[
            pl.BlockSpec((late, model), lambda i: (cut // late, 0)),
            pl.BlockSpec((model, tile), lambda i: (0, i)),
            pl.BlockSpec(memory_space=pl.ANY),
        ],
        out_specs=[whole(block)] * devices,
        out_shape=[jax.ShapeDtypeStruct(block, BF16)] * devices,
        scratch_shapes=[pltpu.VMEM((devices,) + block, BF16)],
        compiler_params=pltpu.CompilerParams(vmem_limit_bytes=VMEM_LIMIT),
        cost_estimate=pl.CostEstimate(
            flops=2 * late * model * width, bytes_accessed=2 * (late * model + model * width), transcendentals=0
        ),
        name="late_values",
    )(off_chip(rows), off_chip(wv), started)


def key_read_kernel(group_devices, *refs):
    count = GROUPS * group_devices
    held = refs[:count]
    taps_ref, query_ref, keys_ref, score_ref, blocks, line = refs[count:]
    sources = blocks.shape[0]
    half = blocks.shape[1]
    tiles = 2 * half // LANES
    me = lax.axis_index("sp")
    group, rank = me // group_devices, me % group_devices
    for offset in range(GROUPS):
        for shift in range(group_devices):
            blocks[(group ^ offset) * group_devices + (rank ^ shift)] = held[shift * GROUPS + offset][...]
    taps = []
    for k in range(5):
        tap = taps_ref[k, pl.ds(group, 1), :]
        taps.append(jnp.concatenate([tap, tap], axis=1))
    asked = query_ref[0].astype(F32)
    asked = jnp.where(lax.broadcasted_iota(jnp.int32, asked.shape, 0) == group, asked, 0.0)
    asked = jnp.sum(asked, axis=0, keepdims=True)
    asked = jnp.broadcast_to(jnp.concatenate([asked, asked], axis=1), (16, LANES))
    part_row = lax.broadcasted_iota(jnp.int32, (16, LANES), 0)
    query = jnp.where(part_row == lane_index((16, LANES)) // STATE, asked, 0.0).astype(BF16)
    edge_left = lane_index((16, LANES)) < STATE
    left = lane_index((half, LANES)) < STATE

    def one_source(source, carry):
        body = blocks[source, :half, :].astype(F32)
        before = blocks[jnp.maximum(source - 1, 0), half - 16 : half, :].astype(F32)
        after = blocks[jnp.minimum(source + 1, sources - 1), :16, :].astype(F32)
        before = jnp.where(source > 0, before, 0.0)
        after = jnp.where(source < sources - 1, after, 0.0)
        top = jnp.where(edge_left, pltpu.roll(before, STATE, 1), pltpu.roll(body[half - 16 :], STATE, 1))
        bottom = jnp.where(edge_left, pltpu.roll(body[:16], STATE, 1), pltpu.roll(after, STATE, 1))
        line[0:16, :] = top
        line[16 : 16 + half, :] = body
        line[16 + half :, :] = bottom
        total = taps[0] * line[14 : 14 + half, :]
        for k in range(1, 5):
            total = total + taps[k] * line[14 + k : 14 + k + half, :]
        y = silu(total).astype(BF16)
        score = lax.dot_general(query, y, (((1,), (1,)), ((), ())), preferred_element_type=F32)
        score_ref[source] = jnp.concatenate(
            [score[part : part + 1, c * LANES : (c + 1) * LANES] for part in range(2) for c in range(tiles // 2)],
            axis=0,
        )
        z = y.astype(F32)
        turned = pltpu.roll(z, STATE, 1)
        keys_ref[source, :half, :] = jnp.where(left, z, turned).astype(BF16)
        keys_ref[source, half:, :] = jnp.where(left, turned, z).astype(BF16)
        return carry

    lax.fori_loop(0, sources, one_source, 0)


def key_read(held, taps, query, group_devices, span):
    sources = len(held)
    vmem = pl.BlockSpec(memory_space=pltpu.VMEM)
    inputs = [*held, taps, query]
    return pl.pallas_call(
        lambda *refs: key_read_kernel(group_devices, *refs),
        in_specs=[vmem] * len(inputs),
        out_specs=[vmem, vmem],
        out_shape=[
            jax.ShapeDtypeStruct((sources, span, LANES), BF16),
            jax.ShapeDtypeStruct((sources, span // LANES, LANES), F32),
        ],
        scratch_shapes=[
            pltpu.VMEM((sources,) + held[0].shape, BF16),
            pltpu.VMEM((span // 2 + 32, LANES), F32),
        ],
        compiler_params=pltpu.CompilerParams(vmem_limit_bytes=VMEM_LIMIT),
        cost_estimate=pl.CostEstimate(flops=10**9, bytes_accessed=4 * 10**6, transcendentals=10**6),
        name="key_read",
    )(*(on_chip(x) for x in inputs))


def read_weights(blocks, cut, score_ref, offset_ref, decay_ref, spikes_ref, spikes, weight_ref):
    sources, tiles = score_ref.shape[:2]
    share = blocks.shape[2]
    heads = share // HEAD
    count = sources * tiles
    lane_row = lax.broadcasted_iota(jnp.int32, (LANES, LANES), 0)
    lane_col = lax.broadcasted_iota(jnp.int32, (LANES, LANES), 1)
    later_lanes = (lane_row > lane_col).astype(F32)
    row = lax.broadcasted_iota(jnp.int32, (count, count), 0)
    col = lax.broadcasted_iota(jnp.int32, (count, count), 1)
    later_rows = (col > row).astype(F32)
    score = score_ref[...].reshape(count, LANES)
    for h in range(heads):
        for c in range(count):
            spikes[h, c : c + 1, :] = spikes_ref[0, h : h + 1, c * LANES : (c + 1) * LANES]
    exact = dict(preferred_element_type=F32, precision=lax.Precision.HIGHEST)
    pieces = LANES // share
    for h in range(heads):
        rates = []
        for source in range(sources):
            sent = blocks[source, cut : cut + heads * tiles * pieces, :]
            if pieces == 1:
                rates.append(sent.astype(F32)[h * tiles : (h + 1) * tiles])
            else:
                picks = []
                for piece in range(pieces):
                    wanted = lax.broadcasted_iota(jnp.int32, (tiles, sent.shape[0]), 0)
                    column = lax.broadcasted_iota(jnp.int32, (tiles, sent.shape[0]), 1)
                    pick = (column == (h * tiles + wanted) * pieces + piece).astype(BF16)
                    picks.append(jnp.dot(pick, sent, preferred_element_type=F32))
                rates.append(jnp.concatenate(picks, axis=1))
        raw = jnp.concatenate(rates, axis=0) + offset_ref[h]
        rate = jnp.maximum(raw, 0.0) + jnp.log1p(jnp.exp(-jnp.abs(raw)))
        decay = jnp.exp(jnp.full((1, LANES), decay_ref[h], F32))
        step = spikes[h] - decay * rate
        within = jnp.dot(step, later_lanes, **exact)
        totals = jnp.broadcast_to(jnp.sum(step, axis=1, keepdims=True), (count, LANES))
        ahead = within + jnp.dot(later_rows, totals, **exact)
        weight = rate * jnp.exp(ahead) * score
        high = rounded(weight)
        weight_ref[:, h] = high.reshape(sources, tiles, LANES)
        weight_ref[:, heads + h] = (weight - high).reshape(sources, tiles, LANES)


def convolved(line, body, before, after, taps_ref, weight_ref, source, start_row, total):
    rows, share = body.shape
    heads = share // HEAD
    line[0:8, :] = before
    line[8 : 8 + rows, :] = body
    line[8 + rows :, :] = after
    taps = [jnp.concatenate([taps_ref[k, h : h + 1, :] for h in range(heads)], axis=1) for k in range(5)]
    tiles = weight_ref.shape[2]
    weight = weight_ref[source].reshape(-1, LANES)
    tile_of = lax.broadcasted_iota(jnp.int32, weight.shape, 0) % tiles
    read = jnp.zeros(total.shape, F32)
    values = []
    for tile in range(rows // LANES):
        start = tile * LANES
        y = taps[0] * line[6 + start : 6 + start + LANES, :]
        for k in range(1, 5):
            y = y + taps[k] * line[6 + k + start : 6 + k + start + LANES, :]
        y = silu(y).astype(BF16)
        masked = jnp.where(tile_of == start_row // LANES + tile, weight, 0.0).astype(BF16)
        read = read + jnp.dot(masked, y, preferred_element_type=F32)
        values.append(y)
    total[...] += read
    return values


def wove(woven, values, keys_ref, source, start_row, out_ref):
    share = values[0].shape[1]
    heads = share // HEAD
    left = lane_index((LANES, LANES)) < HEAD
    for tile, y in enumerate(values):
        start = tile * LANES
        keys = keys_ref[source, start_row + start : start_row + start + LANES, :].astype(F32)
        z = y.astype(F32)
        if share == LANES:
            pieces = [jnp.where(left, z, keys), jnp.where(left, pltpu.roll(z, HEAD, 1), keys)]
        else:
            pieces = [
                jnp.concatenate([z[:, h * HEAD : (h + 1) * HEAD], keys[:, STATE:]], axis=1) for h in range(heads)
            ]
        for h, piece in enumerate(pieces):
            woven[pl.ds(heads * start + h, LANES, heads), :] = piece
        part = slice(heads * start, heads * (start + LANES))
        out_ref[0, part, :] = woven[part, :].astype(BF16)


def line_scratch(rows, share):
    return pltpu.VMEM((rows + 16, share), F32)


def woven_scratch(rows, share):
    return pltpu.VMEM((share // HEAD * rows, LANES), F32)


def early_kernel(cut, *refs):
    blocks, refs = refs[:-15], refs[-15:]
    keys_ref, score_ref, taps_ref, spikes_ref, offset_ref, decay_ref = refs[:6]
    out_ref, read_ref, edges_ref, weight_ref, kept, line, woven, total, spikes = refs[6:]
    source = pl.program_id(0)
    own = lax.axis_index("sp")

    @pl.when(source == 0)
    def _():
        total[...] = jnp.zeros_like(total)
        for offset, block_ref in enumerate(blocks):
            kept[own ^ offset] = block_ref[...]
            edges_ref[own ^ offset, :TILE_ROWS, :] = block_ref[:TILE_ROWS, :]
            edges_ref[own ^ offset, TILE_ROWS:, :] = block_ref[cut - TILE_ROWS : cut, :]
        read_weights(kept, cut, score_ref, offset_ref, decay_ref, spikes_ref, spikes, weight_ref)

    block = kept[source].astype(F32)
    before = kept[jnp.maximum(source - 1, 0), kept.shape[1] - EXTRA :, :].astype(F32)
    before = jnp.where(source > 0, before, 0.0)
    beside = block[block.shape[0] - EXTRA :]
    values = convolved(line, block[:cut], before, beside, taps_ref, weight_ref, source, 0, total)
    wove(woven, values, keys_ref, source, 0, out_ref)
    read_ref[...] = total[...]


def early_rows(blocks, keys, score, taps, spikes, offset, decay, cut):
    sources, span = keys.shape[:2]
    height, share = blocks[0].shape
    heads = share // HEAD
    tiles = span // LANES
    reads = 2 * heads * tiles
    edges = (sources, 2 * TILE_ROWS, share)
    vmem = pl.BlockSpec(memory_space=pltpu.VMEM)
    smem = pl.BlockSpec(memory_space=pltpu.SMEM)
    inputs = [*blocks, keys, score, taps, spikes]
    weight = (sources, 2 * heads, tiles, LANES)
    return pl.pallas_call(
        lambda *refs: early_kernel(cut, *refs),
        grid=(sources,),
        in_specs=[vmem] * len(inputs) + [smem, smem],
        out_specs=[
            pl.BlockSpec((1, heads * cut, LANES), lambda s: (s, 0, 0)),
            whole((reads, share)),
            whole(edges),
            whole(weight),
        ],
        out_shape=[
            jax.ShapeDtypeStruct((sources, heads * span, LANES), BF16),
            jax.ShapeDtypeStruct((reads, share), F32),
            jax.ShapeDtypeStruct(edges, BF16),
            jax.ShapeDtypeStruct(weight, F32),
        ],
        scratch_shapes=[
            pltpu.VMEM((sources, height, share), BF16),
            line_scratch(cut, share),
            woven_scratch(cut, share),
            pltpu.VMEM((reads, share), F32),
            pltpu.VMEM((heads, sources * tiles, LANES), F32),
        ],
        compiler_params=pltpu.CompilerParams(vmem_limit_bytes=VMEM_LIMIT),
        cost_estimate=pl.CostEstimate(flops=2 * 10**9, bytes_accessed=6 * 10**6, transcendentals=10**6),
        name="early_rows",
    )(*(on_chip(x) for x in inputs), offset, decay)


def late_values_of(offset, block_ref, edges_ref, taps_ref, weight_ref, line, total, cut):
    source = lax.axis_index("sp") ^ offset
    sources = edges_ref.shape[0]
    before = edges_ref[source, TILE_ROWS:, :].astype(F32)[TILE_ROWS - 8 :]
    after = edges_ref[jnp.minimum(source + 1, sources - 1), :TILE_ROWS, :].astype(F32)[:8]
    after = jnp.where(source < sources - 1, after, 0.0)
    body = block_ref[...].astype(F32)
    return convolved(line, body, before, after, taps_ref, weight_ref, source, cut, total)


def late_kernel(cut, offsets, *refs):
    count = len(offsets)
    blocks = refs[:count]
    edges_ref, keys_ref, weight_ref, taps_ref, read_ref, _, out_ref, total, line, woven = refs[count:]
    step = pl.program_id(0)

    @pl.when(step == 0)
    def _():
        total[...] = read_ref[...]

    for index, offset in enumerate(offsets):

        @pl.when(step == index)
        def _(index=index, offset=offset):
            values = late_values_of(offset, blocks[index], edges_ref, taps_ref, weight_ref, line, total, cut)
            wove(woven, values, keys_ref, lax.axis_index("sp") ^ offset, cut, out_ref)


def wave_offset(step, offsets):
    offset = step + offsets[0]
    for index in range(1, len(offsets)):
        gap = offsets[index] - offsets[index - 1] - 1
        if gap:
            offset = offset + gap * (step >= index).astype(jnp.int32)
    return offset


def late_out_spec(offsets, shape):
    rows = shape[1] // 2
    return pl.BlockSpec((1, rows, LANES), lambda i: (lax.axis_index("sp") ^ wave_offset(i, offsets), 1, 0))


def late_rows(offsets, late, edges, keys, weight, taps, read, out, cut):
    rows, share = late[0].shape
    vmem = pl.BlockSpec(memory_space=pltpu.VMEM)
    inputs = [late[k] for k in offsets] + [edges, keys, weight, taps, read]
    return pl.pallas_call(
        lambda *refs: late_kernel(cut, offsets, *refs),
        grid=(len(offsets),),
        in_specs=[vmem] * len(inputs) + [pl.BlockSpec(memory_space=pl.ANY)],
        out_specs=[late_out_spec(offsets, out.shape), whole(read.shape)],
        out_shape=[jax.ShapeDtypeStruct(out.shape, BF16), jax.ShapeDtypeStruct(read.shape, F32)],
        scratch_shapes=[line_scratch(rows, share), woven_scratch(rows, share)],
        input_output_aliases={len(inputs): 0},
        compiler_params=pltpu.CompilerParams(vmem_limit_bytes=VMEM_LIMIT),
        cost_estimate=pl.CostEstimate(flops=10**9, bytes_accessed=2 * 10**6, transcendentals=10**6),
        name="late_rows",
    )(*(on_chip(x) for x in inputs), out)


def last_read_kernel(cut, offsets, *refs):
    count = len(offsets)
    blocks = refs[:count]
    edges_ref, weight_ref, taps_ref, read_ref, gate_ref, values_ref, gated_ref, square_ref, line, total = refs[count:]
    total[...] = read_ref[...]
    for index, offset in enumerate(offsets):
        part = line.at[index]
        values = late_values_of(offset, blocks[index], edges_ref, taps_ref, weight_ref, part, total, cut)
        for tile, y in enumerate(values):
            values_ref[index, tile * LANES : (tile + 1) * LANES, :] = y
    tiles = weight_ref.shape[2]
    shape = total.shape
    heads = shape[1] // HEAD
    head = (lax.broadcasted_iota(jnp.int32, shape, 0) // tiles) % heads
    mine = head == lane_index(shape) // HEAD
    read = jnp.sum(jnp.where(mine, total[...], 0.0), axis=0, keepdims=True)
    read = jnp.concatenate([read[:, h * HEAD : (h + 1) * HEAD] for h in range(heads)], axis=0)
    gated = read * silu(gate_ref[0].astype(F32))
    gated_ref[...] = gated
    square = jnp.sum(jnp.sum(gated * gated, axis=1, keepdims=True), axis=0, keepdims=True)
    square_ref[...] = jnp.broadcast_to(square, square_ref.shape)


def last_read(offsets, late, edges, weight, taps, read, gate, cut):
    rows, share = late[0].shape
    vmem = pl.BlockSpec(memory_space=pltpu.VMEM)
    inputs = [late[k] for k in offsets] + [edges, weight, taps, read, gate]
    return pl.pallas_call(
        lambda *refs: last_read_kernel(cut, offsets, *refs),
        in_specs=[vmem] * len(inputs),
        out_specs=[vmem] * 3,
        out_shape=[
            jax.ShapeDtypeStruct((len(offsets), rows, share), BF16),
            jax.ShapeDtypeStruct((share // HEAD, HEAD), F32),
            jax.ShapeDtypeStruct((1, LANES), F32),
        ],
        scratch_shapes=[pltpu.VMEM((len(offsets), rows + 16, share), F32), pltpu.VMEM(read.shape, F32)],
        compiler_params=pltpu.CompilerParams(vmem_limit_bytes=VMEM_LIMIT),
        cost_estimate=pl.CostEstimate(flops=10**9, bytes_accessed=10**6, transcendentals=10**6),
        name="last_read",
    )(*(on_chip(x) for x in inputs))


def last_rows_kernel(cut, offsets, values_ref, keys_ref, _, out_ref, woven):
    step = pl.program_id(0)
    rows = values_ref.shape[1]
    values = [values_ref[step, start : start + LANES, :] for start in range(0, rows, LANES)]
    wove(woven, values, keys_ref, lax.axis_index("sp") ^ wave_offset(step, offsets), cut, out_ref)


def last_rows(offsets, values, keys, out, cut):
    rows, share = values.shape[1:]
    vmem = pl.BlockSpec(memory_space=pltpu.VMEM)
    return pl.pallas_call(
        lambda *refs: last_rows_kernel(cut, offsets, *refs),
        grid=(len(offsets),),
        in_specs=[vmem, vmem, pl.BlockSpec(memory_space=pl.ANY)],
        out_specs=late_out_spec(offsets, out.shape),
        out_shape=jax.ShapeDtypeStruct(out.shape, BF16),
        scratch_shapes=[woven_scratch(rows, share)],
        input_output_aliases={2: 0},
        compiler_params=pltpu.CompilerParams(vmem_limit_bytes=VMEM_LIMIT),
        cost_estimate=pl.CostEstimate(flops=10**9, bytes_accessed=2 * 10**6, transcendentals=0),
        name="last_rows",
    )(on_chip(values), on_chip(keys), out)


def on_device(
    context_input_tensor,
    content_mapping_matrix,
    address_mapping_matrix,
    increment_mapping_matrix,
    increment_speed_offset,
    channel_fading_exponent,
    extra_damping_spikes,
    content_smoothing_coefficients,
    address_smoothing_coefficients,
    newest_lookup_matrix,
    newest_output_switch,
    cluster_scaling_coefficients,
):
    rows = context_input_tensor[0]
    span = rows.shape[0]
    repeats = HEADS // GROUPS
    heads = increment_speed_offset.shape[0]
    group_devices = repeats // heads
    devices = lax.axis_size("sp")
    cut = span // 2

    blocks = key_blocks(rows, address_mapping_matrix, group_devices)
    direct = [None] * (GROUPS - 1)
    for offset in range(1, GROUPS):
        direct[offset - 1] = flip_permute(blocks[offset], offset * group_devices)
    early = early_values(rows, content_mapping_matrix, increment_mapping_matrix.T, blocks[0], devices, cut)
    late = late_values(rows, content_mapping_matrix, early[0], devices, cut)
    held = [blocks[0]] + direct
    relayed = []
    for shift in range(1, group_devices):
        for offset in range(GROUPS):
            relayed.append(flip_permute(held[offset], shift))
    early_blocks, late_blocks = [early[0]], [late[0]]
    for offset in range(1, devices):
        early_blocks.append(flip_permute(early[offset], offset))
        late_blocks.append(flip_permute(late[offset], offset))

    keys, score = key_read(held + relayed, address_smoothing_coefficients, newest_lookup_matrix, group_devices, span)
    taps = content_smoothing_coefficients
    out, read, edges, weight = early_rows(
        early_blocks,
        keys,
        score,
        taps,
        extra_damping_spikes,
        increment_speed_offset,
        channel_fading_exponent,
        cut,
    )
    half = devices // 2
    first = list(range(half))
    middle = [offset for offset in range(half, devices) if offset % group_devices == 0]
    final = [offset for offset in range(half, devices) if offset % group_devices]
    for wave in (first, middle):
        out, read = late_rows(wave, late_blocks, edges, keys, weight, taps, read, out, cut)
    values, gated, group_sq = last_read(final, late_blocks, edges, weight, taps, read, newest_output_switch, cut)
    for level in range(group_devices.bit_length() - 1):
        group_sq = group_sq + flip_permute(group_sq, 2**level)
    out = last_rows(final, values, keys, out, cut)
    scaled = gated * lax.rsqrt(group_sq[0, 0] / (repeats * HEAD) + EPS) * cluster_scaling_coefficients
    store = out.reshape(1, devices * span, heads, HEAD + STATE)
    return store, scaled.astype(BF16).reshape(1, heads, HEAD)


def solution(mesh):
    placed = (
        P(("gr", "tp"), "sp", None),
        P(),
        P(),
        P(),
        P("sp"),
        P("sp"),
        P(("gr", "tp"), "sp", None),
        P(None, "sp", None),
        P(),
        P(("gr", "tp"), None, None),
        P(("gr", "tp"), "sp", None),
        P("sp", None),
    )

    return jax.shard_map(
        on_device,
        mesh=mesh,
        in_specs=placed,
        out_specs=(P(("gr", "tp"), None, "sp", None), P(("gr", "tp"), "sp", None)),
        check_vma=False,
    )
```

```python
import jax
import jax.numpy as jnp
from jax import lax
from jax.experimental import pallas as pl
from jax.experimental.pallas import tpu as pltpu
from jax.sharding import PartitionSpec as P


HEADS = 16
HEAD = 64
GROUPS = 4
STATE = 64
LANES = 128
EXTRA = 8
TILE_ROWS = 16
VMEM_LIMIT = 24 * 2**20
EPS = 1e-05
F32 = jnp.float32
BF16 = jnp.bfloat16


def silu(x):
    return 0.5 * x * (1.0 + jnp.tanh(0.5 * x))


def rounded(x):
    return x.astype(BF16).astype(F32)


def lane_index(shape):
    return lax.broadcasted_iota(jnp.int32, shape, 1)


def whole(shape):
    return pl.BlockSpec(shape, lambda *_: (0,) * len(shape))


def on_chip(x):
    return pltpu.with_memory_space_constraint(x, pltpu.VMEM)


def off_chip(x):
    return pltpu.with_memory_space_constraint(x, pltpu.HBM)


def flip_permute(value, flip):
    pairs = [(source, source ^ flip) for source in range(lax.axis_size("sp"))]
    return lax.ppermute(value, "sp", pairs)


def key_block_kernel(group_devices, low_ref, high_ref, wk_ref, *rest):
    outs, packed = rest[:-1], rest[-1]
    step = pl.program_id(0)
    rows = low_ref.shape[0]
    both = jnp.concatenate([low_ref[...], high_ref[...]], axis=0)
    k_both = rounded(jnp.dot(both, wk_ref[...], preferred_element_type=F32))
    k_low, k_high = k_both[:rows], k_both[rows:]
    left = lane_index((rows, LANES)) < STATE
    for group in range(GROUPS):
        column = slice(group // 2 * LANES, (group // 2 + 1) * LANES)
        a, b = k_low[:, column], k_high[:, column]
        if group % 2 == 0:
            b = pltpu.roll(b, STATE, 1)
        else:
            a = pltpu.roll(a, STATE, 1)
        packed[group, pl.ds(pl.multiple_of(step * rows, rows), rows), :] = jnp.where(left, a, b).astype(BF16)

    @pl.when(step == pl.num_programs(0) - 1)
    def _():
        own = lax.axis_index("sp") // group_devices
        for offset, out in enumerate(outs):
            out[...] = packed[own ^ offset]


def key_blocks(rows, wk, group_devices):
    span, model = rows.shape
    half = span // 2
    tile = half // 2
    steps = half // tile
    block = jax.ShapeDtypeStruct((half, LANES), BF16)
    return pl.pallas_call(
        lambda *refs: key_block_kernel(group_devices, *refs),
        grid=(steps,),
        in_specs=[
            pl.BlockSpec((tile, model), lambda i: (i, 0)),
            pl.BlockSpec((tile, model), lambda i: (i + steps, 0)),
            whole(wk.shape),
        ],
        out_specs=[whole(block.shape)] * GROUPS,
        out_shape=[block] * GROUPS,
        scratch_shapes=[pltpu.VMEM((GROUPS,) + block.shape, BF16)],
        compiler_params=pltpu.CompilerParams(vmem_limit_bytes=VMEM_LIMIT),
        cost_estimate=pl.CostEstimate(
            flops=2 * span * model * GROUPS * STATE, bytes_accessed=2 * span * model, transcendentals=0
        ),
        name="key_blocks",
    )(off_chip(rows), off_chip(rows), off_chip(wk))


def early_value_kernel(x_ref, after_ref, last_ref, other_ref, w_ref, wr_ref, _, *rest):
    outs, (kept, rates) = rest[:-2], rest[-2:]
    step = pl.program_id(0)
    share = kept.shape[2]
    devices = w_ref.shape[1] // share
    rows = x_ref.shape[0]
    x = jnp.concatenate([x_ref[...], after_ref[...], last_ref[...]], axis=0)
    y = jnp.dot(x, w_ref[...], preferred_element_type=F32)
    last = y.shape[0]
    half = EXTRA // 2
    extra = jnp.concatenate([y[rows : rows + half], y[last - half :]], axis=0)
    for device in range(devices):
        lanes = slice(device * share, (device + 1) * share)
        index = step * devices + device
        kept[index, :rows, :] = y[:rows, lanes].astype(BF16)
        kept[index, kept.shape[1] - EXTRA :, :] = extra[:, lanes].astype(BF16)
    part = other_ref.shape[0]
    pieces = part // share
    own_rows = x_ref[pl.ds(pl.multiple_of(step * part, part), part), :]
    both = jnp.concatenate([own_rows, other_ref[...]], axis=0)
    r = lax.dot_general(both, wr_ref[...], (((1,), (1,)), ((), ())), preferred_element_type=F32).astype(BF16)
    eye = (
        lax.broadcasted_iota(jnp.int32, (HEADS, HEADS), 0) == lax.broadcasted_iota(jnp.int32, (HEADS, HEADS), 1)
    ).astype(BF16)
    turned = lax.dot_general(eye, r, (((1,), (1,)), ((), ())), preferred_element_type=F32)
    count = rates.shape[0]
    for piece in range(pieces):
        rates[step * pieces + piece] = turned[:, piece * share : (piece + 1) * share]
        rates[count // 2 + step * pieces + piece] = turned[:, part + piece * share : part + (piece + 1) * share]

    @pl.when(step == pl.num_programs(0) - 1)
    def _():
        heads = share // HEAD
        for device in range(kept.shape[0]):
            tile = [rates[t, h : h + 1, :] for h in range(device * heads, (device + 1) * heads) for t in range(count)]
            kept[device, rows : rows + heads * count, :] = jnp.concatenate(tile, axis=0).astype(BF16)
        own = lax.axis_index("sp")
        for offset, out in enumerate(outs):
            out[...] = kept[own ^ offset]


def early_values(rows, wv, wr, started, devices, cut):
    span, model = rows.shape
    width = wv.shape[1]
    share = width // devices
    tile = max(2 * LANES, share)
    steps = width // tile
    part = cut // steps
    block = (cut + span // HEAD + EXTRA, share)
    x = off_chip(rows)
    return pl.pallas_call(
        early_value_kernel,
        grid=(steps,),
        in_specs=[
            whole((cut, model)),
            pl.BlockSpec((TILE_ROWS, model), lambda i: (cut // TILE_ROWS, 0)),
            pl.BlockSpec((TILE_ROWS, model), lambda i: (span // TILE_ROWS - 1, 0)),
            pl.BlockSpec((part, model), lambda i: (cut // part + i, 0)),
            pl.BlockSpec((model, tile), lambda i: (0, i)),
            whole(wr.shape),
            pl.BlockSpec(memory_space=pl.ANY),
        ],
        out_specs=[whole(block)] * devices,
        out_shape=[jax.ShapeDtypeStruct(block, BF16)] * devices,
        scratch_shapes=[pltpu.VMEM((devices,) + block, BF16), pltpu.VMEM((span // share, HEADS, share), F32)],
        compiler_params=pltpu.CompilerParams(vmem_limit_bytes=VMEM_LIMIT),
        cost_estimate=pl.CostEstimate(
            flops=2 * cut * model * width, bytes_accessed=2 * (span * model + model * width), transcendentals=0
        ),
        name="early_values",
    )(x, x, x, x, off_chip(wv), off_chip(wr), started)


def late_value_kernel(x_ref, w_ref, _, *rest):
    outs, kept = rest[:-1], rest[-1]
    step = pl.program_id(0)
    share = kept.shape[2]
    devices = w_ref.shape[1] // share
    y = jnp.dot(x_ref[...], w_ref[...], preferred_element_type=F32)
    for device in range(devices):
        kept[step * devices + device] = y[:, device * share : (device + 1) * share].astype(BF16)

    @pl.when(step == pl.num_programs(0) - 1)
    def _():
        own = lax.axis_index("sp")
        for offset, out in enumerate(outs):
            out[...] = kept[own ^ offset]


def late_values(rows, wv, started, devices, cut):
    span, model = rows.shape
    width = wv.shape[1]
    share = width // devices
    tile = max(2 * LANES, share)
    late = span - cut
    block = (late, share)
    return pl.pallas_call(
        late_value_kernel,
        grid=(width // tile,),
        in_specs=[
            pl.BlockSpec((late, model), lambda i: (cut // late, 0)),
            pl.BlockSpec((model, tile), lambda i: (0, i)),
            pl.BlockSpec(memory_space=pl.ANY),
        ],
        out_specs=[whole(block)] * devices,
        out_shape=[jax.ShapeDtypeStruct(block, BF16)] * devices,
        scratch_shapes=[pltpu.VMEM((devices,) + block, BF16)],
        compiler_params=pltpu.CompilerParams(vmem_limit_bytes=VMEM_LIMIT),
        cost_estimate=pl.CostEstimate(
            flops=2 * late * model * width, bytes_accessed=2 * (late * model + model * width), transcendentals=0
        ),
        name="late_values",
    )(off_chip(rows), off_chip(wv), started)


def key_read_kernel(group_devices, *refs):
    count = GROUPS * group_devices
    held = refs[:count]
    taps_ref, query_ref, keys_ref, score_ref, blocks, line = refs[count:]
    sources = blocks.shape[0]
    half = blocks.shape[1]
    tiles = 2 * half // LANES
    me = lax.axis_index("sp")
    group, rank = me // group_devices, me % group_devices
    for offset in range(GROUPS):
        for shift in range(group_devices):
            blocks[(group ^ offset) * group_devices + (rank ^ shift)] = held[shift * GROUPS + offset][...]
    taps = []
    for k in range(5):
        tap = taps_ref[k, pl.ds(group, 1), :]
        taps.append(jnp.concatenate([tap, tap], axis=1))
    asked = query_ref[0].astype(F32)
    asked = jnp.where(lax.broadcasted_iota(jnp.int32, asked.shape, 0) == group, asked, 0.0)
    asked = jnp.sum(asked, axis=0, keepdims=True)
    asked = jnp.broadcast_to(jnp.concatenate([asked, asked], axis=1), (16, LANES))
    part_row = lax.broadcasted_iota(jnp.int32, (16, LANES), 0)
    query = jnp.where(part_row == lane_index((16, LANES)) // STATE, asked, 0.0).astype(BF16)
    edge_left = lane_index((16, LANES)) < STATE
    left = lane_index((half, LANES)) < STATE

    def one_source(source, carry):
        body = blocks[source, :half, :].astype(F32)
        before = blocks[jnp.maximum(source - 1, 0), half - 16 : half, :].astype(F32)
        after = blocks[jnp.minimum(source + 1, sources - 1), :16, :].astype(F32)
        before = jnp.where(source > 0, before, 0.0)
        after = jnp.where(source < sources - 1, after, 0.0)
        top = jnp.where(edge_left, pltpu.roll(before, STATE, 1), pltpu.roll(body[half - 16 :], STATE, 1))
        bottom = jnp.where(edge_left, pltpu.roll(body[:16], STATE, 1), pltpu.roll(after, STATE, 1))
        line[0:16, :] = top
        line[16 : 16 + half, :] = body
        line[16 + half :, :] = bottom
        total = taps[0] * line[14 : 14 + half, :]
        for k in range(1, 5):
            total = total + taps[k] * line[14 + k : 14 + k + half, :]
        y = silu(total).astype(BF16)
        score = lax.dot_general(query, y, (((1,), (1,)), ((), ())), preferred_element_type=F32)
        score_ref[source] = jnp.concatenate(
            [score[part : part + 1, c * LANES : (c + 1) * LANES] for part in range(2) for c in range(tiles // 2)],
            axis=0,
        )
        z = y.astype(F32)
        turned = pltpu.roll(z, STATE, 1)
        keys_ref[source, :half, :] = jnp.where(left, z, turned).astype(BF16)
        keys_ref[source, half:, :] = jnp.where(left, turned, z).astype(BF16)
        return carry

    lax.fori_loop(0, sources, one_source, 0)


def key_read(held, taps, query, group_devices, span):
    sources = len(held)
    vmem = pl.BlockSpec(memory_space=pltpu.VMEM)
    inputs = [*held, taps, query]
    return pl.pallas_call(
        lambda *refs: key_read_kernel(group_devices, *refs),
        in_specs=[vmem] * len(inputs),
        out_specs=[vmem, vmem],
        out_shape=[
            jax.ShapeDtypeStruct((sources, span, LANES), BF16),
            jax.ShapeDtypeStruct((sources, span // LANES, LANES), F32),
        ],
        scratch_shapes=[
            pltpu.VMEM((sources,) + held[0].shape, BF16),
            pltpu.VMEM((span // 2 + 32, LANES), F32),
        ],
        compiler_params=pltpu.CompilerParams(vmem_limit_bytes=VMEM_LIMIT),
        cost_estimate=pl.CostEstimate(flops=10**9, bytes_accessed=4 * 10**6, transcendentals=10**6),
        name="key_read",
    )(*(on_chip(x) for x in inputs))


def read_weights(blocks, cut, score_ref, offset_ref, decay_ref, spikes_ref, spikes, weight_ref):
    sources, tiles = score_ref.shape[:2]
    share = blocks.shape[2]
    heads = share // HEAD
    count = sources * tiles
    lane_row = lax.broadcasted_iota(jnp.int32, (LANES, LANES), 0)
    lane_col = lax.broadcasted_iota(jnp.int32, (LANES, LANES), 1)
    later_lanes = (lane_row > lane_col).astype(F32)
    row = lax.broadcasted_iota(jnp.int32, (count, count), 0)
    col = lax.broadcasted_iota(jnp.int32, (count, count), 1)
    later_rows = (col > row).astype(F32)
    score = score_ref[...].reshape(count, LANES)
    for h in range(heads):
        for c in range(count):
            spikes[h, c : c + 1, :] = spikes_ref[0, h : h + 1, c * LANES : (c + 1) * LANES]
    exact = dict(preferred_element_type=F32, precision=lax.Precision.HIGHEST)
    pieces = LANES // share
    for h in range(heads):
        rates = []
        for source in range(sources):
            sent = blocks[source, cut : cut + heads * tiles * pieces, :]
            if pieces == 1:
                rates.append(sent.astype(F32)[h * tiles : (h + 1) * tiles])
            else:
                picks = []
                for piece in range(pieces):
                    wanted = lax.broadcasted_iota(jnp.int32, (tiles, sent.shape[0]), 0)
                    column = lax.broadcasted_iota(jnp.int32, (tiles, sent.shape[0]), 1)
                    pick = (column == (h * tiles + wanted) * pieces + piece).astype(BF16)
                    picks.append(jnp.dot(pick, sent, preferred_element_type=F32))
                rates.append(jnp.concatenate(picks, axis=1))
        raw = jnp.concatenate(rates, axis=0) + offset_ref[h]
        rate = jnp.maximum(raw, 0.0) + jnp.log1p(jnp.exp(-jnp.abs(raw)))
        decay = jnp.exp(jnp.full((1, LANES), decay_ref[h], F32))
        step = spikes[h] - decay * rate
        within = jnp.dot(step, later_lanes, **exact)
        totals = jnp.broadcast_to(jnp.sum(step, axis=1, keepdims=True), (count, LANES))
        ahead = within + jnp.dot(later_rows, totals, **exact)
        weight = rate * jnp.exp(ahead) * score
        high = rounded(weight)
        weight_ref[:, h] = high.reshape(sources, tiles, LANES)
        weight_ref[:, heads + h] = (weight - high).reshape(sources, tiles, LANES)


def convolved(line, body, before, after, taps_ref, weight_ref, source, start_row, total):
    rows, share = body.shape
    heads = share // HEAD
    line[0:8, :] = before
    line[8 : 8 + rows, :] = body
    line[8 + rows :, :] = after
    taps = [jnp.concatenate([taps_ref[k, h : h + 1, :] for h in range(heads)], axis=1) for k in range(5)]
    tiles = weight_ref.shape[2]
    weight = weight_ref[source].reshape(-1, LANES)
    tile_of = lax.broadcasted_iota(jnp.int32, weight.shape, 0) % tiles
    read = jnp.zeros(total.shape, F32)
    values = []
    for tile in range(rows // LANES):
        start = tile * LANES
        y = taps[0] * line[6 + start : 6 + start + LANES, :]
        for k in range(1, 5):
            y = y + taps[k] * line[6 + k + start : 6 + k + start + LANES, :]
        y = silu(y).astype(BF16)
        masked = jnp.where(tile_of == start_row // LANES + tile, weight, 0.0).astype(BF16)
        read = read + jnp.dot(masked, y, preferred_element_type=F32)
        values.append(y)
    total[...] += read
    return values


def wove(woven, values, keys_ref, source, start_row, out_ref):
    share = values[0].shape[1]
    heads = share // HEAD
    left = lane_index((LANES, LANES)) < HEAD
    for tile, y in enumerate(values):
        start = tile * LANES
        keys = keys_ref[source, start_row + start : start_row + start + LANES, :].astype(F32)
        z = y.astype(F32)
        if share == LANES:
            pieces = [jnp.where(left, z, keys), jnp.where(left, pltpu.roll(z, HEAD, 1), keys)]
        else:
            pieces = [
                jnp.concatenate([z[:, h * HEAD : (h + 1) * HEAD], keys[:, STATE:]], axis=1) for h in range(heads)
            ]
        for h, piece in enumerate(pieces):
            woven[pl.ds(heads * start + h, LANES, heads), :] = piece
        part = slice(heads * start, heads * (start + LANES))
        out_ref[0, part, :] = woven[part, :].astype(BF16)


def line_scratch(rows, share):
    return pltpu.VMEM((rows + 16, share), F32)


def woven_scratch(rows, share):
    return pltpu.VMEM((share // HEAD * rows, LANES), F32)


def early_kernel(cut, *refs):
    blocks, refs = refs[:-15], refs[-15:]
    keys_ref, score_ref, taps_ref, spikes_ref, offset_ref, decay_ref = refs[:6]
    out_ref, read_ref, edges_ref, weight_ref, kept, line, woven, total, spikes = refs[6:]
    source = pl.program_id(0)
    own = lax.axis_index("sp")

    @pl.when(source == 0)
    def _():
        total[...] = jnp.zeros_like(total)
        for offset, block_ref in enumerate(blocks):
            kept[own ^ offset] = block_ref[...]
            edges_ref[own ^ offset, :TILE_ROWS, :] = block_ref[:TILE_ROWS, :]
            edges_ref[own ^ offset, TILE_ROWS:, :] = block_ref[cut - TILE_ROWS : cut, :]
        read_weights(kept, cut, score_ref, offset_ref, decay_ref, spikes_ref, spikes, weight_ref)

    block = kept[source].astype(F32)
    before = kept[jnp.maximum(source - 1, 0), kept.shape[1] - EXTRA :, :].astype(F32)
    before = jnp.where(source > 0, before, 0.0)
    beside = block[block.shape[0] - EXTRA :]
    values = convolved(line, block[:cut], before, beside, taps_ref, weight_ref, source, 0, total)
    wove(woven, values, keys_ref, source, 0, out_ref)
    read_ref[...] = total[...]


def early_rows(blocks, keys, score, taps, spikes, offset, decay, cut):
    sources, span = keys.shape[:2]
    height, share = blocks[0].shape
    heads = share // HEAD
    tiles = span // LANES
    reads = 2 * heads * tiles
    edges = (sources, 2 * TILE_ROWS, share)
    vmem = pl.BlockSpec(memory_space=pltpu.VMEM)
    smem = pl.BlockSpec(memory_space=pltpu.SMEM)
    inputs = [*blocks, keys, score, taps, spikes]
    weight = (sources, 2 * heads, tiles, LANES)
    return pl.pallas_call(
        lambda *refs: early_kernel(cut, *refs),
        grid=(sources,),
        in_specs=[vmem] * len(inputs) + [smem, smem],
        out_specs=[
            pl.BlockSpec((1, heads * cut, LANES), lambda s: (s, 0, 0)),
            whole((reads, share)),
            whole(edges),
            whole(weight),
        ],
        out_shape=[
            jax.ShapeDtypeStruct((sources, heads * span, LANES), BF16),
            jax.ShapeDtypeStruct((reads, share), F32),
            jax.ShapeDtypeStruct(edges, BF16),
            jax.ShapeDtypeStruct(weight, F32),
        ],
        scratch_shapes=[
            pltpu.VMEM((sources, height, share), BF16),
            line_scratch(cut, share),
            woven_scratch(cut, share),
            pltpu.VMEM((reads, share), F32),
            pltpu.VMEM((heads, sources * tiles, LANES), F32),
        ],
        compiler_params=pltpu.CompilerParams(vmem_limit_bytes=VMEM_LIMIT),
        cost_estimate=pl.CostEstimate(flops=2 * 10**9, bytes_accessed=6 * 10**6, transcendentals=10**6),
        name="early_rows",
    )(*(on_chip(x) for x in inputs), offset, decay)


def late_values_of(offset, block_ref, edges_ref, taps_ref, weight_ref, line, total, cut):
    source = lax.axis_index("sp") ^ offset
    sources = edges_ref.shape[0]
    before = edges_ref[source, TILE_ROWS:, :].astype(F32)[TILE_ROWS - 8 :]
    after = edges_ref[jnp.minimum(source + 1, sources - 1), :TILE_ROWS, :].astype(F32)[:8]
    after = jnp.where(source < sources - 1, after, 0.0)
    body = block_ref[...].astype(F32)
    return convolved(line, body, before, after, taps_ref, weight_ref, source, cut, total)


def late_kernel(cut, offsets, *refs):
    count = len(offsets)
    blocks = refs[:count]
    edges_ref, keys_ref, weight_ref, taps_ref, read_ref, _, out_ref, total, line, woven = refs[count:]
    step = pl.program_id(0)

    @pl.when(step == 0)
    def _():
        total[...] = read_ref[...]

    for index, offset in enumerate(offsets):

        @pl.when(step == index)
        def _(index=index, offset=offset):
            values = late_values_of(offset, blocks[index], edges_ref, taps_ref, weight_ref, line, total, cut)
            wove(woven, values, keys_ref, lax.axis_index("sp") ^ offset, cut, out_ref)


def wave_offset(step, offsets):
    offset = step + offsets[0]
    for index in range(1, len(offsets)):
        gap = offsets[index] - offsets[index - 1] - 1
        if gap:
            offset = offset + gap * (step >= index).astype(jnp.int32)
    return offset


def late_out_spec(offsets, shape):
    rows = shape[1] // 2
    return pl.BlockSpec((1, rows, LANES), lambda i: (lax.axis_index("sp") ^ wave_offset(i, offsets), 1, 0))


def late_rows(offsets, late, edges, keys, weight, taps, read, out, cut):
    rows, share = late[0].shape
    vmem = pl.BlockSpec(memory_space=pltpu.VMEM)
    inputs = [late[k] for k in offsets] + [edges, keys, weight, taps, read]
    return pl.pallas_call(
        lambda *refs: late_kernel(cut, offsets, *refs),
        grid=(len(offsets),),
        in_specs=[vmem] * len(inputs) + [pl.BlockSpec(memory_space=pl.ANY)],
        out_specs=[late_out_spec(offsets, out.shape), whole(read.shape)],
        out_shape=[jax.ShapeDtypeStruct(out.shape, BF16), jax.ShapeDtypeStruct(read.shape, F32)],
        scratch_shapes=[line_scratch(rows, share), woven_scratch(rows, share)],
        input_output_aliases={len(inputs): 0},
        compiler_params=pltpu.CompilerParams(vmem_limit_bytes=VMEM_LIMIT),
        cost_estimate=pl.CostEstimate(flops=10**9, bytes_accessed=2 * 10**6, transcendentals=10**6),
        name="late_rows",
    )(*(on_chip(x) for x in inputs), out)


def last_read_kernel(cut, offsets, *refs):
    count = len(offsets)
    blocks = refs[:count]
    edges_ref, weight_ref, taps_ref, read_ref, gate_ref, scale_ref, values_ref, gated_ref, square_ref, line, total = refs[
        count:
    ]
    total[...] = read_ref[...]
    for index, offset in enumerate(offsets):
        part = line.at[index]
        values = late_values_of(offset, blocks[index], edges_ref, taps_ref, weight_ref, part, total, cut)
        for tile, y in enumerate(values):
            values_ref[index, tile * LANES : (tile + 1) * LANES, :] = y
    tiles = weight_ref.shape[2]
    shape = total.shape
    heads = shape[1] // HEAD
    head = (lax.broadcasted_iota(jnp.int32, shape, 0) // tiles) % heads
    mine = head == lane_index(shape) // HEAD
    read = jnp.sum(jnp.where(mine, total[...], 0.0), axis=0, keepdims=True)
    read = jnp.concatenate([read[:, h * HEAD : (h + 1) * HEAD] for h in range(heads)], axis=0)
    gated = read * silu(gate_ref[0].astype(F32))
    gated_ref[...] = gated * scale_ref[...]
    square = jnp.sum(jnp.sum(gated * gated, axis=1, keepdims=True), axis=0, keepdims=True)
    square_ref[...] = jnp.broadcast_to(square, square_ref.shape)


def last_read(offsets, late, edges, weight, taps, read, gate, scale, cut):
    rows, share = late[0].shape
    vmem = pl.BlockSpec(memory_space=pltpu.VMEM)
    inputs = [late[k] for k in offsets] + [edges, weight, taps, read, gate, scale]
    return pl.pallas_call(
        lambda *refs: last_read_kernel(cut, offsets, *refs),
        in_specs=[vmem] * len(inputs),
        out_specs=[vmem] * 3,
        out_shape=[
            jax.ShapeDtypeStruct((len(offsets), rows, share), BF16),
            jax.ShapeDtypeStruct((share // HEAD, HEAD), F32),
            jax.ShapeDtypeStruct((1, LANES), F32),
        ],
        scratch_shapes=[pltpu.VMEM((len(offsets), rows + 16, share), F32), pltpu.VMEM(read.shape, F32)],
        compiler_params=pltpu.CompilerParams(vmem_limit_bytes=VMEM_LIMIT),
        cost_estimate=pl.CostEstimate(flops=10**9, bytes_accessed=10**6, transcendentals=10**6),
        name="last_read",
    )(*(on_chip(x) for x in inputs))


def last_rows_kernel(cut, offsets, values_ref, keys_ref, _, out_ref, woven):
    step = pl.program_id(0)
    rows = values_ref.shape[1]
    values = [values_ref[step, start : start + LANES, :] for start in range(0, rows, LANES)]
    wove(woven, values, keys_ref, lax.axis_index("sp") ^ wave_offset(step, offsets), cut, out_ref)


def last_rows(offsets, values, keys, out, cut):
    rows, share = values.shape[1:]
    vmem = pl.BlockSpec(memory_space=pltpu.VMEM)
    return pl.pallas_call(
        lambda *refs: last_rows_kernel(cut, offsets, *refs),
        grid=(len(offsets),),
        in_specs=[vmem, vmem, pl.BlockSpec(memory_space=pl.ANY)],
        out_specs=late_out_spec(offsets, out.shape),
        out_shape=jax.ShapeDtypeStruct(out.shape, BF16),
        scratch_shapes=[woven_scratch(rows, share)],
        input_output_aliases={2: 0},
        compiler_params=pltpu.CompilerParams(vmem_limit_bytes=VMEM_LIMIT),
        cost_estimate=pl.CostEstimate(flops=10**9, bytes_accessed=2 * 10**6, transcendentals=0),
        name="last_rows",
    )(on_chip(values), on_chip(keys), out)


def on_device(
    context_input_tensor,
    content_mapping_matrix,
    address_mapping_matrix,
    increment_mapping_matrix,
    increment_speed_offset,
    channel_fading_exponent,
    extra_damping_spikes,
    content_smoothing_coefficients,
    address_smoothing_coefficients,
    newest_lookup_matrix,
    newest_output_switch,
    cluster_scaling_coefficients,
):
    rows = context_input_tensor[0]
    span = rows.shape[0]
    repeats = HEADS // GROUPS
    heads = increment_speed_offset.shape[0]
    group_devices = repeats // heads
    devices = lax.axis_size("sp")
    cut = span // 2

    blocks = key_blocks(rows, address_mapping_matrix, group_devices)
    direct = [None] * (GROUPS - 1)
    for offset in range(1, GROUPS):
        direct[offset - 1] = flip_permute(blocks[offset], offset * group_devices)
    early = early_values(rows, content_mapping_matrix, increment_mapping_matrix.T, blocks[0], devices, cut)
    late = late_values(rows, content_mapping_matrix, early[0], devices, cut)
    held = [blocks[0]] + direct
    relayed = []
    for shift in range(1, group_devices):
        for offset in range(GROUPS):
            relayed.append(flip_permute(held[offset], shift))
    early_blocks, late_blocks = [early[0]], [late[0]]
    for offset in range(1, devices):
        early_blocks.append(flip_permute(early[offset], offset))
        late_blocks.append(flip_permute(late[offset], offset))

    keys, score = key_read(held + relayed, address_smoothing_coefficients, newest_lookup_matrix, group_devices, span)
    taps = content_smoothing_coefficients
    out, read, edges, weight = early_rows(
        early_blocks,
        keys,
        score,
        taps,
        extra_damping_spikes,
        increment_speed_offset,
        channel_fading_exponent,
        cut,
    )
    half = devices // 2
    first = list(range(half))
    middle = [offset for offset in range(half, devices) if offset % group_devices == 0]
    final = [offset for offset in range(half, devices) if offset % group_devices]
    for wave in (first, middle):
        out, read = late_rows(wave, late_blocks, edges, keys, weight, taps, read, out, cut)
    values, gated, group_sq = last_read(final, late_blocks, edges, weight, taps, read, newest_output_switch, cluster_scaling_coefficients, cut)
    for level in range(group_devices.bit_length() - 1):
        group_sq = group_sq + flip_permute(group_sq, 2**level)
    out = last_rows(final, values, keys, out, cut)
    scaled = gated * lax.rsqrt(group_sq[0, 0] / (repeats * HEAD) + EPS)
    store = out.reshape(1, devices * span, heads, HEAD + STATE)
    return store, scaled.astype(BF16).reshape(1, heads, HEAD)


def solution(mesh):
    placed = (
        P(("gr", "tp"), "sp", None),
        P(),
        P(),
        P(),
        P("sp"),
        P("sp"),
        P(("gr", "tp"), "sp", None),
        P(None, "sp", None),
        P(),
        P(("gr", "tp"), None, None),
        P(("gr", "tp"), "sp", None),
        P("sp", None),
    )

    return jax.shard_map(
        on_device,
        mesh=mesh,
        in_specs=placed,
        out_specs=(P(("gr", "tp"), None, "sp", None), P(("gr", "tp"), "sp", None)),
        check_vma=False,
    )
```
